128 devices in a mesh: sp: 16 (over z, y), tp: 8 (over x, core).
Axes of the slice: x: 4, y: 4, z: 4, core: 2. Of those that a mesh axis runs over, the one named last changes fastest.
Arguments:
- stream_in: bfloat16 [8192, 4096], P('sp', 'tp'), may hold values from -12 to 12
- norm_gain: float32 [2, 4096], replicated, may hold values from 0.1 to 1.9
- value_proj: bfloat16 [2, 4096, 4096], P(None, 'sp', 'tp'), may hold values from -0.09375 to 0.09375
- gate_proj: bfloat16 [2, 4096, 4096], P(None, 'sp', 'tp'), may hold values from -0.09375 to 0.09375
- out_proj: bfloat16 [2, 4096, 4096], P(None, 'sp', 'tp'), may hold values from -0.1875 to 0.1875
- conv_taps: float32 [2, 4, 4096], replicated, may hold values from -3 to 3
- block_gates: bfloat16 [2, 2, 2, 4096, 128], P(None, None, None, 'tp'), may hold values from -0.5 to 0.5
- forget_rate: float32 [2, 2, 4096], replicated, may hold values from 0 to 0.05, as said below
Outputs:
- stream_out: bfloat16 [8192, 4096], P('sp', 'tp')
The draws below stay inside these ranges and needn't reach their ends.
Inputs may be any that keep to these rules, and one draw needn't show every extreme that they name: `forget_rate`: positive.
All inputs are finite; a program needn't handle non-finite values.
Results may differ from the reference program's by a relative error of at most 0.025.
Values may be sent and summed in bfloat16 or wider, within the bound.
No kernel may reach another device: no remote copies, remote signals or barrier semaphores. Data moves between devices by JAX's collectives and lax.ppermute only.
A program may use at most 192 MiB of HBM per device.

```python
import math
import jax
import jax.numpy as jnp
from jax import lax

D = 4096
W = 4096
BLK = 128
LAYERS = 2
TOK_DEV = 512
TOKENS = 8192
N_TP = 8


def draw_stream_in(key, part):
    subkeys = jax.random.split(key, 6)
    base = jax.random.normal(subkeys[0], (TOKENS, D), jnp.float32)
    phase = jax.random.uniform(subkeys[1], (), jnp.float32, -math.pi, math.pi)
    position = jnp.arange(D).astype(jnp.float32) / D
    channel_scale = jnp.exp(0.9 * jnp.cos(2.0 * math.pi * position + phase) + jax.random.uniform(subkeys[2], (D,), jnp.float32, -0.3, 0.3))
    nblocks = (TOKENS + TOK_DEV - 1) // TOK_DEV
    block_mix = jax.random.normal(subkeys[3], (nblocks, D), jnp.float32)
    block_mix = block_mix * jax.random.uniform(subkeys[4], (nblocks, 1), jnp.float32, 0.5, 3.0)
    row_block = jnp.arange(TOKENS) // TOK_DEV
    result = base * channel_scale + block_mix[row_block]
    return jnp.clip(result, -12.0, 12.0).astype(jnp.bfloat16)


def draw_forget_rate(key, part):
    subkeys = jax.random.split(key, 3)
    shape = (LAYERS, 2, W)
    keep_share = 0.5
    slow_pick = jax.random.uniform(subkeys[0], shape, jnp.float32) < keep_share
    slow_rate = jnp.exp(jax.random.uniform(subkeys[1], shape, jnp.float32, math.log(0.02), math.log(0.2))) / TOKENS
    fast_hi = max(0.012, 0.4 / TOK_DEV)
    fast_rate = jnp.exp(jax.random.uniform(subkeys[2], shape, jnp.float32, math.log(fast_hi / 4.0), math.log(fast_hi)))
    return jnp.where(slow_pick, slow_rate, fast_rate)


def block_levels(stream_key, extent, shards, smallest, top_value):
    level, own = 1.0, jax.random.fold_in(stream_key, 6)
    for dim, blocks in shards:
        draws = jnp.exp(jax.random.uniform(jax.random.fold_in(own, dim), (blocks,), jnp.float32, smallest / len(shards), top_value / len(shards)))
        level = level * jnp.repeat(draws, extent[dim] // blocks).reshape([-1 if axis == dim else 1 for axis in range(len(extent))])
    return level


def scatter_about(own_key, dims, scale, reach, pieces=(), kind=jnp.bfloat16):
    level = block_levels(own_key, dims, pieces, -0.22, 0.18) if pieces else 1.0
    array = jax.random.normal(own_key, dims, jnp.float32) * scale * level
    return jnp.minimum(jnp.maximum(array, -reach), reach).astype(kind)


def setup_inputs(seed: int = 0) -> dict:
    seeds = jax.random.split(jax.random.key(seed), 9)
    stream_in = draw_stream_in(jax.random.fold_in(seeds[8], 71), 0)
    norm_gain = jnp.clip(1.0 + 0.18 * jax.random.normal(seeds[1], (LAYERS, D), jnp.float32), 0.1, 1.9)
    value_proj = scatter_about(seeds[2], (LAYERS, D, W), D ** -0.5, 0.09375, ((1, 16), (2, 8)))
    gate_proj = scatter_about(seeds[3], (LAYERS, D, W), D ** -0.5, 0.09375, ((1, 16), (2, 8)))
    out_proj = scatter_about(seeds[4], (LAYERS, D, W), (W // 4) ** -0.5, 0.1875, ((1, 16), (2, 8)))
    conv_taps = scatter_about(seeds[5], (LAYERS, 4, W), 0.8, 3.0, (), jnp.float32)
    block_gates = scatter_about(seeds[6], (LAYERS, 2, 2, W, BLK), BLK ** -0.5, 0.5, ((3, 8),))
    forget_rate = draw_forget_rate(jax.random.fold_in(seeds[8], 71), 0)
    return dict(stream_in=stream_in, norm_gain=norm_gain, value_proj=value_proj, gate_proj=gate_proj, out_proj=out_proj, conv_taps=conv_taps, block_gates=block_gates, forget_rate=forget_rate)


GATE_SCALE = 8.0
NORM_EPS = 1e-06

def pair_combine(earlier, latter):
    return (earlier[0] * latter[0], latter[0] * earlier[1] + latter[1])

def convolve(padded, taps_layer, length):
    values = padded.astype(jnp.float32)
    return sum((values[offset:offset + length] * taps_layer[offset] for offset in range(4)))

def gate_inputs(conv_out, gate_layer):
    count, width = conv_out.shape
    block_size = gate_layer.shape[-1]
    nblocks = width // block_size
    blocked = conv_out.reshape(count, nblocks, block_size)
    weights = gate_layer.astype(jnp.float32).reshape(4, nblocks, block_size, block_size)
    pre = jnp.einsum('tnc,gncd->gtnd', blocked, weights, precision=lax.Precision.HIGHEST)
    return pre.reshape(4, count, width)

def decay_inputs(conv_out, pre, rate_layer, direction):
    recur_gate = jax.nn.sigmoid(pre[2 * direction])
    input_gate = jax.nn.sigmoid(pre[2 * direction + 1])
    log_decay = -GATE_SCALE * recur_gate * rate_layer[direction]
    decay = jnp.exp(log_decay)
    drive = jnp.sqrt(-jnp.expm1(2.0 * log_decay)) * input_gate * conv_out
    return (decay, drive)

def reference(stream_in, norm_gain, value_proj, gate_proj, out_proj, conv_taps, block_gates, forget_rate):
    stream = stream_in
    length = stream_in.shape[0]
    group_width = W // N_TP
    for layer_index in range(LAYERS):
        values = stream.astype(jnp.float32)
        scale = lax.rsqrt(lax.optimization_barrier(jnp.mean(values * values, axis=1, keepdims=True)) + NORM_EPS)
        normed = (values * scale * norm_gain[layer_index]).astype(jnp.bfloat16)
        mix_in = jnp.dot(normed, value_proj[layer_index], preferred_element_type=jnp.float32).astype(jnp.bfloat16)
        gate_z = jnp.dot(normed, gate_proj[layer_index], preferred_element_type=jnp.float32).astype(jnp.bfloat16)
        padded = jnp.pad(mix_in, ((2, 1), (0, 0)))
        conv_out = convolve(padded, conv_taps[layer_index], length)
        pre = gate_inputs(conv_out, block_gates[layer_index])
        fwd_decay, fwd_drive = decay_inputs(conv_out, pre, forget_rate[layer_index], 0)
        bwd_decay, bwd_drive = decay_inputs(conv_out, pre, forget_rate[layer_index], 1)
        _, fwd_state = lax.associative_scan(pair_combine, (fwd_decay, fwd_drive), axis=0)
        _, bwd_flip = lax.associative_scan(pair_combine, (jnp.flip(bwd_decay, 0), jnp.flip(bwd_drive, 0)), axis=0)
        both = fwd_state + jnp.flip(bwd_flip, 0)
        mixed = (both * jax.nn.silu(gate_z.astype(jnp.float32))).astype(jnp.bfloat16)
        branch = jnp.zeros((length, D), jnp.float32)
        for group in range(N_TP):
            part = lax.dot_general(mixed[:, group * group_width:(group + 1) * group_width], out_proj[layer_index][:, group * group_width:(group + 1) * group_width], (((1,), (1,)), ((), ())), preferred_element_type=jnp.float32)
            rounded = lax.optimization_barrier(part.astype(jnp.bfloat16))
            branch = branch + rounded.astype(jnp.float32)
        stream = (values + branch).astype(jnp.bfloat16)
    return stream
```

```python
import jax
import jax.numpy as jnp
from jax import lax
from jax.experimental import pallas as pl
from jax.experimental.pallas import tpu as pltpu
from jax.sharding import PartitionSpec as P

GATE_SCALE = 8.0
NORM_EPS = 1e-06
F32 = jnp.float32
BF16 = jnp.bfloat16


CHUNKS = 8
VMEM_LIMIT = 24 * 2**20
HALO = 16


def to_tiles(array):
    rows, width = array.shape
    return array.reshape(CHUNKS, rows // CHUNKS, width).swapaxes(0, 1).reshape(rows, width)


def to_tokens(array):
    rows, width = array.shape
    return array.reshape(rows // CHUNKS, CHUNKS, width).swapaxes(0, 1).reshape(rows, width)


def shifted(array, axis, move):
    count = lax.axis_size(axis)
    return lax.ppermute(array, axis, [(i, move(i)) for i in range(count)])


def across(array):
    return shifted(array, "tp", lambda i: i ^ 1)


def along_x(array, step):
    return shifted(array, "tp", lambda i: (i + 2 * step) % 8)


def token_halo(top, end):
    rows, width = end.shape
    count = lax.axis_size("sp")
    owners = lax.axis_size("tp")
    ends = jnp.concatenate([end[rows - 9 : rows - 8], end[rows - 1 :], top[:1], top[:1]], axis=0)
    every = lax.all_to_all(
        jnp.broadcast_to(ends[None], (owners, *ends.shape)), "tp", 0, 0, tiled=True
    )
    before = lax.ppermute(every[:, :2], "sp", [(i, i + 1) for i in range(count - 1)])
    after = lax.ppermute(every[:, 2:], "sp", [(i + 1, i) for i in range(count - 1)])
    rest = jnp.zeros((owners, HALO - 4, width), end.dtype)
    return jnp.concatenate([before, after, rest], axis=1)


def gathered_stream(top, end):
    left_top = along_x(top, 1)
    right_end = along_x(end, -1)
    left_end = along_x(end, 1)
    right_top = along_x(top, -1)
    far_top = along_x(left_top, 1)
    far_end = along_x(right_end, -1)
    same = (top, end, left_top, left_end, right_top, right_end, far_top, far_end)
    return same + tuple(across(part) for part in same)


OFFSETS = (0, -1, 1, 2)


def block_of(rank, dx, flip):
    core = rank % 2
    return 2 * ((rank // 2 + dx + 4) % 4) + (1 - core if flip else core)


def weight_copies(weight, which, rank, offsets, target, sems):
    size = target.shape[1]
    copies = []
    for n, (dx, flip) in enumerate(offsets):
        at = pl.multiple_of(block_of(rank, dx, flip) * size, size)
        copies.append(
            pltpu.make_async_copy(
                weight.at[which, pl.ds(at, size), :], target.at[n], sems.at[n]
            )
        )
        copies[-1].start()
    return copies


def contracted(rows, weight_in, copies, total):
    for k, copy in enumerate(copies):
        copy.wait()
        term = jnp.dot(rows[k], weight_in[k], preferred_element_type=F32)
        if k == 0:
            total[...] = term
        else:
            total[...] += term


def row_scale(squares, width):
    return lax.rsqrt(jnp.sum(squares[...], axis=1, keepdims=True) / width + NORM_EPS)


def value_body(which, layer, rank, gain, halo, *refs):
    pieces, weight = refs[:16], refs[16]
    out, rows, squares, weight_in, total, sems = refs[17:]
    offsets = [(dx, flip) for flip in (0, 1) for dx in OFFSETS]
    copies = weight_copies(weight, which, rank[0], offsets, weight_in, sems)
    half, width = pieces[0].shape
    step = 64
    for k, (dx, flip) in enumerate(offsets):
        block = block_of(rank[0], dx, flip)
        scale = gain[layer : layer + 1, pl.ds(pl.multiple_of(block * width, width), width)]

        def put(raw, at, k=k, scale=scale):
            raw = raw.astype(F32)
            rows[k, at, :] = (raw * scale).astype(BF16)
            power = raw * raw
            lanes = sum(power[:, 128 * q : 128 * (q + 1)] for q in range(width // 128))
            if k == 0:
                squares[at, :] = lanes
            else:
                squares[at, :] += lanes

        for side in range(2):
            piece = pieces[2 * k + side]

            def chunk(n, carry, piece=piece, side=side, put=put):
                at = pl.multiple_of(n * step, step)
                put(piece[pl.ds(at, step), :], pl.ds(at + side * half, step))
                return carry

            lax.fori_loop(0, half // step, chunk, 0)
        put(halo[block], pl.ds(2 * half, HALO))
    contracted(rows, weight_in, copies, total)
    result = total[...] * row_scale(squares, width * len(offsets))
    out[...] = result.astype(BF16)


def gate_body(which, rank, rows, squares, weight, out, weight_in, total, sems):
    offsets = [(dx, flip) for flip in (0, 1) for dx in OFFSETS]
    copies = weight_copies(weight, which, rank[0], offsets, weight_in, sems)
    width = weight_in.shape[2]
    contracted(rows, weight_in, copies, total)
    result = total[...] * row_scale(squares, width * len(offsets))
    out[...] = result[: out.shape[0]].astype(BF16)


def in_smem():
    return pl.BlockSpec(memory_space=pltpu.SMEM)


def in_vmem():
    return pl.BlockSpec(memory_space=pltpu.VMEM)


def in_hbm():
    return pl.BlockSpec(memory_space=pltpu.HBM)


def product_cost(rows, width, count):
    return pl.CostEstimate(
        flops=2 * count * rows * width * width,
        bytes_accessed=2 * count * width * width,
        transcendentals=0,
    )


def value_rows(rank, pieces, halo, norm_gain, layer, weights, which):
    half, width = pieces[0].shape
    count = norm_gain.shape[1] // width
    deep = 2 * half + HALO
    return pl.pallas_call(
        lambda *refs: value_body(which, layer, *refs),
        out_shape=[
            jax.ShapeDtypeStruct((deep, width), BF16),
            jax.ShapeDtypeStruct((count, deep, width), BF16),
            jax.ShapeDtypeStruct((deep, 128), F32),
        ],
        in_specs=[in_smem()] + [in_vmem()] * 18 + [in_hbm()],
        out_specs=[in_vmem()] * 3,
        scratch_shapes=[
            pltpu.VMEM((count, width, width), BF16),
            pltpu.VMEM((deep, width), F32),
            pltpu.SemaphoreType.DMA((count,)),
        ],
        compiler_params=pltpu.CompilerParams(vmem_limit_bytes=VMEM_LIMIT),
        cost_estimate=product_cost(deep, width, count),
        name="value_rows",
    )(rank, norm_gain, halo, *pieces, weights)


def gate_rows(rank, rows, squares, weights, which):
    count, deep, width = rows.shape
    return pl.pallas_call(
        lambda *refs: gate_body(which, *refs),
        out_shape=jax.ShapeDtypeStruct((deep - HALO, width), BF16),
        in_specs=[in_smem(), in_vmem(), in_vmem(), in_hbm()],
        out_specs=in_vmem(),
        scratch_shapes=[
            pltpu.VMEM((count, width, width), BF16),
            pltpu.VMEM((deep, width), F32),
            pltpu.SemaphoreType.DMA((count,)),
        ],
        compiler_params=pltpu.CompilerParams(vmem_limit_bytes=VMEM_LIMIT),
        cost_estimate=product_cost(deep, width, count),
        name="gate_rows",
    )(rank, rows, squares, weights)


def scan_body(
    rank, mix, taps, rate, gates, local, fwd_cum, bwd_cum, coef, edge, padded, conv, pre
):
    steps = conv.shape[0] // CHUNKS
    length = conv.shape[0]
    sub = lax.broadcasted_iota(jnp.int32, (CHUNKS, 128), 0)
    rows = mix[...].astype(F32)
    halo = rows[length : length + 8]
    padded[16 : 16 + length] = rows[:length]
    padded[0:8] = jnp.where(
        sub == 0, halo[0:1], pltpu.roll(rows[length - 16 : length - 8], 1, axis=0)
    )
    padded[8:16] = jnp.where(sub == 0, halo[1:2], pltpu.roll(rows[length - 8 : length], 1, axis=0))
    padded[16 + length : 24 + length] = jnp.where(
        sub == CHUNKS - 1, halo[2:3], pltpu.roll(rows[0:8], CHUNKS - 1, axis=0)
    )
    for part in range(8):
        lo = part * (length // 8)
        hi = lo + length // 8
        conv[lo:hi] = sum(padded[lo + 8 * k : hi + 8 * k] * taps[0, k : k + 1] for k in range(4))
    lhs = conv[...].astype(BF16)
    for g in range(4):
        pre[g] = jnp.dot(lhs, gates[0, g // 2, g % 2], preferred_element_type=F32)

    def cell(i, e):
        at = pl.ds(pl.multiple_of(i * CHUNKS, CHUNKS), CHUNKS)
        recur = jax.nn.sigmoid(pre[2 * e, at, :])
        entry = jax.nn.sigmoid(pre[2 * e + 1, at, :])
        log_a = (-GATE_SCALE) * recur * rate[0, e : e + 1]
        decay = jnp.exp(log_a)
        x = 2.0 * log_a
        near = x * (1.0 + x * (0.5 + x * (1.0 / 6 + x * (1.0 / 24 + x * (1.0 / 120)))))
        room = -jnp.where(x > -0.125, near, decay * decay - 1.0)
        return at, decay, jnp.sqrt(room) * entry * conv[at, :]

    zero = jnp.zeros((CHUNKS, 128), F32)
    one = jnp.ones((CHUNKS, 128), F32)
    inner = 8

    def forward(block, carry):
        state, cum = carry
        for n in range(inner):
            at, decay, drive = cell(block * inner + n, 0)
            state = decay * state + drive
            cum = decay * cum
            local[at, :] = state
            fwd_cum[at, :] = cum
        return state, cum

    def backward(block, carry):
        state, cum = carry
        for n in range(inner):
            at, decay, drive = cell(steps - 1 - (block * inner + n), 1)
            state = decay * state + drive
            cum = decay * cum
            local[at, :] += state
            bwd_cum[at, :] = cum
        return state, cum

    state_f, cum_f = lax.fori_loop(0, steps // inner, forward, (zero, one))
    state_b, cum_b = lax.fori_loop(0, steps // inner, backward, (zero, one))
    alpha = jnp.zeros((1, 128), F32)
    beta = jnp.ones((1, 128), F32)
    for s in range(CHUNKS):
        coef[0, s : s + 1] = alpha
        coef[1, s : s + 1] = beta
        alpha = state_f[s : s + 1] + cum_f[s : s + 1] * alpha
        beta = cum_f[s : s + 1] * beta
    sums_f = (beta, alpha)
    alpha = jnp.zeros((1, 128), F32)
    beta = jnp.ones((1, 128), F32)
    for s in reversed(range(CHUNKS)):
        coef[2, s : s + 1] = alpha
        coef[3, s : s + 1] = beta
        alpha = state_b[s : s + 1] + cum_b[s : s + 1] * alpha
        beta = cum_b[s : s + 1] * beta
    edge[...] = jnp.broadcast_to(
        jnp.concatenate([*sums_f, beta, alpha], axis=0)[None], edge.shape
    )


def scanned(rank, mix, conv_taps, forget_rate, block_gates, layer, copies):
    deep, width = mix.shape
    length = deep - HALO
    blocks = width // 128
    column = lambda b, rank: (0, b)
    owned = lambda b, rank: (layer, 0, rank[0] * blocks + b)
    return pl.pallas_call(
        scan_body,
        grid_spec=pltpu.PrefetchScalarGridSpec(
            num_scalar_prefetch=1,
            grid=(blocks,),
            in_specs=[
                pl.BlockSpec((deep, 128), column),
                pl.BlockSpec((1, 4, 128), owned),
                pl.BlockSpec((1, 2, 128), owned),
                pl.BlockSpec((1, 2, 2, 128, 128), lambda b, rank: (layer, 0, 0, b, 0)),
            ],
            out_specs=[
                pl.BlockSpec((length, 128), column),
                pl.BlockSpec((length, 128), column),
                pl.BlockSpec((length, 128), column),
                pl.BlockSpec((4, CHUNKS, 128), lambda b, rank: (0, 0, b)),
                pl.BlockSpec((copies, 4, 128), lambda b, rank: (0, 0, b)),
            ],
            scratch_shapes=[
                pltpu.VMEM((length + 24, 128), F32),
                pltpu.VMEM((length, 128), F32),
                pltpu.VMEM((4, length, 128), F32),
            ],
        ),
        out_shape=[
            jax.ShapeDtypeStruct((length, width), F32),
            jax.ShapeDtypeStruct((length, width), F32),
            jax.ShapeDtypeStruct((length, width), F32),
            jax.ShapeDtypeStruct((4, CHUNKS, width), F32),
            jax.ShapeDtypeStruct((copies, 4, width), F32),
        ],
        compiler_params=pltpu.CompilerParams(vmem_limit_bytes=VMEM_LIMIT),
        cost_estimate=pl.CostEstimate(
            flops=10_000_000_000, bytes_accessed=4_000_000, transcendentals=4_000_000
        ),
        name="scan",
    )(rank, mix, conv_taps, forget_rate, block_gates)


LEAVE = (2, 1, -1, 0)


def features(mixed, weight):
    return lax.dot_general(
        mixed, weight, (((1,), (1,)), ((), ())), preferred_element_type=F32
    ).astype(BF16)


def give_body(
    which, rank, place, edges, local, fwd_cum, bwd_cum, coef, gate, weight,
    mixed, far, rest, weight_in, sems,
):
    copies = weight_copies(weight, which, rank[0], [(dx, 1) for dx in LEAVE], weight_in, sems)
    mine = place[0]
    count, _, width = edges.shape
    enter_f = jnp.zeros((1, width), F32)
    enter_b = jnp.zeros((1, width), F32)
    for r in range(count):
        enter_f = jnp.where(r < mine, edges[r, 1:2] + edges[r, 0:1] * enter_f, enter_f)
        q = count - 1 - r
        enter_b = jnp.where(q > mine, edges[q, 3:4] + edges[q, 2:3] * enter_b, enter_b)
    from_f = coef[0] + coef[1] * enter_f
    from_b = coef[2] + coef[3] * enter_b
    group = 64
    for c in range(width // 128):
        col = slice(128 * c, 128 * (c + 1))
        tiled_f = jnp.concatenate([from_f[:, col]] * (group // CHUNKS), axis=0)
        tiled_b = jnp.concatenate([from_b[:, col]] * (group // CHUNKS), axis=0)

        def part(n, carry, col=col, tiled_f=tiled_f, tiled_b=tiled_b):
            at = pl.ds(pl.multiple_of(n * group, group), group)
            both = local[at, col] + fwd_cum[at, col] * tiled_f + bwd_cum[at, col] * tiled_b
            z = gate[at, col].astype(F32)
            mixed[at, col] = (both * (z * jax.nn.sigmoid(z))).astype(BF16)
            return carry

        lax.fori_loop(0, local.shape[0] // group, part, 0)
    for n, copy in enumerate(copies):
        copy.wait()
        value = features(mixed[...], weight_in[n])
        if n == 0:
            far[...] = value
        else:
            rest[n - 1] = value


def given(rank, place, edges, local, fwd_cum, bwd_cum, coef, gate, weights, which):
    length, width = local.shape
    return pl.pallas_call(
        lambda *refs: give_body(which, *refs),
        in_specs=[in_smem(), in_smem()] + [in_vmem()] * 6 + [in_hbm()],
        out_specs=[in_vmem()] * 3,
        out_shape=[
            jax.ShapeDtypeStruct((length, width), BF16),
            jax.ShapeDtypeStruct((length, width), BF16),
            jax.ShapeDtypeStruct((3, length, width), BF16),
        ],
        scratch_shapes=[
            pltpu.VMEM((4, width, width), BF16),
            pltpu.SemaphoreType.DMA((4,)),
        ],
        compiler_params=pltpu.CompilerParams(vmem_limit_bytes=VMEM_LIMIT),
        cost_estimate=product_cost(length, width, 4),
        name="given",
    )(rank, place, edges, local, fwd_cum, bwd_cum, coef, gate, weights)


def keep_body(which, rank, mixed, weight, out, weight_in, sems):
    copies = weight_copies(weight, which, rank[0], [(dx, 0) for dx in LEAVE], weight_in, sems)
    for n, copy in enumerate(copies):
        copy.wait()
        out[n] = features(mixed[...], weight_in[n])


def kept(rank, mixed, weights, which):
    length, width = mixed.shape
    return pl.pallas_call(
        lambda *refs: keep_body(which, *refs),
        in_specs=[in_smem(), in_vmem(), in_hbm()],
        out_specs=in_vmem(),
        out_shape=jax.ShapeDtypeStruct((4, length, width), BF16),
        scratch_shapes=[
            pltpu.VMEM((4, width, width), BF16),
            pltpu.SemaphoreType.DMA((4,)),
        ],
        compiler_params=pltpu.CompilerParams(vmem_limit_bytes=VMEM_LIMIT),
        cost_estimate=product_cost(length, width, 4),
        name="kept",
    )(rank, mixed, weights)


def per_device(
    stream_in, norm_gain, value_proj, gate_proj, out_proj, conv_taps, block_gates, forget_rate
):
    rank = lax.axis_index("tp").reshape(1)
    place = lax.axis_index("sp").reshape(1)
    length, width = stream_in.shape
    half = length // 2
    stream = to_tiles(stream_in)
    top, end = stream[:half], stream[half:]
    weights = []
    for layer in range(value_proj.shape[0]):
        held = jnp.stack([value_proj[layer], gate_proj[layer], out_proj[layer]])
        weights.append(lax.all_gather(held, "sp", axis=1, tiled=True))
    for layer in range(value_proj.shape[0]):
        full = weights[layer]
        pieces = gathered_stream(top, end)
        halo = token_halo(top, end)
        mix_in, rows, squares = value_rows(rank, pieces, halo, norm_gain, layer, full, 0)
        local, fwd_cum, bwd_cum, coef, edge = scanned(
            rank, mix_in, conv_taps, forget_rate, block_gates, layer, lax.axis_size("sp")
        )
        edges = lax.all_to_all(edge, "sp", 0, 0, tiled=True)
        gate_z = gate_rows(rank, rows, squares, full, 1)
        mixed, far_give, rest_give = given(
            rank, place, edges, local, fwd_cum, bwd_cum, coef, gate_z, full, 2
        )
        far_away = across(far_give).astype(F32)
        rest_away = across(rest_give).astype(F32)
        keep = kept(rank, mixed, full, 2).astype(F32)
        far = (keep[0] + far_away).astype(BF16)
        up = keep[1] + rest_away[0]
        down = keep[2] + rest_away[1]
        own = keep[3] + rest_away[2]
        relay_top = along_x(far[:half], 1)
        relay_end = along_x(far[half:], -1)
        up_end = along_x(up[half:].astype(BF16), 1)
        down_top = along_x(down[:half].astype(BF16), -1)
        up_top = along_x((up[:half] + relay_top.astype(F32)).astype(BF16), 1)
        down_end = along_x((down[half:] + relay_end.astype(F32)).astype(BF16), -1)
        top = top.astype(F32) + own[:half] + up_top.astype(F32) + down_top.astype(F32)
        end = end.astype(F32) + own[half:] + up_end.astype(F32) + down_end.astype(F32)
        top, end = top.astype(BF16), end.astype(BF16)
    return to_tokens(jnp.concatenate([top, end], axis=0))


def solution(mesh):
    placed = (
        P("sp", "tp"),
        P(),
        P(None, "sp", "tp"),
        P(None, "sp", "tp"),
        P(None, "sp", "tp"),
        P(),
        P(None, None, None, "tp", None),
        P(),
    )
    return jax.shard_map(
        per_device, mesh=mesh, in_specs=placed, out_specs=P("sp", "tp"), check_vma=False
    )
```

```python
import jax
import jax.numpy as jnp
from jax import lax
from jax.experimental import pallas as pl
from jax.experimental.pallas import tpu as pltpu
from jax.sharding import PartitionSpec as P


GATE_SCALE = 8.0
NORM_EPS = 1e-06
F32 = jnp.float32
BF16 = jnp.bfloat16


CHUNKS = 8
VMEM_LIMIT = 24 * 2**20
WEIGHT_LIMIT = 50 * 2**20
HALO = 16


def to_tiles(array):
    rows, width = array.shape
    return array.reshape(CHUNKS, rows // CHUNKS, width).swapaxes(0, 1).reshape(rows, width)


def to_tokens(array):
    rows, width = array.shape
    return array.reshape(rows // CHUNKS, CHUNKS, width).swapaxes(0, 1).reshape(rows, width)


def shifted(array, axis, move):
    count = lax.axis_size(axis)
    return lax.ppermute(array, axis, [(i, move(i)) for i in range(count)])


def across(array):
    return shifted(array, "tp", lambda i: i ^ 1)


def along_x(array, step):
    return shifted(array, "tp", lambda i: (i + 2 * step) % 8)


def token_halo(top, end):
    rows, width = end.shape
    count = lax.axis_size("sp")
    owners = lax.axis_size("tp")
    ends = jnp.concatenate([end[rows - 9 : rows - 8], end[rows - 1 :], top[:1], top[:1]], axis=0)
    copies = jnp.broadcast_to(ends[None], (owners, *ends.shape))
    every = lax.all_to_all(copies, "tp", 0, 0, tiled=True)
    before = lax.ppermute(every[:, :2], "sp", [(i, i + 1) for i in range(count - 1)])
    after = lax.ppermute(every[:, 2:], "sp", [(i + 1, i) for i in range(count - 1)])
    rest = jnp.zeros((owners, HALO - 4, width), end.dtype)
    return jnp.concatenate([before, after, rest], axis=1)


def gathered_stream(top, end):
    left_top = along_x(top, 1)
    right_end = along_x(end, -1)
    left_end = along_x(end, 1)
    right_top = along_x(top, -1)
    far_top = along_x(left_top, 1)
    far_end = along_x(right_end, -1)
    same = (top, end, left_top, left_end, right_top, right_end, far_top, far_end)
    return same + tuple(across(part) for part in same)


OFFSETS = (0, -1, 1, 2)


def block_of(rank, dx, flip):
    core = rank % 2
    return 2 * ((rank // 2 + dx + 4) % 4) + (1 - core if flip else core)


def weight_copies(weight, which, rank, offsets, target, sems):
    size = target.shape[1]
    copies = []
    for n, (dx, flip) in enumerate(offsets):
        at = pl.multiple_of(block_of(rank, dx, flip) * size, size)
        copies.append(
            pltpu.make_async_copy(
                weight.at[which, pl.ds(at, size), :], target.at[n], sems.at[n]
            )
        )
        copies[-1].start()
    return copies


def contracted(rows, weight_in, copies, total):
    for k, copy in enumerate(copies):
        copy.wait()
        term = jnp.dot(rows[k], weight_in[k], preferred_element_type=F32)
        if k == 0:
            total[...] = term
        else:
            total[...] += term


def row_scale(squares, width):
    return lax.rsqrt(jnp.sum(squares[...], axis=1, keepdims=True) / width + NORM_EPS)


def value_body(which, layer, rank, gain, halo, *refs):
    pieces, weight = refs[:16], refs[16]
    out, rows, squares, weight_in, total, sems = refs[17:]
    offsets = [(dx, flip) for flip in (0, 1) for dx in OFFSETS]
    copies = weight_copies(weight, which, rank[0], offsets, weight_in, sems)
    half, width = pieces[0].shape
    step = 64
    for k, (dx, flip) in enumerate(offsets):
        block = block_of(rank[0], dx, flip)
        scale = gain[layer : layer + 1, pl.ds(pl.multiple_of(block * width, width), width)]

        def put(raw, at, k=k, scale=scale):
            raw = raw.astype(F32)
            rows[k, at, :] = (raw * scale).astype(BF16)
            power = raw * raw
            lanes = sum(power[:, 128 * q : 128 * (q + 1)] for q in range(width // 128))
            if k == 0:
                squares[at, :] = lanes
            else:
                squares[at, :] += lanes

        for side in range(2):
            piece = pieces[2 * k + side]

            def chunk(n, carry, piece=piece, side=side, put=put):
                at = pl.multiple_of(n * step, step)
                put(piece[pl.ds(at, step), :], pl.ds(at + side * half, step))
                return carry

            lax.fori_loop(0, half // step, chunk, 0)
        put(halo[block], pl.ds(2 * half, HALO))
    contracted(rows, weight_in, copies, total)
    result = total[...] * row_scale(squares, width * len(offsets))
    out[...] = result.astype(BF16)


def gate_body(which, rank, rows, squares, weight, out, weight_in, total, sems):
    offsets = [(dx, flip) for flip in (0, 1) for dx in OFFSETS]
    copies = weight_copies(weight, which, rank[0], offsets, weight_in, sems)
    width = weight_in.shape[2]
    contracted(rows, weight_in, copies, total)
    result = total[...] * row_scale(squares, width * len(offsets))
    out[...] = result[: out.shape[0]].astype(BF16)


def in_smem():
    return pl.BlockSpec(memory_space=pltpu.SMEM)


def in_vmem():
    return pl.BlockSpec(memory_space=pltpu.VMEM)


def in_hbm():
    return pl.BlockSpec(memory_space=pltpu.HBM)


def product_cost(rows, width, count):
    return pl.CostEstimate(
        flops=2 * count * rows * width * width,
        bytes_accessed=2 * count * width * width,
        transcendentals=0,
    )


def value_rows(rank, pieces, halo, norm_gain, layer, weights, which):
    half, width = pieces[0].shape
    count = norm_gain.shape[1] // width
    deep = 2 * half + HALO
    return pl.pallas_call(
        lambda *refs: value_body(which, layer, *refs),
        out_shape=[
            jax.ShapeDtypeStruct((deep, width), BF16),
            jax.ShapeDtypeStruct((count, deep, width), BF16),
            jax.ShapeDtypeStruct((deep, 128), F32),
        ],
        in_specs=[in_smem()] + [in_vmem()] * 18 + [in_hbm()],
        out_specs=[in_vmem()] * 3,
        scratch_shapes=[
            pltpu.VMEM((count, width, width), BF16),
            pltpu.VMEM((deep, width), F32),
            pltpu.SemaphoreType.DMA((count,)),
        ],
        compiler_params=pltpu.CompilerParams(vmem_limit_bytes=WEIGHT_LIMIT),
        cost_estimate=product_cost(deep, width, count),
        name="value_rows",
    )(rank, norm_gain, halo, *pieces, weights)


def gate_rows(rank, rows, squares, weights, which):
    count, deep, width = rows.shape
    return pl.pallas_call(
        lambda *refs: gate_body(which, *refs),
        out_shape=jax.ShapeDtypeStruct((deep - HALO, width), BF16),
        in_specs=[in_smem(), in_vmem(), in_vmem(), in_hbm()],
        out_specs=in_vmem(),
        scratch_shapes=[
            pltpu.VMEM((count, width, width), BF16),
            pltpu.VMEM((deep, width), F32),
            pltpu.SemaphoreType.DMA((count,)),
        ],
        compiler_params=pltpu.CompilerParams(vmem_limit_bytes=WEIGHT_LIMIT),
        cost_estimate=product_cost(deep, width, count),
        name="gate_rows",
    )(rank, rows, squares, weights)


def scan_body(
    rank, mix, taps, rate, gates, local, fwd_cum, bwd_cum, coef, edge, padded, conv, pre
):
    steps = conv.shape[0] // CHUNKS
    length = conv.shape[0]
    sub = lax.broadcasted_iota(jnp.int32, (CHUNKS, 128), 0)
    rows = mix[...].astype(F32)
    halo = rows[length : length + 8]
    padded[16 : 16 + length] = rows[:length]
    padded[0:8] = jnp.where(
        sub == 0, halo[0:1], pltpu.roll(rows[length - 16 : length - 8], 1, axis=0)
    )
    padded[8:16] = jnp.where(sub == 0, halo[1:2], pltpu.roll(rows[length - 8 : length], 1, axis=0))
    padded[16 + length : 24 + length] = jnp.where(
        sub == CHUNKS - 1, halo[2:3], pltpu.roll(rows[0:8], CHUNKS - 1, axis=0)
    )
    for part in range(8):
        lo = part * (length // 8)
        hi = lo + length // 8
        conv[lo:hi] = sum(padded[lo + 8 * k : hi + 8 * k] * taps[0, k : k + 1] for k in range(4))
    lhs = conv[...].astype(BF16)
    for g in range(4):
        pre[g] = jnp.dot(lhs, gates[0, g // 2, g % 2], preferred_element_type=F32)

    def cell(i, e):
        at = pl.ds(pl.multiple_of(i * CHUNKS, CHUNKS), CHUNKS)
        recur = jax.nn.sigmoid(pre[2 * e, at, :])
        entry = jax.nn.sigmoid(pre[2 * e + 1, at, :])
        log_a = (-GATE_SCALE) * recur * rate[0, e : e + 1]
        decay = jnp.exp(log_a)
        x = 2.0 * log_a
        near = x * (1.0 + x * (0.5 + x * (1.0 / 6 + x * (1.0 / 24 + x * (1.0 / 120)))))
        room = -jnp.where(x > -0.125, near, decay * decay - 1.0)
        return at, decay, jnp.sqrt(room) * entry * conv[at, :]

    zero = jnp.zeros((CHUNKS, 128), F32)
    one = jnp.ones((CHUNKS, 128), F32)
    inner = 8

    def forward(block, carry):
        state, cum = carry
        for n in range(inner):
            at, decay, drive = cell(block * inner + n, 0)
            state = decay * state + drive
            cum = decay * cum
            local[at, :] = state
            fwd_cum[at, :] = cum
        return state, cum

    def backward(block, carry):
        state, cum = carry
        for n in range(inner):
            at, decay, drive = cell(steps - 1 - (block * inner + n), 1)
            state = decay * state + drive
            cum = decay * cum
            local[at, :] += state
            bwd_cum[at, :] = cum
        return state, cum

    state_f, cum_f = lax.fori_loop(0, steps // inner, forward, (zero, one))
    state_b, cum_b = lax.fori_loop(0, steps // inner, backward, (zero, one))
    alpha = jnp.zeros((1, 128), F32)
    beta = jnp.ones((1, 128), F32)
    for s in range(CHUNKS):
        coef[0, s : s + 1] = alpha
        coef[1, s : s + 1] = beta
        alpha = state_f[s : s + 1] + cum_f[s : s + 1] * alpha
        beta = cum_f[s : s + 1] * beta
    sums_f = (beta, alpha)
    alpha = jnp.zeros((1, 128), F32)
    beta = jnp.ones((1, 128), F32)
    for s in reversed(range(CHUNKS)):
        coef[2, s : s + 1] = alpha
        coef[3, s : s + 1] = beta
        alpha = state_b[s : s + 1] + cum_b[s : s + 1] * alpha
        beta = cum_b[s : s + 1] * beta
    edge[...] = jnp.broadcast_to(
        jnp.concatenate([*sums_f, beta, alpha], axis=0)[None], edge.shape
    )


def scanned(rank, mix, conv_taps, forget_rate, block_gates, layer, copies):
    deep, width = mix.shape
    length = deep - HALO
    blocks = width // 128
    column = lambda b, rank: (0, b)
    owned = lambda b, rank: (layer, 0, rank[0] * blocks + b)
    return pl.pallas_call(
        scan_body,
        grid_spec=pltpu.PrefetchScalarGridSpec(
            num_scalar_prefetch=1,
            grid=(blocks,),
            in_specs=[
                pl.BlockSpec((deep, 128), column),
                pl.BlockSpec((1, 4, 128), owned),
                pl.BlockSpec((1, 2, 128), owned),
                pl.BlockSpec((1, 2, 2, 128, 128), lambda b, rank: (layer, 0, 0, b, 0)),
            ],
            out_specs=[
                pl.BlockSpec((length, 128), column),
                pl.BlockSpec((length, 128), column),
                pl.BlockSpec((length, 128), column),
                pl.BlockSpec((4, CHUNKS, 128), lambda b, rank: (0, 0, b)),
                pl.BlockSpec((copies, 4, 128), lambda b, rank: (0, 0, b)),
            ],
            scratch_shapes=[
                pltpu.VMEM((length + 24, 128), F32),
                pltpu.VMEM((length, 128), F32),
                pltpu.VMEM((4, length, 128), F32),
            ],
        ),
        out_shape=[
            jax.ShapeDtypeStruct((length, width), F32),
            jax.ShapeDtypeStruct((length, width), F32),
            jax.ShapeDtypeStruct((length, width), F32),
            jax.ShapeDtypeStruct((4, CHUNKS, width), F32),
            jax.ShapeDtypeStruct((copies, 4, width), F32),
        ],
        compiler_params=pltpu.CompilerParams(vmem_limit_bytes=VMEM_LIMIT),
        cost_estimate=pl.CostEstimate(
            flops=10_000_000_000, bytes_accessed=4_000_000, transcendentals=4_000_000
        ),
        name="scan",
    )(rank, mix, conv_taps, forget_rate, block_gates)


LEAVE = (2, 1, -1, 0)


def features(mixed, weight):
    return lax.dot_general(
        mixed, weight, (((1,), (1,)), ((), ())), preferred_element_type=F32
    ).astype(BF16)


def give_body(
    which, rank, place, edges, local, fwd_cum, bwd_cum, coef, gate, weight,
    mixed, far, rest, weight_in, sems,
):
    copies = weight_copies(weight, which, rank[0], [(dx, 1) for dx in LEAVE], weight_in, sems)
    mine = place[0]
    count, _, width = edges.shape
    enter_f = jnp.zeros((1, width), F32)
    enter_b = jnp.zeros((1, width), F32)
    for r in range(count):
        enter_f = jnp.where(r < mine, edges[r, 1:2] + edges[r, 0:1] * enter_f, enter_f)
        q = count - 1 - r
        enter_b = jnp.where(q > mine, edges[q, 3:4] + edges[q, 2:3] * enter_b, enter_b)
    from_f = coef[0] + coef[1] * enter_f
    from_b = coef[2] + coef[3] * enter_b
    group = 64
    for c in range(width // 128):
        col = slice(128 * c, 128 * (c + 1))
        tiled_f = jnp.concatenate([from_f[:, col]] * (group // CHUNKS), axis=0)
        tiled_b = jnp.concatenate([from_b[:, col]] * (group // CHUNKS), axis=0)

        def part(n, carry, col=col, tiled_f=tiled_f, tiled_b=tiled_b):
            at = pl.ds(pl.multiple_of(n * group, group), group)
            both = local[at, col] + fwd_cum[at, col] * tiled_f + bwd_cum[at, col] * tiled_b
            z = gate[at, col].astype(F32)
            mixed[at, col] = (both * (z * jax.nn.sigmoid(z))).astype(BF16)
            return carry

        lax.fori_loop(0, local.shape[0] // group, part, 0)
    for n, copy in enumerate(copies):
        copy.wait()
        value = features(mixed[...], weight_in[n])
        if n == 0:
            far[...] = value
        else:
            rest[n - 1] = value


def given(rank, place, edges, local, fwd_cum, bwd_cum, coef, gate, weights, which):
    length, width = local.shape
    return pl.pallas_call(
        lambda *refs: give_body(which, *refs),
        in_specs=[in_smem(), in_smem()] + [in_vmem()] * 6 + [in_hbm()],
        out_specs=[in_vmem()] * 3,
        out_shape=[
            jax.ShapeDtypeStruct((length, width), BF16),
            jax.ShapeDtypeStruct((length, width), BF16),
            jax.ShapeDtypeStruct((3, length, width), BF16),
        ],
        scratch_shapes=[
            pltpu.VMEM((4, width, width), BF16),
            pltpu.SemaphoreType.DMA((4,)),
        ],
        compiler_params=pltpu.CompilerParams(vmem_limit_bytes=WEIGHT_LIMIT),
        cost_estimate=product_cost(length, width, 4),
        name="given",
    )(rank, place, edges, local, fwd_cum, bwd_cum, coef, gate, weights)


def keep_body(which, rank, mixed, weight, out, weight_in, sems):
    copies = weight_copies(weight, which, rank[0], [(dx, 0) for dx in LEAVE], weight_in, sems)
    for n, copy in enumerate(copies):
        copy.wait()
        out[n] = features(mixed[...], weight_in[n])


def kept(rank, mixed, weights, which):
    length, width = mixed.shape
    return pl.pallas_call(
        lambda *refs: keep_body(which, *refs),
        in_specs=[in_smem(), in_vmem(), in_hbm()],
        out_specs=in_vmem(),
        out_shape=jax.ShapeDtypeStruct((4, length, width), BF16),
        scratch_shapes=[
            pltpu.VMEM((4, width, width), BF16),
            pltpu.SemaphoreType.DMA((4,)),
        ],
        compiler_params=pltpu.CompilerParams(vmem_limit_bytes=WEIGHT_LIMIT),
        cost_estimate=product_cost(length, width, 4),
        name="kept",
    )(rank, mixed, weights)


def per_device(
    stream_in, norm_gain, value_proj, gate_proj, out_proj, conv_taps, block_gates, forget_rate
):
    rank = lax.axis_index("tp").reshape(1)
    place = lax.axis_index("sp").reshape(1)
    length, _ = stream_in.shape
    half = length // 2
    stream = to_tiles(stream_in)
    top, end = stream[:half], stream[half:]
    weights = []
    for layer in range(value_proj.shape[0]):
        held = jnp.stack([value_proj[layer], gate_proj[layer], out_proj[layer]])
        weights.append(lax.all_gather(held, "sp", axis=1, tiled=True))
    for layer in range(value_proj.shape[0]):
        full = weights[layer]
        pieces = gathered_stream(top, end)
        halo = token_halo(top, end)
        mix_in, rows, squares = value_rows(rank, pieces, halo, norm_gain, layer, full, 0)
        local, fwd_cum, bwd_cum, coef, edge = scanned(
            rank, mix_in, conv_taps, forget_rate, block_gates, layer, lax.axis_size("sp")
        )
        edges = lax.all_to_all(edge, "sp", 0, 0, tiled=True)
        gate_z = gate_rows(rank, rows, squares, full, 1)
        mixed, far_give, rest_give = given(
            rank, place, edges, local, fwd_cum, bwd_cum, coef, gate_z, full, 2
        )
        far_away = across(far_give).astype(F32)
        rest_away = across(rest_give).astype(F32)
        keep = kept(rank, mixed, full, 2).astype(F32)
        far = (keep[0] + far_away).astype(BF16)
        up = keep[1] + rest_away[0]
        down = keep[2] + rest_away[1]
        own = keep[3] + rest_away[2]
        relay_top = along_x(far[:half], 1)
        relay_end = along_x(far[half:], -1)
        up_end = along_x(up[half:].astype(BF16), 1)
        down_top = along_x(down[:half].astype(BF16), -1)
        up_top = along_x((up[:half] + relay_top.astype(F32)).astype(BF16), 1)
        down_end = along_x((down[half:] + relay_end.astype(F32)).astype(BF16), -1)
        top = top.astype(F32) + own[:half] + up_top.astype(F32) + down_top.astype(F32)
        end = end.astype(F32) + own[half:] + up_end.astype(F32) + down_end.astype(F32)
        top, end = top.astype(BF16), end.astype(BF16)
    return to_tokens(jnp.concatenate([top, end], axis=0))


def solution(mesh):
    placed = (
        P("sp", "tp"),
        P(),
        P(None, "sp", "tp"),
        P(None, "sp", "tp"),
        P(None, "sp", "tp"),
        P(),
        P(None, None, None, "tp", None),
        P(),
    )
    return jax.shard_map(
        per_device, mesh=mesh, in_specs=placed, out_specs=P("sp", "tp"), check_vma=False
    )
```

```python
import jax
import jax.numpy as jnp
from jax import lax
from jax.experimental import pallas as pl
from jax.experimental.pallas import tpu as pltpu
from jax.sharding import PartitionSpec as P


GATE_SCALE = 8.0
NORM_EPS = 1e-06
F32 = jnp.float32
BF16 = jnp.bfloat16


CHUNKS = 8
SCAN_LIMIT = 16 * 2**20
PROJECT_LIMIT = 49 * 2**20
GIVE_LIMIT = 53 * 2**20
KEEP_LIMIT = 44 * 2**20
HALO = 16


def to_tiles(array):
    rows, width = array.shape
    return array.reshape(CHUNKS, rows // CHUNKS, width).swapaxes(0, 1).reshape(rows, width)


def to_tokens(array):
    rows, width = array.shape
    return array.reshape(rows // CHUNKS, CHUNKS, width).swapaxes(0, 1).reshape(rows, width)


def shifted(array, axis, move):
    count = lax.axis_size(axis)
    return lax.ppermute(array, axis, [(i, move(i)) for i in range(count)])


def across(array):
    return shifted(array, "tp", lambda i: i ^ 1)


def along_x(array, step):
    return shifted(array, "tp", lambda i: (i + 2 * step) % 8)


def token_halo(top, end):
    rows, width = end.shape
    count = lax.axis_size("sp")
    owners = lax.axis_size("tp")
    ends = jnp.concatenate([end[rows - 9 : rows - 8], end[rows - 1 :], top[:1], top[:1]], axis=0)
    copies = jnp.broadcast_to(ends[None], (owners, *ends.shape))
    every = lax.all_to_all(copies, "tp", 0, 0, tiled=True)
    before = lax.ppermute(every[:, :2], "sp", [(i, i + 1) for i in range(count - 1)])
    after = lax.ppermute(every[:, 2:], "sp", [(i + 1, i) for i in range(count - 1)])
    rest = jnp.zeros((owners, HALO - 4, width), end.dtype)
    return jnp.concatenate([before, after, rest], axis=1)


def gathered_stream(top, end):
    left_top = along_x(top, 1)
    right_end = along_x(end, -1)
    left_end = along_x(end, 1)
    right_top = along_x(top, -1)
    far_top = along_x(left_top, 1)
    far_end = along_x(right_end, -1)
    same = (top, end, left_top, left_end, right_top, right_end, far_top, far_end)
    return same + tuple(across(part) for part in same)


OFFSETS = (0, -1, 1, 2)


def block_of(rank, dx, flip):
    core = rank % 2
    return 2 * ((rank // 2 + dx + 4) % 4) + (1 - core if flip else core)


DEPTH = 2


def weight_copies(weight, which, rank, offsets, target, sems):
    size = target.shape[1]
    copies = []
    for n, (dx, flip) in enumerate(offsets):
        at = pl.multiple_of(block_of(rank, dx, flip) * size, size)
        copies.append(
            pltpu.make_async_copy(
                weight.at[which, pl.ds(at, size), :], target.at[n], sems.at[n]
            )
        )
    for copy in copies[:DEPTH]:
        copy.start()
    return copies


def arrived(copies, n):
    copies[n].wait()
    if n + DEPTH < len(copies):
        copies[n + DEPTH].start()


def project_body(which, layer, wide, rank, gain, *refs):
    pieces, refs = refs[:16], refs[16:]
    if wide:
        halo, refs = refs[0], refs[1:]
    weight, out, weight_in, total, squares, sems = refs
    offsets = [(dx, flip) for flip in (0, 1) for dx in OFFSETS]
    copies = weight_copies(weight, which, rank[0], offsets, weight_in, sems)
    width = weight_in.shape[2]

    def scaled(k):
        block = block_of(rank[0], *offsets[k])
        scale = gain[layer : layer + 1, pl.ds(pl.multiple_of(block * width, width), width)]
        parts = [pieces[2 * k][...], pieces[2 * k + 1][...]]
        if wide:
            parts.append(halo[block])
        rows, lanes = [], []
        for part in parts:
            raw = part.astype(F32)
            rows.append((raw * scale).astype(BF16))
            power = raw * raw
            lanes.append(sum(power[:, 128 * q : 128 * (q + 1)] for q in range(width // 128)))
        lanes = jnp.concatenate(lanes, axis=0)
        if k == 0:
            squares[...] = lanes
        else:
            squares[...] += lanes
        return jnp.concatenate(rows, axis=0)

    following = scaled(0)
    for k in range(len(offsets)):
        arrived(copies, k)
        rows = following
        term = jnp.dot(rows, weight_in[k], preferred_element_type=F32)
        if k == 0:
            total[...] = term
        else:
            total[...] += term
        if k + 1 < len(offsets):
            following = scaled(k + 1)
    mean = jnp.sum(squares[...], axis=1, keepdims=True) / (width * len(offsets))
    out[...] = (total[...] * lax.rsqrt(mean + NORM_EPS)).astype(BF16)


def in_smem():
    return pl.BlockSpec(memory_space=pltpu.SMEM)


def in_vmem():
    return pl.BlockSpec(memory_space=pltpu.VMEM)


def in_hbm():
    return pl.BlockSpec(memory_space=pltpu.HBM)


def product_cost(rows, width, count):
    return pl.CostEstimate(
        flops=2 * count * rows * width * width,
        bytes_accessed=2 * count * width * width,
        transcendentals=0,
    )


def projected(rank, pieces, halo, norm_gain, layer, weights, which):
    half, width = pieces[0].shape
    count = norm_gain.shape[1] // width
    wide = halo is not None
    rows = 2 * half + (HALO if wide else 0)
    extra = [halo] if wide else []
    return pl.pallas_call(
        lambda *refs: project_body(which, layer, wide, *refs),
        out_shape=jax.ShapeDtypeStruct((rows, width), BF16),
        in_specs=[in_smem()] + [in_vmem()] * (17 + len(extra)) + [in_hbm()],
        out_specs=in_vmem(),
        scratch_shapes=[
            pltpu.VMEM((count, width, width), BF16),
            pltpu.VMEM((rows, width), F32),
            pltpu.VMEM((rows, 128), F32),
            pltpu.SemaphoreType.DMA((count,)),
        ],
        compiler_params=pltpu.CompilerParams(vmem_limit_bytes=PROJECT_LIMIT),
        cost_estimate=product_cost(rows, width, count),
    )(rank, norm_gain, *pieces, *extra, weights)


def scan_body(
    rank, mix, taps, rate, gates, local, fwd_cum, bwd_cum, coef, edge, padded, conv, pre
):
    steps = conv.shape[0] // CHUNKS
    length = conv.shape[0]
    sub = lax.broadcasted_iota(jnp.int32, (CHUNKS, 128), 0)
    rows = mix[...].astype(F32)
    halo = rows[length : length + 8]
    padded[16 : 16 + length] = rows[:length]
    padded[0:8] = jnp.where(
        sub == 0, halo[0:1], pltpu.roll(rows[length - 16 : length - 8], 1, axis=0)
    )
    padded[8:16] = jnp.where(sub == 0, halo[1:2], pltpu.roll(rows[length - 8 : length], 1, axis=0))
    padded[16 + length : 24 + length] = jnp.where(
        sub == CHUNKS - 1, halo[2:3], pltpu.roll(rows[0:8], CHUNKS - 1, axis=0)
    )
    for part in range(8):
        lo = part * (length // 8)
        hi = lo + length // 8
        conv[lo:hi] = sum(padded[lo + 8 * k : hi + 8 * k] * taps[0, k : k + 1] for k in range(4))
    lhs = conv[...].astype(BF16)
    for g in range(4):
        pre[g] = jnp.dot(lhs, gates[0, g // 2, g % 2], preferred_element_type=F32)

    def cell(i, e):
        at = pl.ds(pl.multiple_of(i * CHUNKS, CHUNKS), CHUNKS)
        recur = jax.nn.sigmoid(pre[2 * e, at, :])
        entry = jax.nn.sigmoid(pre[2 * e + 1, at, :])
        log_a = (-GATE_SCALE) * recur * rate[0, e : e + 1]
        decay = jnp.exp(log_a)
        x = 2.0 * log_a
        near = x * (1.0 + x * (0.5 + x * (1.0 / 6 + x * (1.0 / 24 + x * (1.0 / 120)))))
        room = -jnp.where(x > -0.125, near, decay * decay - 1.0)
        return at, decay, jnp.sqrt(room) * entry * conv[at, :]

    zero = jnp.zeros((CHUNKS, 128), F32)
    one = jnp.ones((CHUNKS, 128), F32)
    inner = 8

    def forward(block, carry):
        state, cum = carry
        for n in range(inner):
            at, decay, drive = cell(block * inner + n, 0)
            state = decay * state + drive
            cum = decay * cum
            local[at, :] = state
            fwd_cum[at, :] = cum
        return state, cum

    def backward(block, carry):
        state, cum = carry
        for n in range(inner):
            at, decay, drive = cell(steps - 1 - (block * inner + n), 1)
            state = decay * state + drive
            cum = decay * cum
            local[at, :] += state
            bwd_cum[at, :] = cum
        return state, cum

    state_f, cum_f = lax.fori_loop(0, steps // inner, forward, (zero, one))
    state_b, cum_b = lax.fori_loop(0, steps // inner, backward, (zero, one))
    alpha = jnp.zeros((1, 128), F32)
    beta = jnp.ones((1, 128), F32)
    for s in range(CHUNKS):
        coef[0, s : s + 1] = alpha
        coef[1, s : s + 1] = beta
        alpha = state_f[s : s + 1] + cum_f[s : s + 1] * alpha
        beta = cum_f[s : s + 1] * beta
    sums_f = (beta, alpha)
    alpha = jnp.zeros((1, 128), F32)
    beta = jnp.ones((1, 128), F32)
    for s in reversed(range(CHUNKS)):
        coef[2, s : s + 1] = alpha
        coef[3, s : s + 1] = beta
        alpha = state_b[s : s + 1] + cum_b[s : s + 1] * alpha
        beta = cum_b[s : s + 1] * beta
    edge[...] = jnp.broadcast_to(
        jnp.concatenate([*sums_f, beta, alpha], axis=0)[None], edge.shape
    )


def scanned(rank, mix, conv_taps, forget_rate, block_gates, layer, copies):
    deep, width = mix.shape
    length = deep - HALO
    blocks = width // 128
    column = lambda b, rank: (0, b)
    owned = lambda b, rank: (layer, 0, rank[0] * blocks + b)
    return pl.pallas_call(
        scan_body,
        grid_spec=pltpu.PrefetchScalarGridSpec(
            num_scalar_prefetch=1,
            grid=(blocks,),
            in_specs=[
                pl.BlockSpec((deep, 128), column),
                pl.BlockSpec((1, 4, 128), owned),
                pl.BlockSpec((1, 2, 128), owned),
                pl.BlockSpec((1, 2, 2, 128, 128), lambda b, rank: (layer, 0, 0, b, 0)),
            ],
            out_specs=[
                pl.BlockSpec((length, 128), column),
                pl.BlockSpec((length, 128), column),
                pl.BlockSpec((length, 128), column),
                pl.BlockSpec((4, CHUNKS, 128), lambda b, rank: (0, 0, b)),
                pl.BlockSpec((copies, 4, 128), lambda b, rank: (0, 0, b)),
            ],
            scratch_shapes=[
                pltpu.VMEM((length + 24, 128), F32),
                pltpu.VMEM((length, 128), F32),
                pltpu.VMEM((4, length, 128), F32),
            ],
        ),
        out_shape=[
            jax.ShapeDtypeStruct((length, width), F32),
            jax.ShapeDtypeStruct((length, width), F32),
            jax.ShapeDtypeStruct((length, width), F32),
            jax.ShapeDtypeStruct((4, CHUNKS, width), F32),
            jax.ShapeDtypeStruct((copies, 4, width), F32),
        ],
        compiler_params=pltpu.CompilerParams(vmem_limit_bytes=SCAN_LIMIT),
        cost_estimate=pl.CostEstimate(
            flops=10_000_000_000, bytes_accessed=4_000_000, transcendentals=4_000_000
        ),
        name="scan",
    )(rank, mix, conv_taps, forget_rate, block_gates)


LEAVE = (2, 1, -1, 0)


def features(mixed, weight):
    return lax.dot_general(
        mixed, weight, (((1,), (1,)), ((), ())), preferred_element_type=F32
    ).astype(BF16)


def give_body(
    which, rank, place, edges, local, fwd_cum, bwd_cum, coef, gate, weight,
    mixed, far, rest, weight_in, sems,
):
    copies = weight_copies(weight, which, rank[0], [(dx, 1) for dx in LEAVE], weight_in, sems)
    mine = place[0]
    count, _, width = edges.shape
    enter_f = jnp.zeros((1, width), F32)
    enter_b = jnp.zeros((1, width), F32)
    for r in range(count):
        enter_f = jnp.where(r < mine, edges[r, 1:2] + edges[r, 0:1] * enter_f, enter_f)
        q = count - 1 - r
        enter_b = jnp.where(q > mine, edges[q, 3:4] + edges[q, 2:3] * enter_b, enter_b)
    from_f = coef[0] + coef[1] * enter_f
    from_b = coef[2] + coef[3] * enter_b
    group = 64
    for c in range(width // 128):
        col = slice(128 * c, 128 * (c + 1))
        tiled_f = jnp.concatenate([from_f[:, col]] * (group // CHUNKS), axis=0)
        tiled_b = jnp.concatenate([from_b[:, col]] * (group // CHUNKS), axis=0)

        def part(n, carry, col=col, tiled_f=tiled_f, tiled_b=tiled_b):
            at = pl.ds(pl.multiple_of(n * group, group), group)
            both = local[at, col] + fwd_cum[at, col] * tiled_f + bwd_cum[at, col] * tiled_b
            z = gate[at, col].astype(F32)
            mixed[at, col] = (both * (z * jax.nn.sigmoid(z))).astype(BF16)
            return carry

        lax.fori_loop(0, local.shape[0] // group, part, 0)
    for n in range(len(copies)):
        arrived(copies, n)
        value = features(mixed[...], weight_in[n])
        if n == 0:
            far[...] = value
        else:
            rest[n - 1] = value


def given(rank, place, edges, local, fwd_cum, bwd_cum, coef, gate, weights, which):
    length, width = local.shape
    return pl.pallas_call(
        lambda *refs: give_body(which, *refs),
        in_specs=[in_smem(), in_smem()] + [in_vmem()] * 6 + [in_hbm()],
        out_specs=[in_vmem()] * 3,
        out_shape=[
            jax.ShapeDtypeStruct((length, width), BF16),
            jax.ShapeDtypeStruct((length, width), BF16),
            jax.ShapeDtypeStruct((3, length, width), BF16),
        ],
        scratch_shapes=[
            pltpu.VMEM((4, width, width), BF16),
            pltpu.SemaphoreType.DMA((4,)),
        ],
        compiler_params=pltpu.CompilerParams(vmem_limit_bytes=GIVE_LIMIT),
        cost_estimate=product_cost(length, width, 4),
        name="given",
    )(rank, place, edges, local, fwd_cum, bwd_cum, coef, gate, weights)


def keep_body(which, rank, mixed, weight, out, weight_in, sems):
    copies = weight_copies(weight, which, rank[0], [(dx, 0) for dx in LEAVE], weight_in, sems)
    for n in range(len(copies)):
        arrived(copies, n)
        out[n] = features(mixed[...], weight_in[n])


def kept(rank, mixed, weights, which):
    length, width = mixed.shape
    return pl.pallas_call(
        lambda *refs: keep_body(which, *refs),
        in_specs=[in_smem(), in_vmem(), in_hbm()],
        out_specs=in_vmem(),
        out_shape=jax.ShapeDtypeStruct((4, length, width), BF16),
        scratch_shapes=[
            pltpu.VMEM((4, width, width), BF16),
            pltpu.SemaphoreType.DMA((4,)),
        ],
        compiler_params=pltpu.CompilerParams(vmem_limit_bytes=KEEP_LIMIT),
        cost_estimate=product_cost(length, width, 4),
        name="kept",
    )(rank, mixed, weights)


def per_device(
    stream_in, norm_gain, value_proj, gate_proj, out_proj, conv_taps, block_gates, forget_rate
):
    rank = lax.axis_index("tp").reshape(1)
    place = lax.axis_index("sp").reshape(1)
    length, _ = stream_in.shape
    half = length // 2
    stream = to_tiles(stream_in)
    top, end = stream[:half], stream[half:]
    weights = []
    for layer in range(value_proj.shape[0]):
        held = jnp.stack([value_proj[layer], gate_proj[layer], out_proj[layer]])
        weights.append(lax.all_gather(held, "sp", axis=1, tiled=True))
    for layer in range(value_proj.shape[0]):
        full = weights[layer]
        pieces = gathered_stream(top, end)
        halo = token_halo(top, end)
        mix_in = projected(rank, pieces, halo, norm_gain, layer, full, 0)
        local, fwd_cum, bwd_cum, coef, edge = scanned(
            rank, mix_in, conv_taps, forget_rate, block_gates, layer, lax.axis_size("sp")
        )
        edges = lax.all_to_all(edge, "sp", 0, 0, tiled=True)
        gate_z = projected(rank, pieces, None, norm_gain, layer, full, 1)
        mixed, far_give, rest_give = given(
            rank, place, edges, local, fwd_cum, bwd_cum, coef, gate_z, full, 2
        )
        far_away = across(far_give).astype(F32)
        rest_away = across(rest_give).astype(F32)
        keep = kept(rank, mixed, full, 2).astype(F32)
        far = (keep[0] + far_away).astype(BF16)
        up = keep[1] + rest_away[0]
        down = keep[2] + rest_away[1]
        own = keep[3] + rest_away[2]
        relay_top = along_x(far[:half], 1)
        relay_end = along_x(far[half:], -1)
        up_end = along_x(up[half:].astype(BF16), 1)
        down_top = along_x(down[:half].astype(BF16), -1)
        up_top = along_x((up[:half] + relay_top.astype(F32)).astype(BF16), 1)
        down_end = along_x((down[half:] + relay_end.astype(F32)).astype(BF16), -1)
        top = top.astype(F32) + own[:half] + up_top.astype(F32) + down_top.astype(F32)
        end = end.astype(F32) + own[half:] + up_end.astype(F32) + down_end.astype(F32)
        top, end = top.astype(BF16), end.astype(BF16)
    return to_tokens(jnp.concatenate([top, end], axis=0))


def solution(mesh):
    placed = (
        P("sp", "tp"),
        P(),
        P(None, "sp", "tp"),
        P(None, "sp", "tp"),
        P(None, "sp", "tp"),
        P(),
        P(None, None, None, "tp", None),
        P(),
    )
    return jax.shard_map(
        per_device, mesh=mesh, in_specs=placed, out_specs=P("sp", "tp"), check_vma=False
    )
```

```python
import jax
import jax.numpy as jnp
from jax import lax
from jax.experimental import pallas as pl
from jax.experimental.pallas import tpu as pltpu
from jax.sharding import PartitionSpec as P


GATE_SCALE = 8.0
NORM_EPS = 1e-06
F32 = jnp.float32
BF16 = jnp.bfloat16


CHUNKS = 8
SCAN_LIMIT = 24 * 2**20
VALUE_LIMIT = 54 * 2**20
GATE_LIMIT = 54 * 2**20
GIVE_LIMIT = 12 * 2**20
KEEP_LIMIT = 8 * 2**20
HALO = 16


def to_tiles(array):
    rows, width = array.shape
    return array.reshape(CHUNKS, rows // CHUNKS, width).swapaxes(0, 1).reshape(rows, width)


def to_tokens(array):
    rows, width = array.shape
    return array.reshape(rows // CHUNKS, CHUNKS, width).swapaxes(0, 1).reshape(rows, width)


def shifted(array, axis, move):
    count = lax.axis_size(axis)
    return lax.ppermute(array, axis, [(i, move(i)) for i in range(count)])


def across(array):
    return shifted(array, "tp", lambda i: i ^ 1)


def along_x(array, step):
    return shifted(array, "tp", lambda i: (i + 2 * step) % 8)


def token_halo(top, end):
    rows, width = end.shape
    count = lax.axis_size("sp")
    owners = lax.axis_size("tp")
    ends = jnp.concatenate([end[rows - 9 : rows - 8], end[rows - 1 :], top[:1], top[:1]], axis=0)
    copies = jnp.broadcast_to(ends[None], (owners, *ends.shape))
    every = lax.all_to_all(copies, "tp", 0, 0, tiled=True)
    before = lax.ppermute(every[:, :2], "sp", [(i, i + 1) for i in range(count - 1)])
    after = lax.ppermute(every[:, 2:], "sp", [(i + 1, i) for i in range(count - 1)])
    rest = jnp.zeros((owners, HALO - 4, width), end.dtype)
    return jnp.concatenate([before, after, rest], axis=1)


def gathered_stream(top, end):
    left_top = along_x(top, 1)
    right_end = along_x(end, -1)
    left_end = along_x(end, 1)
    right_top = along_x(top, -1)
    far_top = along_x(left_top, 1)
    far_end = along_x(right_end, -1)
    same = (top, end, left_top, left_end, right_top, right_end, far_top, far_end)
    return same + tuple(across(part) for part in same)


def block_of(rank, dx, flip):
    core = rank % 2
    return 2 * ((rank // 2 + dx + 4) % 4) + (1 - core if flip else core)


SHIFTS = (0, -1, 1, 2)


def along_plane(array, axis, step):
    dz, dy = (step, 0) if axis == "z" else (0, step)
    pairs = [
        (4 * z + y, 4 * ((z + dz) % 4) + (y + dy) % 4) for z in range(4) for y in range(4)
    ]
    return lax.ppermute(array, "sp", pairs)


def around(array, axis):
    half = array.shape[0] // 2
    before = along_plane(array, axis, 1)
    after = along_plane(array, axis, -1)
    return (
        before,
        after,
        along_plane(before[:half], axis, 1),
        along_plane(after[half:], axis, -1),
    )


def gathered_pieces(weights):
    half = weights[0].shape[0] // 2
    pieces = []
    for at, (first, second) in ((0, "yz"), (half, "zy")):
        own = jnp.concatenate([w[at : at + half] for w in weights], axis=0)
        bundle = jnp.concatenate((own,) + around(own, first), axis=0)
        pieces += [bundle, *around(bundle, second)]
    return tuple(pieces)


def block_copies(weight, which, rank, offsets, target, sems):
    size = target.shape[1]
    copies = []
    for n, (dx, flip) in enumerate(offsets):
        at = pl.multiple_of(block_of(rank, dx, flip) * size, size)
        copies.append(
            pltpu.make_async_copy(
                weight.at[which, pl.ds(at, size), :], target.at[n], sems.at[n]
            )
        )
    return copies


def weight_copies(sources, which, place, target, sems):
    blocks, size, _ = target.shape
    if len(sources) == 1:
        return [
            pltpu.make_async_copy(
                sources[0].at[which, pl.ds(n * size, size), :], target.at[n], sems.at[n]
            )
            for n in range(blocks)
        ]
    copies = []
    rows = size // 4
    group = sources[3].shape[0] // 2
    for half in range(2):
        own, before, after, far_top, far_end = sources[5 * half : 5 * half + 5]
        for outer in range(4):
            for inner in range(4):
                if outer < 3:
                    ref, start = (own, before, after)[outer], inner * group
                else:
                    ref, start = (far_top, far_end)[inner // 2], (inner % 2) * group
                dz, dy = (outer, inner) if half == 0 else (inner, outer)
                z = (place // 4 + 4 + SHIFTS[dz]) % 4
                y = (place % 4 + 4 + SHIFTS[dy]) % 4
                at = pl.multiple_of((y % 2) * (2 * rows) + half * rows, rows)
                copies.append(
                    pltpu.make_async_copy(
                        ref.at[pl.ds(start + which * rows, rows), :],
                        target.at[2 * z + y // 2, pl.ds(at, rows), :],
                        sems.at[len(copies)],
                    )
                )
    return copies


ARRIVE = [(dx, flip) for flip in (0, 1) for dx in (0, -1, 1, 2)]
LEAVE = [(dx, flip) for flip in (1, 0) for dx in (2, 1, -1, 0)]


def contracted(rows, weight, total):
    total[...] = jnp.zeros_like(total)

    def step(k, carry):
        total[...] += jnp.dot(rows[k], weight[k], preferred_element_type=F32)
        return carry

    lax.fori_loop(0, rows.shape[0], step, 0)


def row_scale(squares, width):
    return lax.rsqrt(jnp.sum(squares[...], axis=1, keepdims=True) / width + NORM_EPS)


def scaled_rows(layer, rank, gain, pieces, halo, rows, squares):
    half, width = pieces[0].shape
    step = 64
    for k, (dx, flip) in enumerate(ARRIVE):
        block = block_of(rank, dx, flip)
        scale = gain[layer : layer + 1, pl.ds(pl.multiple_of(block * width, width), width)]

        def put(raw, at, k=k, block=block, scale=scale):
            raw = raw.astype(F32)
            rows[block, at, :] = (raw * scale).astype(BF16)
            power = raw * raw
            lanes = sum(power[:, 128 * q : 128 * (q + 1)] for q in range(width // 128))
            if k == 0:
                squares[at, :] = lanes
            else:
                squares[at, :] += lanes

        def chunk(n, carry, k=k, put=put):
            at = pl.multiple_of(n * step, step)
            for side in range(2):
                put(pieces[2 * k + side][pl.ds(at, step), :], pl.ds(at + side * half, step))
            return carry

        lax.fori_loop(0, half // step, chunk, 0)
        if halo is not None:
            put(halo[block], pl.ds(2 * half, HALO))


def value_body(layer, rank, place, gain, halo, *refs):
    pieces, sources = refs[:16], refs[16:-6]
    out, rows, squares, value_in, total, sems = refs[-6:]
    values = weight_copies(sources, 0, place[0], value_in, sems)
    for copy in values:
        copy.start()
    scaled_rows(layer, rank[0], gain, pieces, halo, rows, squares)
    for copy in values:
        copy.wait()
    contracted(rows, value_in, total)
    out[...] = (total[...] * row_scale(squares, out.shape[1] * len(ARRIVE))).astype(BF16)


def gate_body(layer, which, rank, place, gain, *refs):
    pieces, sources, full = refs[:16], refs[16:-9], refs[-9]
    out, out_in, rows, squares, gate_in, total, sems, out_sems = refs[-8:]
    gates = weight_copies(sources, 1, place[0], gate_in, sems)
    others = block_copies(full, which, rank[0], LEAVE, out_in, out_sems)
    for copy in gates:
        copy.start()
    scaled_rows(layer, rank[0], gain, pieces, None, rows, squares)
    for copy in gates:
        copy.wait()
    for copy in others:
        copy.start()
    contracted(rows, gate_in, total)
    out[...] = (total[...] * row_scale(squares, out.shape[1] * len(ARRIVE))).astype(BF16)
    for copy in others:
        copy.wait()


def in_smem():
    return pl.BlockSpec(memory_space=pltpu.SMEM)


def in_vmem():
    return pl.BlockSpec(memory_space=pltpu.VMEM)


def in_hbm():
    return pl.BlockSpec(memory_space=pltpu.HBM)


def product_cost(rows, width, count):
    return pl.CostEstimate(
        flops=2 * count * rows * width * width,
        bytes_accessed=2 * count * width * width,
        transcendentals=0,
    )


def value_rows(rank, place, pieces, halo, norm_gain, layer, sources):
    half, width = pieces[0].shape
    count = norm_gain.shape[1] // width
    deep = 2 * half + HALO
    return pl.pallas_call(
        lambda *refs: value_body(layer, *refs),
        out_shape=jax.ShapeDtypeStruct((deep, width), BF16),
        in_specs=[in_smem()] * 2 + [in_vmem()] * 18 + [in_hbm()] * len(sources),
        out_specs=in_vmem(),
        scratch_shapes=[
            pltpu.VMEM((count, deep, width), BF16),
            pltpu.VMEM((deep, 128), F32),
            pltpu.VMEM((count, width, width), BF16),
            pltpu.VMEM((deep, width), F32),
            pltpu.SemaphoreType.DMA((32,)),
        ],
        compiler_params=pltpu.CompilerParams(vmem_limit_bytes=VALUE_LIMIT),
        cost_estimate=product_cost(deep, width, count),
        name="value_rows",
    )(rank, place, norm_gain, halo, *pieces, *sources)


def gate_rows(rank, place, pieces, norm_gain, layer, sources, full, which):
    half, width = pieces[0].shape
    count = norm_gain.shape[1] // width
    length = 2 * half
    return pl.pallas_call(
        lambda *refs: gate_body(layer, which, *refs),
        out_shape=[
            jax.ShapeDtypeStruct((length, width), BF16),
            jax.ShapeDtypeStruct((count, width, width), BF16),
        ],
        in_specs=[in_smem()] * 2 + [in_vmem()] * 17 + [in_hbm()] * (len(sources) + 1),
        out_specs=[in_vmem()] * 2,
        scratch_shapes=[
            pltpu.VMEM((count, length, width), BF16),
            pltpu.VMEM((length, 128), F32),
            pltpu.VMEM((count, width, width), BF16),
            pltpu.VMEM((length, width), F32),
            pltpu.SemaphoreType.DMA((32,)),
            pltpu.SemaphoreType.DMA((count,)),
        ],
        compiler_params=pltpu.CompilerParams(vmem_limit_bytes=GATE_LIMIT),
        cost_estimate=product_cost(length, width, count),
        name="gate_rows",
    )(rank, place, norm_gain, *pieces, *sources, full)


def scan_body(
    rank, mix, taps, rate, gates, local, fwd_cum, bwd_cum, coef, edge, padded, conv, pre
):
    steps = conv.shape[0] // CHUNKS
    length = conv.shape[0]
    sub = lax.broadcasted_iota(jnp.int32, (CHUNKS, 128), 0)
    rows = mix[...].astype(F32)
    halo = rows[length : length + 8]
    padded[16 : 16 + length] = rows[:length]
    padded[0:8] = jnp.where(
        sub == 0, halo[0:1], pltpu.roll(rows[length - 16 : length - 8], 1, axis=0)
    )
    padded[8:16] = jnp.where(sub == 0, halo[1:2], pltpu.roll(rows[length - 8 : length], 1, axis=0))
    padded[16 + length : 24 + length] = jnp.where(
        sub == CHUNKS - 1, halo[2:3], pltpu.roll(rows[0:8], CHUNKS - 1, axis=0)
    )
    for part in range(8):
        lo = part * (length // 8)
        hi = lo + length // 8
        conv[lo:hi] = sum(padded[lo + 8 * k : hi + 8 * k] * taps[0, k : k + 1] for k in range(4))
    lhs = conv[...].astype(BF16)
    for g in range(4):
        pre[g] = jnp.dot(lhs, gates[0, g // 2, g % 2], preferred_element_type=F32)

    def cell(i, e):
        at = pl.ds(pl.multiple_of(i * CHUNKS, CHUNKS), CHUNKS)
        recur = jax.nn.sigmoid(pre[2 * e, at, :])
        entry = jax.nn.sigmoid(pre[2 * e + 1, at, :])
        log_a = (-GATE_SCALE) * recur * rate[0, e : e + 1]
        decay = jnp.exp(log_a)
        x = 2.0 * log_a
        near = x * (1.0 + x * (0.5 + x * (1.0 / 6 + x * (1.0 / 24 + x * (1.0 / 120)))))
        room = -jnp.where(x > -0.125, near, decay * decay - 1.0)
        return at, decay, jnp.sqrt(room) * entry * conv[at, :]

    zero = jnp.zeros((CHUNKS, 128), F32)
    one = jnp.ones((CHUNKS, 128), F32)
    inner = 8

    def forward(block, carry):
        state, cum = carry
        for n in range(inner):
            at, decay, drive = cell(block * inner + n, 0)
            state = decay * state + drive
            cum = decay * cum
            local[at, :] = state
            fwd_cum[at, :] = cum
        return state, cum

    def backward(block, carry):
        state, cum = carry
        for n in range(inner):
            at, decay, drive = cell(steps - 1 - (block * inner + n), 1)
            state = decay * state + drive
            cum = decay * cum
            local[at, :] += state
            bwd_cum[at, :] = cum
        return state, cum

    state_f, cum_f = lax.fori_loop(0, steps // inner, forward, (zero, one))
    state_b, cum_b = lax.fori_loop(0, steps // inner, backward, (zero, one))
    alpha = jnp.zeros((1, 128), F32)
    beta = jnp.ones((1, 128), F32)
    for s in range(CHUNKS):
        coef[0, s : s + 1] = alpha
        coef[1, s : s + 1] = beta
        alpha = state_f[s : s + 1] + cum_f[s : s + 1] * alpha
        beta = cum_f[s : s + 1] * beta
    sums_f = (beta, alpha)
    alpha = jnp.zeros((1, 128), F32)
    beta = jnp.ones((1, 128), F32)
    for s in reversed(range(CHUNKS)):
        coef[2, s : s + 1] = alpha
        coef[3, s : s + 1] = beta
        alpha = state_b[s : s + 1] + cum_b[s : s + 1] * alpha
        beta = cum_b[s : s + 1] * beta
    edge[...] = jnp.broadcast_to(
        jnp.concatenate([*sums_f, beta, alpha], axis=0)[None], edge.shape
    )


def scanned(rank, mix, conv_taps, forget_rate, block_gates, layer, copies):
    deep, width = mix.shape
    length = deep - HALO
    blocks = width // 128
    column = lambda b, rank: (0, b)
    owned = lambda b, rank: (layer, 0, rank[0] * blocks + b)
    return pl.pallas_call(
        scan_body,
        grid_spec=pltpu.PrefetchScalarGridSpec(
            num_scalar_prefetch=1,
            grid=(blocks,),
            in_specs=[
                pl.BlockSpec((deep, 128), column),
                pl.BlockSpec((1, 4, 128), owned),
                pl.BlockSpec((1, 2, 128), owned),
                pl.BlockSpec((1, 2, 2, 128, 128), lambda b, rank: (layer, 0, 0, b, 0)),
            ],
            out_specs=[
                pl.BlockSpec((length, 128), column),
                pl.BlockSpec((length, 128), column),
                pl.BlockSpec((length, 128), column),
                pl.BlockSpec((4, CHUNKS, 128), lambda b, rank: (0, 0, b)),
                pl.BlockSpec((copies, 4, 128), lambda b, rank: (0, 0, b)),
            ],
            scratch_shapes=[
                pltpu.VMEM((length + 24, 128), F32),
                pltpu.VMEM((length, 128), F32),
                pltpu.VMEM((4, length, 128), F32),
            ],
        ),
        out_shape=[
            jax.ShapeDtypeStruct((length, width), F32),
            jax.ShapeDtypeStruct((length, width), F32),
            jax.ShapeDtypeStruct((length, width), F32),
            jax.ShapeDtypeStruct((4, CHUNKS, width), F32),
            jax.ShapeDtypeStruct((copies, 4, width), F32),
        ],
        compiler_params=pltpu.CompilerParams(vmem_limit_bytes=SCAN_LIMIT),
        cost_estimate=pl.CostEstimate(
            flops=10_000_000_000, bytes_accessed=4_000_000, transcendentals=4_000_000
        ),
        name="scan",
    )(rank, mix, conv_taps, forget_rate, block_gates)


def features(mixed, weight):
    return lax.dot_general(
        mixed, weight, (((1,), (1,)), ((), ())), preferred_element_type=F32
    ).astype(BF16)


def give_body(
    place, edges, local, fwd_cum, bwd_cum, coef, gate, weight, mixed, far, rest
):
    mine = place[0]
    count, _, width = edges.shape
    enter_f = jnp.zeros((1, width), F32)
    enter_b = jnp.zeros((1, width), F32)
    for r in range(count):
        enter_f = jnp.where(r < mine, edges[r, 1:2] + edges[r, 0:1] * enter_f, enter_f)
        q = count - 1 - r
        enter_b = jnp.where(q > mine, edges[q, 3:4] + edges[q, 2:3] * enter_b, enter_b)
    from_f = coef[0] + coef[1] * enter_f
    from_b = coef[2] + coef[3] * enter_b
    group = 64
    for c in range(width // 128):
        col = slice(128 * c, 128 * (c + 1))
        tiled_f = jnp.concatenate([from_f[:, col]] * (group // CHUNKS), axis=0)
        tiled_b = jnp.concatenate([from_b[:, col]] * (group // CHUNKS), axis=0)

        def part(n, carry, col=col, tiled_f=tiled_f, tiled_b=tiled_b):
            at = pl.ds(pl.multiple_of(n * group, group), group)
            both = local[at, col] + fwd_cum[at, col] * tiled_f + bwd_cum[at, col] * tiled_b
            z = gate[at, col].astype(F32)
            mixed[at, col] = (both * (z * jax.nn.sigmoid(z))).astype(BF16)
            return carry

        lax.fori_loop(0, local.shape[0] // group, part, 0)
    far[...] = features(mixed[...], weight[0])

    def step(n, carry):
        rest[n] = features(mixed[...], weight[n + 1])
        return carry

    lax.fori_loop(0, 3, step, 0)


def given(place, edges, local, fwd_cum, bwd_cum, coef, gate, weight):
    length, width = local.shape
    return pl.pallas_call(
        give_body,
        in_specs=[in_smem()] + [in_vmem()] * 7,
        out_specs=[in_vmem()] * 3,
        out_shape=[
            jax.ShapeDtypeStruct((length, width), BF16),
            jax.ShapeDtypeStruct((length, width), BF16),
            jax.ShapeDtypeStruct((3, length, width), BF16),
        ],
        compiler_params=pltpu.CompilerParams(vmem_limit_bytes=GIVE_LIMIT),
        cost_estimate=product_cost(length, width, 4),
        name="given",
    )(place, edges, local, fwd_cum, bwd_cum, coef, gate, weight)


def keep_body(mixed, weight, out):
    def step(n, carry):
        out[n] = features(mixed[...], weight[n + 4])
        return carry

    lax.fori_loop(0, 4, step, 0)


def kept(mixed, weight):
    length, width = mixed.shape
    return pl.pallas_call(
        keep_body,
        in_specs=[in_vmem()] * 2,
        out_specs=in_vmem(),
        out_shape=jax.ShapeDtypeStruct((4, length, width), BF16),
        compiler_params=pltpu.CompilerParams(vmem_limit_bytes=KEEP_LIMIT),
        cost_estimate=product_cost(length, width, 4),
        name="kept",
    )(mixed, weight)


def per_device(
    stream_in, norm_gain, value_proj, gate_proj, out_proj, conv_taps, block_gates, forget_rate
):
    rank = lax.axis_index("tp").reshape(1)
    place = lax.axis_index("sp").reshape(1)
    length, _ = stream_in.shape
    half = length // 2
    stream = to_tiles(stream_in)
    top, end = stream[:half], stream[half:]
    pieces_0 = gathered_pieces([value_proj[0], gate_proj[0]])
    outs_0 = lax.all_gather(out_proj[:1], "sp", axis=1, tiled=True)
    held = jnp.stack([value_proj[1], gate_proj[1], out_proj[1]])
    full_1 = lax.all_gather(held, "sp", axis=1, tiled=True)
    weights = [(pieces_0, outs_0, 0), ((full_1,), full_1, 2)]
    for layer in range(value_proj.shape[0]):
        sources, full, which = weights[layer]
        pieces = gathered_stream(top, end)
        halo = token_halo(top, end)
        mix_in = value_rows(rank, place, pieces, halo, norm_gain, layer, sources)
        local, fwd_cum, bwd_cum, coef, edge = scanned(
            rank, mix_in, conv_taps, forget_rate, block_gates, layer, lax.axis_size("sp")
        )
        edges = lax.all_to_all(edge, "sp", 0, 0, tiled=True)
        gate_z, out_weight = gate_rows(rank, place, pieces, norm_gain, layer, sources, full, which)
        mixed, far_give, rest_give = given(
            place, edges, local, fwd_cum, bwd_cum, coef, gate_z, out_weight
        )
        far_away = across(far_give).astype(F32)
        rest_away = across(rest_give).astype(F32)
        keep = kept(mixed, out_weight).astype(F32)
        far = (keep[0] + far_away).astype(BF16)
        up = keep[1] + rest_away[0]
        down = keep[2] + rest_away[1]
        own = keep[3] + rest_away[2]
        relay_top = along_x(far[:half], 1)
        relay_end = along_x(far[half:], -1)
        up_end = along_x(up[half:].astype(BF16), 1)
        down_top = along_x(down[:half].astype(BF16), -1)
        up_top = along_x((up[:half] + relay_top.astype(F32)).astype(BF16), 1)
        down_end = along_x((down[half:] + relay_end.astype(F32)).astype(BF16), -1)
        top = top.astype(F32) + own[:half] + up_top.astype(F32) + down_top.astype(F32)
        end = end.astype(F32) + own[half:] + up_end.astype(F32) + down_end.astype(F32)
        top, end = top.astype(BF16), end.astype(BF16)
    return to_tokens(jnp.concatenate([top, end], axis=0))


def solution(mesh):
    placed = (
        P("sp", "tp"),
        P(),
        P(None, "sp", "tp"),
        P(None, "sp", "tp"),
        P(None, "sp", "tp"),
        P(),
        P(None, None, None, "tp", None),
        P(),
    )
    return jax.shard_map(
        per_device, mesh=mesh, in_specs=placed, out_specs=P("sp", "tp"), check_vma=False
    )
```

```python
import jax
import jax.numpy as jnp
from jax import lax
from jax.experimental import pallas as pl
from jax.experimental.pallas import tpu as pltpu
from jax.sharding import PartitionSpec as P


GATE_SCALE = 8.0
NORM_EPS = 1e-06
F32 = jnp.float32
BF16 = jnp.bfloat16


CHUNKS = 8
SCAN_LIMIT = 24 * 2**20
VALUE_LIMIT = 54 * 2**20
GATE_LIMIT = 54 * 2**20
GIVE_LIMIT = 12 * 2**20
KEEP_LIMIT = 8 * 2**20
HALO = 16


def to_tiles(array):
    rows, width = array.shape
    return array.reshape(CHUNKS, rows // CHUNKS, width).swapaxes(0, 1).reshape(rows, width)


def to_tokens(array):
    rows, width = array.shape
    return array.reshape(rows // CHUNKS, CHUNKS, width).swapaxes(0, 1).reshape(rows, width)


def shifted(array, axis, move):
    count = lax.axis_size(axis)
    return lax.ppermute(array, axis, [(i, move(i)) for i in range(count)])


def across(array):
    return shifted(array, "tp", lambda i: i ^ 1)


def along_x(array, step):
    return shifted(array, "tp", lambda i: (i + 2 * step) % 8)


def token_halo(top, end):
    rows, width = end.shape
    count = lax.axis_size("sp")
    owners = lax.axis_size("tp")
    ends = jnp.concatenate([end[rows - 9 : rows - 8], end[rows - 1 :], top[:1], top[:1]], axis=0)
    copies = jnp.broadcast_to(ends[None], (owners, *ends.shape))
    every = lax.all_to_all(copies, "tp", 0, 0, tiled=True)
    before = lax.ppermute(every[:, :2], "sp", [(i, i + 1) for i in range(count - 1)])
    after = lax.ppermute(every[:, 2:], "sp", [(i + 1, i) for i in range(count - 1)])
    rest = jnp.zeros((owners, HALO - 4, width), end.dtype)
    return jnp.concatenate([before, after, rest], axis=1)


def gathered_stream(top, end):
    left_top = along_x(top, 1)
    right_end = along_x(end, -1)
    left_end = along_x(end, 1)
    right_top = along_x(top, -1)
    far_top = along_x(left_top, 1)
    far_end = along_x(right_end, -1)
    same = (top, end, left_top, left_end, right_top, right_end, far_top, far_end)
    return same + tuple(across(part) for part in same)


def block_of(rank, dx, flip):
    core = rank % 2
    return 2 * ((rank // 2 + dx + 4) % 4) + (1 - core if flip else core)


SHIFTS = (0, -1, 1, 2)


def along_plane(array, axis, step):
    dz, dy = (step, 0) if axis == "z" else (0, step)
    pairs = [
        (4 * z + y, 4 * ((z + dz) % 4) + (y + dy) % 4) for z in range(4) for y in range(4)
    ]
    return lax.ppermute(array, "sp", pairs)


def around(array, axis):
    half = array.shape[0] // 2
    before = along_plane(array, axis, 1)
    after = along_plane(array, axis, -1)
    return (
        before,
        after,
        along_plane(before[:half], axis, 1),
        along_plane(after[half:], axis, -1),
    )


def gathered_pieces(weights):
    half = weights[0].shape[0] // 2
    pieces = []
    for at, (first, second) in ((0, "yz"), (half, "zy")):
        own = jnp.concatenate([w[at : at + half] for w in weights], axis=0)
        before, after, far_top, far_end = around(own, first)
        top = jnp.concatenate([own, before], axis=0)
        end = jnp.concatenate([after, far_top, far_end], axis=0)
        top_before = along_plane(top, second, 1)
        top_after = along_plane(top, second, -1)
        end_after = along_plane(end, second, -1)
        end_before = along_plane(end, second, 1)
        pieces += [top, end, top_before, end_before, top_after, end_after]
        pieces += [along_plane(top_before, second, 1), along_plane(end_after, second, -1)]
    return tuple(pieces)


def block_copies(weight, which, rank, offsets, target, sems):
    size = target.shape[1]
    copies = []
    for n, (dx, flip) in enumerate(offsets):
        at = pl.multiple_of(block_of(rank, dx, flip) * size, size)
        copies.append(
            pltpu.make_async_copy(
                weight.at[which, pl.ds(at, size), :], target.at[n], sems.at[n]
            )
        )
    return copies


def weight_copies(sources, which, place, target, sems):
    blocks, size, _ = target.shape
    if len(sources) == 1:
        return [
            pltpu.make_async_copy(
                sources[0].at[which, pl.ds(n * size, size), :], target.at[n], sems.at[n]
            )
            for n in range(blocks)
        ]
    copies = []
    rows = size // 4
    group = sources[0].shape[0] // 2
    for half in range(2):
        for outer in range(4):
            for inner in range(4):
                ref = sources[8 * half + 2 * outer + inner // 2]
                start = (inner % 2) * group
                dz, dy = (outer, inner) if half == 0 else (inner, outer)
                z = (place // 4 + 4 + SHIFTS[dz]) % 4
                y = (place % 4 + 4 + SHIFTS[dy]) % 4
                at = pl.multiple_of((y % 2) * (2 * rows) + half * rows, rows)
                copies.append(
                    pltpu.make_async_copy(
                        ref.at[pl.ds(start + which * rows, rows), :],
                        target.at[2 * z + y // 2, pl.ds(at, rows), :],
                        sems.at[len(copies)],
                    )
                )
    return copies


ARRIVE = [(dx, flip) for flip in (0, 1) for dx in (0, -1, 1, 2)]
LEAVE = [(dx, flip) for flip in (1, 0) for dx in (2, 1, -1, 0)]


def contracted(rows, weight, total):
    total[...] = jnp.zeros_like(total)

    def step(k, carry):
        total[...] += jnp.dot(rows[k], weight[k], preferred_element_type=F32)
        return carry

    lax.fori_loop(0, rows.shape[0], step, 0)


def row_scale(squares, width):
    return lax.rsqrt(jnp.sum(squares[...], axis=1, keepdims=True) / width + NORM_EPS)


def piece_copies(rank, pieces, rows, sems):
    half = pieces[0].shape[0]
    return [
        pltpu.make_async_copy(
            pieces[2 * k + side],
            rows.at[block_of(rank, dx, flip), pl.ds(side * half, half), :],
            sems.at[2 * k + side],
        )
        for k, (dx, flip) in enumerate(ARRIVE)
        for side in range(2)
    ]


def scaled_rows(layer, rank, gain, copies, halo, rows, squares):
    width = rows.shape[2]
    half = (rows.shape[1] - (0 if halo is None else HALO)) // 2
    step = 64
    for k, (dx, flip) in enumerate(ARRIVE):
        copies[2 * k].wait()
        copies[2 * k + 1].wait()
        block = block_of(rank, dx, flip)
        scale = gain[layer : layer + 1, pl.ds(pl.multiple_of(block * width, width), width)]

        def put(raw, at, k=k, block=block, scale=scale):
            raw = raw.astype(F32)
            rows[block, at, :] = (raw * scale).astype(BF16)
            power = raw * raw
            lanes = sum(power[:, 128 * q : 128 * (q + 1)] for q in range(width // 128))
            if k == 0:
                squares[at, :] = lanes
            else:
                squares[at, :] += lanes

        def chunk(n, carry, block=block, put=put):
            for side in range(2):
                at = pl.ds(pl.multiple_of(n * step + side * half, step), step)
                put(rows[block, at, :], at)
            return carry

        lax.fori_loop(0, half // step, chunk, 0)
        if halo is not None:
            put(halo[block], pl.ds(2 * half, HALO))


def value_body(layer, rank, place, gain, halo, *refs):
    pieces, sources = refs[:16], refs[16:-7]
    out, rows, squares, value_in, total, sems, piece_sems = refs[-7:]
    values = weight_copies(sources, 0, place[0], value_in, sems)
    arriving = piece_copies(rank[0], pieces, rows, piece_sems)
    for copy in arriving + values:
        copy.start()
    scaled_rows(layer, rank[0], gain, arriving, halo, rows, squares)
    for copy in values:
        copy.wait()
    contracted(rows, value_in, total)
    out[...] = (total[...] * row_scale(squares, out.shape[1] * len(ARRIVE))).astype(BF16)


def gate_body(layer, which, rank, place, gain, *refs):
    pieces, sources, full = refs[:16], refs[16:-10], refs[-10]
    out, out_in, rows, squares, gate_in, total, sems, out_sems, piece_sems = refs[-9:]
    gates = weight_copies(sources, 1, place[0], gate_in, sems)
    others = block_copies(full, which, rank[0], LEAVE, out_in, out_sems)
    arriving = piece_copies(rank[0], pieces, rows, piece_sems)
    for copy in arriving + gates:
        copy.start()
    scaled_rows(layer, rank[0], gain, arriving, None, rows, squares)
    for copy in gates:
        copy.wait()
    for copy in others:
        copy.start()
    contracted(rows, gate_in, total)
    out[...] = (total[...] * row_scale(squares, out.shape[1] * len(ARRIVE))).astype(BF16)
    for copy in others:
        copy.wait()


def in_smem():
    return pl.BlockSpec(memory_space=pltpu.SMEM)


def in_vmem():
    return pl.BlockSpec(memory_space=pltpu.VMEM)


def in_hbm():
    return pl.BlockSpec(memory_space=pltpu.HBM)


def product_cost(rows, width, count):
    return pl.CostEstimate(
        flops=2 * count * rows * width * width,
        bytes_accessed=2 * count * width * width,
        transcendentals=0,
    )


def value_rows(rank, place, pieces, halo, norm_gain, layer, sources):
    half, width = pieces[0].shape
    count = norm_gain.shape[1] // width
    deep = 2 * half + HALO
    return pl.pallas_call(
        lambda *refs: value_body(layer, *refs),
        out_shape=jax.ShapeDtypeStruct((deep, width), BF16),
        in_specs=[in_smem()] * 2 + [in_vmem()] * 2 + [in_hbm()] * (16 + len(sources)),
        out_specs=in_vmem(),
        scratch_shapes=[
            pltpu.VMEM((count, deep, width), BF16),
            pltpu.VMEM((deep, 128), F32),
            pltpu.VMEM((count, width, width), BF16),
            pltpu.VMEM((deep, width), F32),
            pltpu.SemaphoreType.DMA((32,)),
            pltpu.SemaphoreType.DMA((16,)),
        ],
        compiler_params=pltpu.CompilerParams(vmem_limit_bytes=VALUE_LIMIT),
        cost_estimate=product_cost(deep, width, count),
        name="value_rows",
    )(rank, place, norm_gain, halo, *pieces, *sources)


def gate_rows(rank, place, pieces, norm_gain, layer, sources, full, which):
    half, width = pieces[0].shape
    count = norm_gain.shape[1] // width
    length = 2 * half
    return pl.pallas_call(
        lambda *refs: gate_body(layer, which, *refs),
        out_shape=[
            jax.ShapeDtypeStruct((length, width), BF16),
            jax.ShapeDtypeStruct((count, width, width), BF16),
        ],
        in_specs=[in_smem()] * 2 + [in_vmem()] + [in_hbm()] * (17 + len(sources)),
        out_specs=[in_vmem()] * 2,
        scratch_shapes=[
            pltpu.VMEM((count, length, width), BF16),
            pltpu.VMEM((length, 128), F32),
            pltpu.VMEM((count, width, width), BF16),
            pltpu.VMEM((length, width), F32),
            pltpu.SemaphoreType.DMA((32,)),
            pltpu.SemaphoreType.DMA((count,)),
            pltpu.SemaphoreType.DMA((16,)),
        ],
        compiler_params=pltpu.CompilerParams(vmem_limit_bytes=GATE_LIMIT),
        cost_estimate=product_cost(length, width, count),
        name="gate_rows",
    )(rank, place, norm_gain, *pieces, *sources, full)


def scan_body(
    rank, mix, taps, rate, gates, local, fwd_cum, bwd_cum, coef, edge, padded, conv, pre
):
    steps = conv.shape[0] // CHUNKS
    length = conv.shape[0]
    sub = lax.broadcasted_iota(jnp.int32, (CHUNKS, 128), 0)
    rows = mix[...].astype(F32)
    halo = rows[length : length + 8]
    padded[16 : 16 + length] = rows[:length]
    padded[0:8] = jnp.where(
        sub == 0, halo[0:1], pltpu.roll(rows[length - 16 : length - 8], 1, axis=0)
    )
    padded[8:16] = jnp.where(sub == 0, halo[1:2], pltpu.roll(rows[length - 8 : length], 1, axis=0))
    padded[16 + length : 24 + length] = jnp.where(
        sub == CHUNKS - 1, halo[2:3], pltpu.roll(rows[0:8], CHUNKS - 1, axis=0)
    )
    for part in range(8):
        lo = part * (length // 8)
        hi = lo + length // 8
        conv[lo:hi] = sum(padded[lo + 8 * k : hi + 8 * k] * taps[0, k : k + 1] for k in range(4))
    lhs = conv[...].astype(BF16)
    for g in range(4):
        pre[g] = jnp.dot(lhs, gates[0, g // 2, g % 2], preferred_element_type=F32)

    def cell(i, e):
        at = pl.ds(pl.multiple_of(i * CHUNKS, CHUNKS), CHUNKS)
        recur = jax.nn.sigmoid(pre[2 * e, at, :])
        entry = jax.nn.sigmoid(pre[2 * e + 1, at, :])
        log_a = (-GATE_SCALE) * recur * rate[0, e : e + 1]
        decay = jnp.exp(log_a)
        x = 2.0 * log_a
        near = x * (1.0 + x * (0.5 + x * (1.0 / 6 + x * (1.0 / 24 + x * (1.0 / 120)))))
        room = -jnp.where(x > -0.125, near, decay * decay - 1.0)
        return at, decay, jnp.sqrt(room) * entry * conv[at, :]

    zero = jnp.zeros((CHUNKS, 128), F32)
    one = jnp.ones((CHUNKS, 128), F32)
    inner = 8

    def forward(block, carry):
        state, cum = carry
        for n in range(inner):
            at, decay, drive = cell(block * inner + n, 0)
            state = decay * state + drive
            cum = decay * cum
            local[at, :] = state
            fwd_cum[at, :] = cum
        return state, cum

    def backward(block, carry):
        state, cum = carry
        for n in range(inner):
            at, decay, drive = cell(steps - 1 - (block * inner + n), 1)
            state = decay * state + drive
            cum = decay * cum
            local[at, :] += state
            bwd_cum[at, :] = cum
        return state, cum

    state_f, cum_f = lax.fori_loop(0, steps // inner, forward, (zero, one))
    state_b, cum_b = lax.fori_loop(0, steps // inner, backward, (zero, one))
    alpha = jnp.zeros((1, 128), F32)
    beta = jnp.ones((1, 128), F32)
    for s in range(CHUNKS):
        coef[0, s : s + 1] = alpha
        coef[1, s : s + 1] = beta
        alpha = state_f[s : s + 1] + cum_f[s : s + 1] * alpha
        beta = cum_f[s : s + 1] * beta
    sums_f = (beta, alpha)
    alpha = jnp.zeros((1, 128), F32)
    beta = jnp.ones((1, 128), F32)
    for s in reversed(range(CHUNKS)):
        coef[2, s : s + 1] = alpha
        coef[3, s : s + 1] = beta
        alpha = state_b[s : s + 1] + cum_b[s : s + 1] * alpha
        beta = cum_b[s : s + 1] * beta
    edge[...] = jnp.broadcast_to(
        jnp.concatenate([*sums_f, beta, alpha], axis=0)[None], edge.shape
    )


def scanned(rank, mix, conv_taps, forget_rate, block_gates, layer, copies):
    deep, width = mix.shape
    length = deep - HALO
    blocks = width // 128
    column = lambda b, rank: (0, b)
    owned = lambda b, rank: (layer, 0, rank[0] * blocks + b)
    return pl.pallas_call(
        scan_body,
        grid_spec=pltpu.PrefetchScalarGridSpec(
            num_scalar_prefetch=1,
            grid=(blocks,),
            in_specs=[
                pl.BlockSpec((deep, 128), column),
                pl.BlockSpec((1, 4, 128), owned),
                pl.BlockSpec((1, 2, 128), owned),
                pl.BlockSpec((1, 2, 2, 128, 128), lambda b, rank: (layer, 0, 0, b, 0)),
            ],
            out_specs=[
                pl.BlockSpec((length, 128), column),
                pl.BlockSpec((length, 128), column),
                pl.BlockSpec((length, 128), column),
                pl.BlockSpec((4, CHUNKS, 128), lambda b, rank: (0, 0, b)),
                pl.BlockSpec((copies, 4, 128), lambda b, rank: (0, 0, b)),
            ],
            scratch_shapes=[
                pltpu.VMEM((length + 24, 128), F32),
                pltpu.VMEM((length, 128), F32),
                pltpu.VMEM((4, length, 128), F32),
            ],
        ),
        out_shape=[
            jax.ShapeDtypeStruct((length, width), F32),
            jax.ShapeDtypeStruct((length, width), F32),
            jax.ShapeDtypeStruct((length, width), F32),
            jax.ShapeDtypeStruct((4, CHUNKS, width), F32),
            jax.ShapeDtypeStruct((copies, 4, width), F32),
        ],
        compiler_params=pltpu.CompilerParams(vmem_limit_bytes=SCAN_LIMIT),
        cost_estimate=pl.CostEstimate(
            flops=10_000_000_000, bytes_accessed=4_000_000, transcendentals=4_000_000
        ),
        name="scan",
    )(rank, mix, conv_taps, forget_rate, block_gates)


def features(mixed, weight):
    return lax.dot_general(
        mixed, weight, (((1,), (1,)), ((), ())), preferred_element_type=F32
    ).astype(BF16)


def give_body(
    place, edges, local, fwd_cum, bwd_cum, coef, gate, weight, mixed, far, rest
):
    mine = place[0]
    count, _, width = edges.shape
    enter_f = jnp.zeros((1, width), F32)
    enter_b = jnp.zeros((1, width), F32)
    for r in range(count):
        enter_f = jnp.where(r < mine, edges[r, 1:2] + edges[r, 0:1] * enter_f, enter_f)
        q = count - 1 - r
        enter_b = jnp.where(q > mine, edges[q, 3:4] + edges[q, 2:3] * enter_b, enter_b)
    from_f = coef[0] + coef[1] * enter_f
    from_b = coef[2] + coef[3] * enter_b
    group = 64
    for c in range(width // 128):
        col = slice(128 * c, 128 * (c + 1))
        tiled_f = jnp.concatenate([from_f[:, col]] * (group // CHUNKS), axis=0)
        tiled_b = jnp.concatenate([from_b[:, col]] * (group // CHUNKS), axis=0)

        def part(n, carry, col=col, tiled_f=tiled_f, tiled_b=tiled_b):
            at = pl.ds(pl.multiple_of(n * group, group), group)
            both = local[at, col] + fwd_cum[at, col] * tiled_f + bwd_cum[at, col] * tiled_b
            z = gate[at, col].astype(F32)
            mixed[at, col] = (both * (z * jax.nn.sigmoid(z))).astype(BF16)
            return carry

        lax.fori_loop(0, local.shape[0] // group, part, 0)
    far[...] = features(mixed[...], weight[0])

    def step(n, carry):
        rest[n] = features(mixed[...], weight[n + 1])
        return carry

    lax.fori_loop(0, 3, step, 0)


def given(place, edges, local, fwd_cum, bwd_cum, coef, gate, weight):
    length, width = local.shape
    return pl.pallas_call(
        give_body,
        in_specs=[in_smem()] + [in_vmem()] * 7,
        out_specs=[in_vmem()] * 3,
        out_shape=[
            jax.ShapeDtypeStruct((length, width), BF16),
            jax.ShapeDtypeStruct((length, width), BF16),
            jax.ShapeDtypeStruct((3, length, width), BF16),
        ],
        compiler_params=pltpu.CompilerParams(vmem_limit_bytes=GIVE_LIMIT),
        cost_estimate=product_cost(length, width, 4),
        name="given",
    )(place, edges, local, fwd_cum, bwd_cum, coef, gate, weight)


def keep_body(mixed, weight, out):
    def step(n, carry):
        out[n] = features(mixed[...], weight[n + 4])
        return carry

    lax.fori_loop(0, 4, step, 0)


def kept(mixed, weight):
    length, width = mixed.shape
    return pl.pallas_call(
        keep_body,
        in_specs=[in_vmem()] * 2,
        out_specs=in_vmem(),
        out_shape=jax.ShapeDtypeStruct((4, length, width), BF16),
        compiler_params=pltpu.CompilerParams(vmem_limit_bytes=KEEP_LIMIT),
        cost_estimate=product_cost(length, width, 4),
        name="kept",
    )(mixed, weight)


def per_device(
    stream_in, norm_gain, value_proj, gate_proj, out_proj, conv_taps, block_gates, forget_rate
):
    rank = lax.axis_index("tp").reshape(1)
    place = lax.axis_index("sp").reshape(1)
    length, _ = stream_in.shape
    half = length // 2
    stream = to_tiles(stream_in)
    top, end = stream[:half], stream[half:]
    pieces_0 = gathered_pieces([value_proj[0], gate_proj[0]])
    outs_0 = lax.all_gather(out_proj[:1], "sp", axis=1, tiled=True)
    held = jnp.stack([value_proj[1], gate_proj[1], out_proj[1]])
    full_1 = lax.all_gather(held, "sp", axis=1, tiled=True)
    weights = [(pieces_0, outs_0, 0), ((full_1,), full_1, 2)]
    for layer in range(value_proj.shape[0]):
        sources, full, which = weights[layer]
        pieces = gathered_stream(top, end)
        halo = token_halo(top, end)
        mix_in = value_rows(rank, place, pieces, halo, norm_gain, layer, sources)
        local, fwd_cum, bwd_cum, coef, edge = scanned(
            rank, mix_in, conv_taps, forget_rate, block_gates, layer, lax.axis_size("sp")
        )
        edges = lax.all_to_all(edge, "sp", 0, 0, tiled=True)
        gate_z, out_weight = gate_rows(rank, place, pieces, norm_gain, layer, sources, full, which)
        mixed, far_give, rest_give = given(
            place, edges, local, fwd_cum, bwd_cum, coef, gate_z, out_weight
        )
        far_away = across(far_give).astype(F32)
        rest_away = across(rest_give).astype(F32)
        keep = kept(mixed, out_weight).astype(F32)
        far = (keep[0] + far_away).astype(BF16)
        up = keep[1] + rest_away[0]
        down = keep[2] + rest_away[1]
        own = keep[3] + rest_away[2]
        relay_top = along_x(far[:half], 1)
        relay_end = along_x(far[half:], -1)
        up_end = along_x(up[half:].astype(BF16), 1)
        down_top = along_x(down[:half].astype(BF16), -1)
        up_top = along_x((up[:half] + relay_top.astype(F32)).astype(BF16), 1)
        down_end = along_x((down[half:] + relay_end.astype(F32)).astype(BF16), -1)
        top = top.astype(F32) + own[:half] + up_top.astype(F32) + down_top.astype(F32)
        end = end.astype(F32) + own[half:] + up_end.astype(F32) + down_end.astype(F32)
        top, end = top.astype(BF16), end.astype(BF16)
    return to_tokens(jnp.concatenate([top, end], axis=0))


def solution(mesh):
    placed = (
        P("sp", "tp"),
        P(),
        P(None, "sp", "tp"),
        P(None, "sp", "tp"),
        P(None, "sp", "tp"),
        P(),
        P(None, None, None, "tp", None),
        P(),
    )
    return jax.shard_map(
        per_device, mesh=mesh, in_specs=placed, out_specs=P("sp", "tp"), check_vma=False
    )
```

```python
import jax
import jax.numpy as jnp
from jax import lax
from jax.experimental import pallas as pl
from jax.experimental.pallas import tpu as pltpu
from jax.sharding import PartitionSpec as P


GATE_SCALE = 8.0
NORM_EPS = 1e-06
F32 = jnp.float32
BF16 = jnp.bfloat16


CHUNKS = 8
SCAN_LIMIT = 24 * 2**20
VALUE_LIMIT = 54 * 2**20
GATE_LIMIT = 54 * 2**20
GIVE_LIMIT = 12 * 2**20
KEEP_LIMIT = 8 * 2**20
HALO = 16


def to_tiles(array):
    rows, width = array.shape
    return array.reshape(CHUNKS, rows // CHUNKS, width).swapaxes(0, 1).reshape(rows, width)


def to_tokens(array):
    rows, width = array.shape
    return array.reshape(rows // CHUNKS, CHUNKS, width).swapaxes(0, 1).reshape(rows, width)


def shifted(array, axis, move):
    count = lax.axis_size(axis)
    return lax.ppermute(array, axis, [(i, move(i)) for i in range(count)])


def across(array):
    return shifted(array, "tp", lambda i: i ^ 1)


def along_x(array, step):
    return shifted(array, "tp", lambda i: (i + 2 * step) % 8)


def token_halo(top, end):
    rows, width = end.shape
    count = lax.axis_size("sp")
    owners = lax.axis_size("tp")
    ends = jnp.concatenate([end[rows - 9 : rows - 8], end[rows - 1 :], top[:1], top[:1]], axis=0)
    copies = jnp.broadcast_to(ends[None], (owners, *ends.shape))
    every = lax.all_to_all(copies, "tp", 0, 0, tiled=True)
    before = lax.ppermute(every[:, :2], "sp", [(i, i + 1) for i in range(count - 1)])
    after = lax.ppermute(every[:, 2:], "sp", [(i + 1, i) for i in range(count - 1)])
    rest = jnp.zeros((owners, HALO - 4, width), end.dtype)
    return jnp.concatenate([before, after, rest], axis=1)


def gathered_stream(top, end):
    left_top = along_x(top, 1)
    right_end = along_x(end, -1)
    left_end = along_x(end, 1)
    right_top = along_x(top, -1)
    far_top = along_x(left_top, 1)
    far_end = along_x(right_end, -1)
    same = (top, end, left_top, left_end, right_top, right_end, far_top, far_end)
    return same + tuple(across(part) for part in same)


def block_of(rank, dx, flip):
    core = rank % 2
    return 2 * ((rank // 2 + dx + 4) % 4) + (1 - core if flip else core)


SHIFTS = (0, -1, 1, 2)


def along_plane(array, axis, step):
    dz, dy = (step, 0) if axis == "z" else (0, step)
    pairs = [
        (4 * z + y, 4 * ((z + dz) % 4) + (y + dy) % 4) for z in range(4) for y in range(4)
    ]
    return lax.ppermute(array, "sp", pairs)


def around(array, axis):
    half = array.shape[0] // 2
    before = along_plane(array, axis, 1)
    after = along_plane(array, axis, -1)
    return (
        before,
        after,
        along_plane(before[:half], axis, 1),
        along_plane(after[half:], axis, -1),
    )


def gathered_pieces(weights):
    half = weights[0].shape[0] // 2
    pieces = []
    for at, (first, second) in ((0, "yz"), (half, "zy")):
        own = jnp.concatenate([w[at : at + half] for w in weights], axis=0)
        before, after, far_top, far_end = around(own, first)
        top = jnp.concatenate([own, before], axis=0)
        end = jnp.concatenate([after, far_top, far_end], axis=0)
        top_before = along_plane(top, second, 1)
        top_after = along_plane(top, second, -1)
        end_after = along_plane(end, second, -1)
        end_before = along_plane(end, second, 1)
        pieces += [top, end, top_before, end_before, top_after, end_after]
        pieces += [along_plane(top_before, second, 1), along_plane(end_after, second, -1)]
    return tuple(pieces)


def block_copies(weight, which, rank, offsets, target, sems):
    size = target.shape[1]
    copies = []
    for n, (dx, flip) in enumerate(offsets):
        at = pl.multiple_of(block_of(rank, dx, flip) * size, size)
        copies.append(
            pltpu.make_async_copy(
                weight.at[which, pl.ds(at, size), :], target.at[n], sems.at[n]
            )
        )
    return copies


def weight_copies(sources, which, place, target, sems):
    blocks, size, _ = target.shape
    if len(sources) == 1:
        return [
            pltpu.make_async_copy(
                sources[0].at[which, pl.ds(n * size, size), :], target.at[n], sems.at[n]
            )
            for n in range(blocks)
        ]
    copies = []
    rows = size // 4
    group = sources[0].shape[0] // 2
    for half in range(2):
        for outer in range(4):
            for inner in range(4):
                ref = sources[8 * half + 2 * outer + inner // 2]
                start = (inner % 2) * group
                dz, dy = (outer, inner) if half == 0 else (inner, outer)
                z = (place // 4 + 4 + SHIFTS[dz]) % 4
                y = (place % 4 + 4 + SHIFTS[dy]) % 4
                at = pl.multiple_of((y % 2) * (2 * rows) + half * rows, rows)
                copies.append(
                    pltpu.make_async_copy(
                        ref.at[pl.ds(start + which * rows, rows), :],
                        target.at[2 * z + y // 2, pl.ds(at, rows), :],
                        sems.at[len(copies)],
                    )
                )
    return copies


ARRIVE = [(dx, flip) for flip in (0, 1) for dx in (0, -1, 1, 2)]
LEAVE = [(dx, flip) for flip in (1, 0) for dx in (2, 1, -1, 0)]


def contracted(rows, weight, total):
    total[...] = jnp.zeros_like(total)

    def step(k, carry):
        total[...] += jnp.dot(rows[k], weight[k], preferred_element_type=F32)
        return carry

    lax.fori_loop(0, rows.shape[0], step, 0)


def row_scale(squares, width):
    return lax.rsqrt(jnp.sum(squares[...], axis=1, keepdims=True) / width + NORM_EPS)


def piece_copies(rank, pieces, rows, sems):
    half = pieces[0].shape[0]
    return [
        pltpu.make_async_copy(
            pieces[2 * k + side],
            rows.at[block_of(rank, dx, flip), pl.ds(side * half, half), :],
            sems.at[2 * k + side],
        )
        for k, (dx, flip) in enumerate(ARRIVE)
        for side in range(2)
    ]


WINDOW = 8


def opened(copies):
    for copy in copies[:WINDOW]:
        copy.start()


def awaited(copies, first, last):
    for n in range(first, last):
        copies[n].wait()
        if n + WINDOW < len(copies):
            copies[n + WINDOW].start()


def scaled_rows(layer, rank, gain, copies, halo, rows, squares):
    width = rows.shape[2]
    half = (rows.shape[1] - (0 if halo is None else HALO)) // 2
    step = 64
    for k, (dx, flip) in enumerate(ARRIVE):
        awaited(copies, 2 * k, 2 * k + 2)
        block = block_of(rank, dx, flip)
        scale = gain[layer : layer + 1, pl.ds(pl.multiple_of(block * width, width), width)]

        def put(raw, at, k=k, block=block, scale=scale):
            raw = raw.astype(F32)
            rows[block, at, :] = (raw * scale).astype(BF16)
            power = raw * raw
            lanes = sum(power[:, 128 * q : 128 * (q + 1)] for q in range(width // 128))
            if k == 0:
                squares[at, :] = lanes
            else:
                squares[at, :] += lanes

        def chunk(n, carry, block=block, put=put):
            for side in range(2):
                at = pl.ds(pl.multiple_of(n * step + side * half, step), step)
                put(rows[block, at, :], at)
            return carry

        lax.fori_loop(0, half // step, chunk, 0)
        if halo is not None:
            put(halo[block], pl.ds(2 * half, HALO))


def value_body(layer, rank, place, gain, halo, *refs):
    pieces, sources = refs[:16], refs[16:-7]
    out, rows, squares, value_in, total, sems, piece_sems = refs[-7:]
    values = weight_copies(sources, 0, place[0], value_in, sems)
    copies = piece_copies(rank[0], pieces, rows, piece_sems) + values
    opened(copies)
    scaled_rows(layer, rank[0], gain, copies, halo, rows, squares)
    awaited(copies, 16, len(copies))
    contracted(rows, value_in, total)
    out[...] = (total[...] * row_scale(squares, out.shape[1] * len(ARRIVE))).astype(BF16)


def gate_body(layer, which, rank, place, gain, *refs):
    pieces, sources, full = refs[:16], refs[16:-10], refs[-10]
    out, out_in, rows, squares, gate_in, total, sems, out_sems, piece_sems = refs[-9:]
    gates = weight_copies(sources, 1, place[0], gate_in, sems)
    others = block_copies(full, which, rank[0], LEAVE, out_in, out_sems)
    copies = piece_copies(rank[0], pieces, rows, piece_sems) + gates + others
    opened(copies)
    scaled_rows(layer, rank[0], gain, copies, None, rows, squares)
    awaited(copies, 16, 16 + len(gates))
    contracted(rows, gate_in, total)
    out[...] = (total[...] * row_scale(squares, out.shape[1] * len(ARRIVE))).astype(BF16)
    awaited(copies, 16 + len(gates), len(copies))


def in_smem():
    return pl.BlockSpec(memory_space=pltpu.SMEM)


def in_vmem():
    return pl.BlockSpec(memory_space=pltpu.VMEM)


def in_hbm():
    return pl.BlockSpec(memory_space=pltpu.HBM)


def product_cost(rows, width, count):
    return pl.CostEstimate(
        flops=2 * count * rows * width * width,
        bytes_accessed=2 * count * width * width,
        transcendentals=0,
    )


def value_rows(rank, place, pieces, halo, norm_gain, layer, sources):
    half, width = pieces[0].shape
    count = norm_gain.shape[1] // width
    deep = 2 * half + HALO
    return pl.pallas_call(
        lambda *refs: value_body(layer, *refs),
        out_shape=jax.ShapeDtypeStruct((deep, width), BF16),
        in_specs=[in_smem()] * 2 + [in_vmem()] * 2 + [in_hbm()] * (16 + len(sources)),
        out_specs=in_vmem(),
        scratch_shapes=[
            pltpu.VMEM((count, deep, width), BF16),
            pltpu.VMEM((deep, 128), F32),
            pltpu.VMEM((count, width, width), BF16),
            pltpu.VMEM((deep, width), F32),
            pltpu.SemaphoreType.DMA((32,)),
            pltpu.SemaphoreType.DMA((16,)),
        ],
        compiler_params=pltpu.CompilerParams(vmem_limit_bytes=VALUE_LIMIT),
        cost_estimate=product_cost(deep, width, count),
        name="value_rows",
    )(rank, place, norm_gain, halo, *pieces, *sources)


def gate_rows(rank, place, pieces, norm_gain, layer, sources, full, which):
    half, width = pieces[0].shape
    count = norm_gain.shape[1] // width
    length = 2 * half
    return pl.pallas_call(
        lambda *refs: gate_body(layer, which, *refs),
        out_shape=[
            jax.ShapeDtypeStruct((length, width), BF16),
            jax.ShapeDtypeStruct((count, width, width), BF16),
        ],
        in_specs=[in_smem()] * 2 + [in_vmem()] + [in_hbm()] * (17 + len(sources)),
        out_specs=[in_vmem()] * 2,
        scratch_shapes=[
            pltpu.VMEM((count, length, width), BF16),
            pltpu.VMEM((length, 128), F32),
            pltpu.VMEM((count, width, width), BF16),
            pltpu.VMEM((length, width), F32),
            pltpu.SemaphoreType.DMA((32,)),
            pltpu.SemaphoreType.DMA((count,)),
            pltpu.SemaphoreType.DMA((16,)),
        ],
        compiler_params=pltpu.CompilerParams(vmem_limit_bytes=GATE_LIMIT),
        cost_estimate=product_cost(length, width, count),
        name="gate_rows",
    )(rank, place, norm_gain, *pieces, *sources, full)


def scan_body(
    rank, mix, taps, rate, gates, local, fwd_cum, bwd_cum, coef, edge, padded, conv, pre
):
    steps = conv.shape[0] // CHUNKS
    length = conv.shape[0]
    sub = lax.broadcasted_iota(jnp.int32, (CHUNKS, 128), 0)
    rows = mix[...].astype(F32)
    halo = rows[length : length + 8]
    padded[16 : 16 + length] = rows[:length]
    padded[0:8] = jnp.where(
        sub == 0, halo[0:1], pltpu.roll(rows[length - 16 : length - 8], 1, axis=0)
    )
    padded[8:16] = jnp.where(sub == 0, halo[1:2], pltpu.roll(rows[length - 8 : length], 1, axis=0))
    padded[16 + length : 24 + length] = jnp.where(
        sub == CHUNKS - 1, halo[2:3], pltpu.roll(rows[0:8], CHUNKS - 1, axis=0)
    )
    for part in range(8):
        lo = part * (length // 8)
        hi = lo + length // 8
        conv[lo:hi] = sum(padded[lo + 8 * k : hi + 8 * k] * taps[0, k : k + 1] for k in range(4))
    lhs = conv[...].astype(BF16)
    for g in range(4):
        pre[g] = jnp.dot(lhs, gates[0, g // 2, g % 2], preferred_element_type=F32)

    def cell(i, e):
        at = pl.ds(pl.multiple_of(i * CHUNKS, CHUNKS), CHUNKS)
        recur = jax.nn.sigmoid(pre[2 * e, at, :])
        entry = jax.nn.sigmoid(pre[2 * e + 1, at, :])
        log_a = (-GATE_SCALE) * recur * rate[0, e : e + 1]
        decay = jnp.exp(log_a)
        x = 2.0 * log_a
        near = x * (1.0 + x * (0.5 + x * (1.0 / 6 + x * (1.0 / 24 + x * (1.0 / 120)))))
        room = -jnp.where(x > -0.125, near, decay * decay - 1.0)
        return at, decay, jnp.sqrt(room) * entry * conv[at, :]

    zero = jnp.zeros((CHUNKS, 128), F32)
    one = jnp.ones((CHUNKS, 128), F32)
    inner = 8

    def forward(block, carry):
        state, cum = carry
        for n in range(inner):
            at, decay, drive = cell(block * inner + n, 0)
            state = decay * state + drive
            cum = decay * cum
            local[at, :] = state
            fwd_cum[at, :] = cum
        return state, cum

    def backward(block, carry):
        state, cum = carry
        for n in range(inner):
            at, decay, drive = cell(steps - 1 - (block * inner + n), 1)
            state = decay * state + drive
            cum = decay * cum
            local[at, :] += state
            bwd_cum[at, :] = cum
        return state, cum

    state_f, cum_f = lax.fori_loop(0, steps // inner, forward, (zero, one))
    state_b, cum_b = lax.fori_loop(0, steps // inner, backward, (zero, one))
    alpha = jnp.zeros((1, 128), F32)
    beta = jnp.ones((1, 128), F32)
    for s in range(CHUNKS):
        coef[0, s : s + 1] = alpha
        coef[1, s : s + 1] = beta
        alpha = state_f[s : s + 1] + cum_f[s : s + 1] * alpha
        beta = cum_f[s : s + 1] * beta
    sums_f = (beta, alpha)
    alpha = jnp.zeros((1, 128), F32)
    beta = jnp.ones((1, 128), F32)
    for s in reversed(range(CHUNKS)):
        coef[2, s : s + 1] = alpha
        coef[3, s : s + 1] = beta
        alpha = state_b[s : s + 1] + cum_b[s : s + 1] * alpha
        beta = cum_b[s : s + 1] * beta
    edge[...] = jnp.broadcast_to(
        jnp.concatenate([*sums_f, beta, alpha], axis=0)[None], edge.shape
    )


def scanned(rank, mix, conv_taps, forget_rate, block_gates, layer, copies):
    deep, width = mix.shape
    length = deep - HALO
    blocks = width // 128
    column = lambda b, rank: (0, b)
    owned = lambda b, rank: (layer, 0, rank[0] * blocks + b)
    return pl.pallas_call(
        scan_body,
        grid_spec=pltpu.PrefetchScalarGridSpec(
            num_scalar_prefetch=1,
            grid=(blocks,),
            in_specs=[
                pl.BlockSpec((deep, 128), column),
                pl.BlockSpec((1, 4, 128), owned),
                pl.BlockSpec((1, 2, 128), owned),
                pl.BlockSpec((1, 2, 2, 128, 128), lambda b, rank: (layer, 0, 0, b, 0)),
            ],
            out_specs=[
                pl.BlockSpec((length, 128), column),
                pl.BlockSpec((length, 128), column),
                pl.BlockSpec((length, 128), column),
                pl.BlockSpec((4, CHUNKS, 128), lambda b, rank: (0, 0, b)),
                pl.BlockSpec((copies, 4, 128), lambda b, rank: (0, 0, b)),
            ],
            scratch_shapes=[
                pltpu.VMEM((length + 24, 128), F32),
                pltpu.VMEM((length, 128), F32),
                pltpu.VMEM((4, length, 128), F32),
            ],
        ),
        out_shape=[
            jax.ShapeDtypeStruct((length, width), F32),
            jax.ShapeDtypeStruct((length, width), F32),
            jax.ShapeDtypeStruct((length, width), F32),
            jax.ShapeDtypeStruct((4, CHUNKS, width), F32),
            jax.ShapeDtypeStruct((copies, 4, width), F32),
        ],
        compiler_params=pltpu.CompilerParams(vmem_limit_bytes=SCAN_LIMIT),
        cost_estimate=pl.CostEstimate(
            flops=10_000_000_000, bytes_accessed=4_000_000, transcendentals=4_000_000
        ),
        name="scan",
    )(rank, mix, conv_taps, forget_rate, block_gates)


def features(mixed, weight):
    return lax.dot_general(
        mixed, weight, (((1,), (1,)), ((), ())), preferred_element_type=F32
    ).astype(BF16)


def give_body(
    place, edges, local, fwd_cum, bwd_cum, coef, gate, weight, mixed, far, rest
):
    mine = place[0]
    count, _, width = edges.shape
    enter_f = jnp.zeros((1, width), F32)
    enter_b = jnp.zeros((1, width), F32)
    for r in range(count):
        enter_f = jnp.where(r < mine, edges[r, 1:2] + edges[r, 0:1] * enter_f, enter_f)
        q = count - 1 - r
        enter_b = jnp.where(q > mine, edges[q, 3:4] + edges[q, 2:3] * enter_b, enter_b)
    from_f = coef[0] + coef[1] * enter_f
    from_b = coef[2] + coef[3] * enter_b
    group = 64
    for c in range(width // 128):
        col = slice(128 * c, 128 * (c + 1))
        tiled_f = jnp.concatenate([from_f[:, col]] * (group // CHUNKS), axis=0)
        tiled_b = jnp.concatenate([from_b[:, col]] * (group // CHUNKS), axis=0)

        def part(n, carry, col=col, tiled_f=tiled_f, tiled_b=tiled_b):
            at = pl.ds(pl.multiple_of(n * group, group), group)
            both = local[at, col] + fwd_cum[at, col] * tiled_f + bwd_cum[at, col] * tiled_b
            z = gate[at, col].astype(F32)
            mixed[at, col] = (both * (z * jax.nn.sigmoid(z))).astype(BF16)
            return carry

        lax.fori_loop(0, local.shape[0] // group, part, 0)
    far[...] = features(mixed[...], weight[0])

    def step(n, carry):
        rest[n] = features(mixed[...], weight[n + 1])
        return carry

    lax.fori_loop(0, 3, step, 0)


def given(place, edges, local, fwd_cum, bwd_cum, coef, gate, weight):
    length, width = local.shape
    return pl.pallas_call(
        give_body,
        in_specs=[in_smem()] + [in_vmem()] * 7,
        out_specs=[in_vmem()] * 3,
        out_shape=[
            jax.ShapeDtypeStruct((length, width), BF16),
            jax.ShapeDtypeStruct((length, width), BF16),
            jax.ShapeDtypeStruct((3, length, width), BF16),
        ],
        compiler_params=pltpu.CompilerParams(vmem_limit_bytes=GIVE_LIMIT),
        cost_estimate=product_cost(length, width, 4),
        name="given",
    )(place, edges, local, fwd_cum, bwd_cum, coef, gate, weight)


def keep_body(mixed, weight, far, rest):
    far[...] = features(mixed[...], weight[4])

    def step(n, carry):
        rest[n] = features(mixed[...], weight[n + 5])
        return carry

    lax.fori_loop(0, 3, step, 0)


def kept(mixed, weight):
    length, width = mixed.shape
    return pl.pallas_call(
        keep_body,
        in_specs=[in_vmem()] * 2,
        out_specs=[in_vmem()] * 2,
        out_shape=[
            jax.ShapeDtypeStruct((length, width), BF16),
            jax.ShapeDtypeStruct((3, length, width), BF16),
        ],
        compiler_params=pltpu.CompilerParams(vmem_limit_bytes=KEEP_LIMIT),
        cost_estimate=product_cost(length, width, 4),
        name="kept",
    )(mixed, weight)


def total_of(*parts):
    return sum(part.astype(F32) for part in parts)


def per_device(
    stream_in, norm_gain, value_proj, gate_proj, out_proj, conv_taps, block_gates, forget_rate
):
    rank = lax.axis_index("tp").reshape(1)
    place = lax.axis_index("sp").reshape(1)
    length, _ = stream_in.shape
    half = length // 2
    stream = to_tiles(stream_in)
    top, end = stream[:half], stream[half:]
    pieces_0 = gathered_pieces([value_proj[0], gate_proj[0]])
    outs_0 = lax.all_gather(out_proj[:1], "sp", axis=1, tiled=True)
    held = jnp.stack([value_proj[1], gate_proj[1], out_proj[1]])
    full_1 = lax.all_gather(held, "sp", axis=1, tiled=True)
    weights = [(pieces_0, outs_0, 0), ((full_1,), full_1, 2)]
    for layer in range(value_proj.shape[0]):
        sources, full, which = weights[layer]
        pieces = gathered_stream(top, end)
        halo = token_halo(top, end)
        mix_in = value_rows(rank, place, pieces, halo, norm_gain, layer, sources)
        local, fwd_cum, bwd_cum, coef, edge = scanned(
            rank, mix_in, conv_taps, forget_rate, block_gates, layer, lax.axis_size("sp")
        )
        edges = lax.all_to_all(edge, "sp", 0, 0, tiled=True)
        gate_z, out_weight = gate_rows(rank, place, pieces, norm_gain, layer, sources, full, which)
        mixed, far_give, rest_give = given(
            place, edges, local, fwd_cum, bwd_cum, coef, gate_z, out_weight
        )
        far_away = across(far_give)
        rest_away = across(rest_give)
        far_keep, rest_keep = kept(mixed, out_weight)
        far = total_of(far_keep, far_away).astype(BF16)
        halves = (slice(0, half), slice(half, length))
        up, down, own = (
            [(rest_keep[n, rows], rest_away[n, rows]) for rows in halves] for n in range(3)
        )
        relay_top = along_x(far[:half], 1)
        relay_end = along_x(far[half:], -1)
        up_end = along_x(total_of(*up[1]).astype(BF16), 1)
        down_top = along_x(total_of(*down[0]).astype(BF16), -1)
        up_top = along_x(total_of(*up[0], relay_top).astype(BF16), 1)
        down_end = along_x(total_of(*down[1], relay_end).astype(BF16), -1)
        up_top, down_top, up_end, down_end = lax.optimization_barrier(
            (up_top, down_top, up_end, down_end)
        )
        top = total_of(top, *own[0], up_top, down_top).astype(BF16)
        end = total_of(end, *own[1], up_end, down_end).astype(BF16)
    return to_tokens(jnp.concatenate([top, end], axis=0))


def solution(mesh):
    placed = (
        P("sp", "tp"),
        P(),
        P(None, "sp", "tp"),
        P(None, "sp", "tp"),
        P(None, "sp", "tp"),
        P(),
        P(None, None, None, "tp", None),
        P(),
    )
    return jax.shard_map(
        per_device, mesh=mesh, in_specs=placed, out_specs=P("sp", "tp"), check_vma=False
    )
```

```python
import jax
import jax.numpy as jnp
from jax import lax
from jax.experimental import pallas as pl
from jax.experimental.pallas import tpu as pltpu
from jax.sharding import PartitionSpec as P


GATE_SCALE = 8.0
NORM_EPS = 1e-06
F32 = jnp.float32
BF16 = jnp.bfloat16


CHUNKS = 8
SCAN_LIMIT = 24 * 2**20
VALUE_LIMIT = 54 * 2**20
GATE_LIMIT = 54 * 2**20
GIVE_LIMIT = 12 * 2**20
KEEP_LIMIT = 8 * 2**20
HALO = 16


def to_tiles(array):
    rows, width = array.shape
    return array.reshape(CHUNKS, rows // CHUNKS, width).swapaxes(0, 1).reshape(rows, width)


def to_tokens(array):
    rows, width = array.shape
    return array.reshape(rows // CHUNKS, CHUNKS, width).swapaxes(0, 1).reshape(rows, width)


def shifted(array, axis, move):
    count = lax.axis_size(axis)
    return lax.ppermute(array, axis, [(i, move(i)) for i in range(count)])


def across(array):
    return shifted(array, "tp", lambda i: i ^ 1)


def along_x(array, step):
    return shifted(array, "tp", lambda i: (i + 2 * step) % 8)


def token_halo(top, end):
    rows, width = end.shape
    count = lax.axis_size("sp")
    owners = lax.axis_size("tp")
    ends = jnp.concatenate([end[rows - 9 : rows - 8], end[rows - 1 :], top[:1], top[:1]], axis=0)
    copies = jnp.broadcast_to(ends[None], (owners, *ends.shape))
    every = lax.all_to_all(copies, "tp", 0, 0, tiled=True)
    before = lax.ppermute(every[:, :2], "sp", [(i, i + 1) for i in range(count - 1)])
    after = lax.ppermute(every[:, 2:], "sp", [(i + 1, i) for i in range(count - 1)])
    rest = jnp.zeros((owners, HALO - 4, width), end.dtype)
    return jnp.concatenate([before, after, rest], axis=1)


def gathered_stream(top, end):
    left_top = along_x(top, 1)
    right_end = along_x(end, -1)
    left_end = along_x(end, 1)
    right_top = along_x(top, -1)
    far_top = along_x(left_top, 1)
    far_end = along_x(right_end, -1)
    same = (top, end, left_top, left_end, right_top, right_end, far_top, far_end)
    return same + tuple(across(part) for part in same)


def block_of(rank, dx, flip):
    core = rank % 2
    return 2 * ((rank // 2 + dx + 4) % 4) + (1 - core if flip else core)


SHIFTS = (0, -1, 1, 2)


def along_plane(array, axis, step):
    dz, dy = (step, 0) if axis == "z" else (0, step)
    pairs = [
        (4 * z + y, 4 * ((z + dz) % 4) + (y + dy) % 4) for z in range(4) for y in range(4)
    ]
    return lax.ppermute(array, "sp", pairs)


def around(array, axis):
    half = array.shape[0] // 2
    before = along_plane(array, axis, 1)
    after = along_plane(array, axis, -1)
    return (
        before,
        after,
        along_plane(before[:half], axis, 1),
        along_plane(after[half:], axis, -1),
    )


def gathered_pieces(weights):
    half = weights[0].shape[0] // 2
    pieces = []
    for at, (first, second) in ((0, "yz"), (half, "zy")):
        own = jnp.concatenate([w[at : at + half] for w in weights], axis=0)
        before, after, far_top, far_end = around(own, first)
        top = jnp.concatenate([own, before], axis=0)
        end = jnp.concatenate([after, far_top, far_end], axis=0)
        top_before = along_plane(top, second, 1)
        top_after = along_plane(top, second, -1)
        end_after = along_plane(end, second, -1)
        end_before = along_plane(end, second, 1)
        pieces += [top, end, top_before, end_before, top_after, end_after]
        pieces += [along_plane(top_before, second, 1), along_plane(end_after, second, -1)]
    return tuple(pieces)


def block_copies(weight, which, rank, offsets, target, sems):
    size = target.shape[1]
    copies = []
    for n, (dx, flip) in enumerate(offsets):
        at = pl.multiple_of(block_of(rank, dx, flip) * size, size)
        copies.append(
            pltpu.make_async_copy(
                weight.at[which, pl.ds(at, size), :], target.at[n], sems.at[n]
            )
        )
    return copies


def weight_copies(sources, which, place, target, sems):
    blocks, size, _ = target.shape
    if len(sources) == 1:
        return [
            pltpu.make_async_copy(
                sources[0].at[which, pl.ds(n * size, size), :], target.at[n], sems.at[n]
            )
            for n in range(blocks)
        ]
    copies = []
    rows = size // 4
    group = sources[0].shape[0] // 2
    for half in range(2):
        for outer in range(4):
            for inner in range(4):
                ref = sources[8 * half + 2 * outer + inner // 2]
                start = (inner % 2) * group
                dz, dy = (outer, inner) if half == 0 else (inner, outer)
                z = (place // 4 + 4 + SHIFTS[dz]) % 4
                y = (place % 4 + 4 + SHIFTS[dy]) % 4
                at = pl.multiple_of((y % 2) * (2 * rows) + half * rows, rows)
                copies.append(
                    pltpu.make_async_copy(
                        ref.at[pl.ds(start + which * rows, rows), :],
                        target.at[2 * z + y // 2, pl.ds(at, rows), :],
                        sems.at[len(copies)],
                    )
                )
    return copies


ARRIVE = [(dx, flip) for flip in (0, 1) for dx in (0, -1, 1, 2)]
LEAVE = [(dx, flip) for flip in (1, 0) for dx in (2, 1, -1, 0)]


def contracted(rows, weight, total):
    total[...] = jnp.zeros_like(total)

    def step(k, carry):
        total[...] += jnp.dot(rows[k], weight[k], preferred_element_type=F32)
        return carry

    lax.fori_loop(0, rows.shape[0], step, 0)


def row_scale(squares, width):
    return lax.rsqrt(jnp.sum(squares[...], axis=1, keepdims=True) / width + NORM_EPS)


def piece_copies(rank, pieces, rows, sems):
    half = pieces[0].shape[0]
    return [
        pltpu.make_async_copy(
            pieces[2 * k + side],
            rows.at[block_of(rank, dx, flip), pl.ds(side * half, half), :],
            sems.at[2 * k + side],
        )
        for k, (dx, flip) in enumerate(ARRIVE)
        for side in range(2)
    ]


def scaled_rows(layer, rank, gain, copies, halo, rows, squares):
    width = rows.shape[2]
    half = (rows.shape[1] - (0 if halo is None else HALO)) // 2
    step = 64
    for k, (dx, flip) in enumerate(ARRIVE):
        copies[2 * k].wait()
        copies[2 * k + 1].wait()
        block = block_of(rank, dx, flip)
        scale = gain[layer : layer + 1, pl.ds(pl.multiple_of(block * width, width), width)]

        def put(raw, at, k=k, block=block, scale=scale):
            raw = raw.astype(F32)
            rows[block, at, :] = (raw * scale).astype(BF16)
            power = raw * raw
            lanes = sum(power[:, 128 * q : 128 * (q + 1)] for q in range(width // 128))
            if k == 0:
                squares[at, :] = lanes
            else:
                squares[at, :] += lanes

        def chunk(n, carry, block=block, put=put):
            for side in range(2):
                at = pl.ds(pl.multiple_of(n * step + side * half, step), step)
                put(rows[block, at, :], at)
            return carry

        lax.fori_loop(0, half // step, chunk, 0)
        if halo is not None:
            put(halo[block], pl.ds(2 * half, HALO))


def value_body(layer, rank, place, gain, halo, *refs):
    pieces, sources = refs[:16], refs[16:-7]
    out, rows, squares, value_in, total, sems, piece_sems = refs[-7:]
    values = weight_copies(sources, 0, place[0], value_in, sems)
    arriving = piece_copies(rank[0], pieces, rows, piece_sems)
    for copy in arriving + values:
        copy.start()
    scaled_rows(layer, rank[0], gain, arriving, halo, rows, squares)
    for copy in values:
        copy.wait()
    contracted(rows, value_in, total)
    out[...] = (total[...] * row_scale(squares, out.shape[1] * len(ARRIVE))).astype(BF16)


def gate_body(layer, which, rank, place, gain, *refs):
    pieces, sources, full = refs[:16], refs[16:-10], refs[-10]
    out, out_in, rows, squares, gate_in, total, sems, out_sems, piece_sems = refs[-9:]
    gates = weight_copies(sources, 1, place[0], gate_in, sems)
    others = block_copies(full, which, rank[0], LEAVE, out_in, out_sems)
    arriving = piece_copies(rank[0], pieces, rows, piece_sems)
    for copy in arriving + gates:
        copy.start()
    scaled_rows(layer, rank[0], gain, arriving, None, rows, squares)
    for copy in gates:
        copy.wait()
    for copy in others:
        copy.start()
    contracted(rows, gate_in, total)
    out[...] = (total[...] * row_scale(squares, out.shape[1] * len(ARRIVE))).astype(BF16)
    for copy in others:
        copy.wait()


def in_smem():
    return pl.BlockSpec(memory_space=pltpu.SMEM)


def in_vmem():
    return pl.BlockSpec(memory_space=pltpu.VMEM)


def in_hbm():
    return pl.BlockSpec(memory_space=pltpu.HBM)


def product_cost(rows, width, count):
    return pl.CostEstimate(
        flops=2 * count * rows * width * width,
        bytes_accessed=2 * count * width * width,
        transcendentals=0,
    )


def value_rows(rank, place, pieces, halo, norm_gain, layer, sources):
    half, width = pieces[0].shape
    count = norm_gain.shape[1] // width
    deep = 2 * half + HALO
    return pl.pallas_call(
        lambda *refs: value_body(layer, *refs),
        out_shape=jax.ShapeDtypeStruct((deep, width), BF16),
        in_specs=[in_smem()] * 2 + [in_vmem()] * 2 + [in_hbm()] * (16 + len(sources)),
        out_specs=in_vmem(),
        scratch_shapes=[
            pltpu.VMEM((count, deep, width), BF16),
            pltpu.VMEM((deep, 128), F32),
            pltpu.VMEM((count, width, width), BF16),
            pltpu.VMEM((deep, width), F32),
            pltpu.SemaphoreType.DMA((32,)),
            pltpu.SemaphoreType.DMA((16,)),
        ],
        compiler_params=pltpu.CompilerParams(vmem_limit_bytes=VALUE_LIMIT),
        cost_estimate=product_cost(deep, width, count),
        name="value_rows",
    )(rank, place, norm_gain, halo, *pieces, *sources)


def gate_rows(rank, place, pieces, norm_gain, layer, sources, full, which):
    half, width = pieces[0].shape
    count = norm_gain.shape[1] // width
    length = 2 * half
    return pl.pallas_call(
        lambda *refs: gate_body(layer, which, *refs),
        out_shape=[
            jax.ShapeDtypeStruct((length, width), BF16),
            jax.ShapeDtypeStruct((count, width, width), BF16),
        ],
        in_specs=[in_smem()] * 2 + [in_vmem()] + [in_hbm()] * (17 + len(sources)),
        out_specs=[in_vmem()] * 2,
        scratch_shapes=[
            pltpu.VMEM((count, length, width), BF16),
            pltpu.VMEM((length, 128), F32),
            pltpu.VMEM((count, width, width), BF16),
            pltpu.VMEM((length, width), F32),
            pltpu.SemaphoreType.DMA((32,)),
            pltpu.SemaphoreType.DMA((count,)),
            pltpu.SemaphoreType.DMA((16,)),
        ],
        compiler_params=pltpu.CompilerParams(vmem_limit_bytes=GATE_LIMIT),
        cost_estimate=product_cost(length, width, count),
        name="gate_rows",
    )(rank, place, norm_gain, *pieces, *sources, full)


def scan_body(
    rank, mix, taps, rate, gates, local, fwd_cum, bwd_cum, coef, edge, padded, conv, pre
):
    steps = conv.shape[0] // CHUNKS
    length = conv.shape[0]
    sub = lax.broadcasted_iota(jnp.int32, (CHUNKS, 128), 0)
    rows = mix[...].astype(F32)
    halo = rows[length : length + 8]
    padded[16 : 16 + length] = rows[:length]
    padded[0:8] = jnp.where(
        sub == 0, halo[0:1], pltpu.roll(rows[length - 16 : length - 8], 1, axis=0)
    )
    padded[8:16] = jnp.where(sub == 0, halo[1:2], pltpu.roll(rows[length - 8 : length], 1, axis=0))
    padded[16 + length : 24 + length] = jnp.where(
        sub == CHUNKS - 1, halo[2:3], pltpu.roll(rows[0:8], CHUNKS - 1, axis=0)
    )
    for part in range(8):
        lo = part * (length // 8)
        hi = lo + length // 8
        conv[lo:hi] = sum(padded[lo + 8 * k : hi + 8 * k] * taps[0, k : k + 1] for k in range(4))
    lhs = conv[...].astype(BF16)
    for g in range(4):
        pre[g] = jnp.dot(lhs, gates[0, g // 2, g % 2], preferred_element_type=F32)

    def cell(i, e):
        at = pl.ds(pl.multiple_of(i * CHUNKS, CHUNKS), CHUNKS)
        recur = jax.nn.sigmoid(pre[2 * e, at, :])
        entry = jax.nn.sigmoid(pre[2 * e + 1, at, :])
        log_a = (-GATE_SCALE) * recur * rate[0, e : e + 1]
        decay = jnp.exp(log_a)
        x = 2.0 * log_a
        near = x * (1.0 + x * (0.5 + x * (1.0 / 6 + x * (1.0 / 24 + x * (1.0 / 120)))))
        room = -jnp.where(x > -0.125, near, decay * decay - 1.0)
        return at, decay, jnp.sqrt(room) * entry * conv[at, :]

    zero = jnp.zeros((CHUNKS, 128), F32)
    one = jnp.ones((CHUNKS, 128), F32)
    inner = 8

    def forward(block, carry):
        state, cum = carry
        for n in range(inner):
            at, decay, drive = cell(block * inner + n, 0)
            state = decay * state + drive
            cum = decay * cum
            local[at, :] = state
            fwd_cum[at, :] = cum
        return state, cum

    def backward(block, carry):
        state, cum = carry
        for n in range(inner):
            at, decay, drive = cell(steps - 1 - (block * inner + n), 1)
            state = decay * state + drive
            cum = decay * cum
            local[at, :] += state
            bwd_cum[at, :] = cum
        return state, cum

    state_f, cum_f = lax.fori_loop(0, steps // inner, forward, (zero, one))
    state_b, cum_b = lax.fori_loop(0, steps // inner, backward, (zero, one))
    alpha = jnp.zeros((1, 128), F32)
    beta = jnp.ones((1, 128), F32)
    for s in range(CHUNKS):
        coef[0, s : s + 1] = alpha
        coef[1, s : s + 1] = beta
        alpha = state_f[s : s + 1] + cum_f[s : s + 1] * alpha
        beta = cum_f[s : s + 1] * beta
    sums_f = (beta, alpha)
    alpha = jnp.zeros((1, 128), F32)
    beta = jnp.ones((1, 128), F32)
    for s in reversed(range(CHUNKS)):
        coef[2, s : s + 1] = alpha
        coef[3, s : s + 1] = beta
        alpha = state_b[s : s + 1] + cum_b[s : s + 1] * alpha
        beta = cum_b[s : s + 1] * beta
    edge[...] = jnp.broadcast_to(
        jnp.concatenate([*sums_f, beta, alpha], axis=0)[None], edge.shape
    )


def scanned(rank, mix, conv_taps, forget_rate, block_gates, layer, copies):
    deep, width = mix.shape
    length = deep - HALO
    blocks = width // 128
    column = lambda b, rank: (0, b)
    owned = lambda b, rank: (layer, 0, rank[0] * blocks + b)
    return pl.pallas_call(
        scan_body,
        grid_spec=pltpu.PrefetchScalarGridSpec(
            num_scalar_prefetch=1,
            grid=(blocks,),
            in_specs=[
                pl.BlockSpec((deep, 128), column),
                pl.BlockSpec((1, 4, 128), owned),
                pl.BlockSpec((1, 2, 128), owned),
                pl.BlockSpec((1, 2, 2, 128, 128), lambda b, rank: (layer, 0, 0, b, 0)),
            ],
            out_specs=[
                pl.BlockSpec((length, 128), column),
                pl.BlockSpec((length, 128), column),
                pl.BlockSpec((length, 128), column),
                pl.BlockSpec((4, CHUNKS, 128), lambda b, rank: (0, 0, b)),
                pl.BlockSpec((copies, 4, 128), lambda b, rank: (0, 0, b)),
            ],
            scratch_shapes=[
                pltpu.VMEM((length + 24, 128), F32),
                pltpu.VMEM((length, 128), F32),
                pltpu.VMEM((4, length, 128), F32),
            ],
        ),
        out_shape=[
            jax.ShapeDtypeStruct((length, width), F32),
            jax.ShapeDtypeStruct((length, width), F32),
            jax.ShapeDtypeStruct((length, width), F32),
            jax.ShapeDtypeStruct((4, CHUNKS, width), F32),
            jax.ShapeDtypeStruct((copies, 4, width), F32),
        ],
        compiler_params=pltpu.CompilerParams(vmem_limit_bytes=SCAN_LIMIT),
        cost_estimate=pl.CostEstimate(
            flops=10_000_000_000, bytes_accessed=4_000_000, transcendentals=4_000_000
        ),
        name="scan",
    )(rank, mix, conv_taps, forget_rate, block_gates)


def features(mixed, weight):
    return lax.dot_general(
        mixed, weight, (((1,), (1,)), ((), ())), preferred_element_type=F32
    ).astype(BF16)


def give_body(
    place, edges, local, fwd_cum, bwd_cum, coef, gate, weight, mixed, far, rest
):
    mine = place[0]
    count, _, width = edges.shape
    enter_f = jnp.zeros((1, width), F32)
    enter_b = jnp.zeros((1, width), F32)
    for r in range(count):
        enter_f = jnp.where(r < mine, edges[r, 1:2] + edges[r, 0:1] * enter_f, enter_f)
        q = count - 1 - r
        enter_b = jnp.where(q > mine, edges[q, 3:4] + edges[q, 2:3] * enter_b, enter_b)
    from_f = coef[0] + coef[1] * enter_f
    from_b = coef[2] + coef[3] * enter_b
    group = 64
    for c in range(width // 128):
        col = slice(128 * c, 128 * (c + 1))
        tiled_f = jnp.concatenate([from_f[:, col]] * (group // CHUNKS), axis=0)
        tiled_b = jnp.concatenate([from_b[:, col]] * (group // CHUNKS), axis=0)

        def part(n, carry, col=col, tiled_f=tiled_f, tiled_b=tiled_b):
            at = pl.ds(pl.multiple_of(n * group, group), group)
            both = local[at, col] + fwd_cum[at, col] * tiled_f + bwd_cum[at, col] * tiled_b
            z = gate[at, col].astype(F32)
            mixed[at, col] = (both * (z * jax.nn.sigmoid(z))).astype(BF16)
            return carry

        lax.fori_loop(0, local.shape[0] // group, part, 0)
    far[...] = features(mixed[...], weight[0])

    def step(n, carry):
        rest[n] = features(mixed[...], weight[n + 1])
        return carry

    lax.fori_loop(0, 3, step, 0)


def given(place, edges, local, fwd_cum, bwd_cum, coef, gate, weight):
    length, width = local.shape
    return pl.pallas_call(
        give_body,
        in_specs=[in_smem()] + [in_vmem()] * 7,
        out_specs=[in_vmem()] * 3,
        out_shape=[
            jax.ShapeDtypeStruct((length, width), BF16),
            jax.ShapeDtypeStruct((length, width), BF16),
            jax.ShapeDtypeStruct((3, length, width), BF16),
        ],
        compiler_params=pltpu.CompilerParams(vmem_limit_bytes=GIVE_LIMIT),
        cost_estimate=product_cost(length, width, 4),
        name="given",
    )(place, edges, local, fwd_cum, bwd_cum, coef, gate, weight)


def keep_body(mixed, weight, far, rest):
    far[...] = features(mixed[...], weight[4])

    def step(n, carry):
        rest[n] = features(mixed[...], weight[n + 5])
        return carry

    lax.fori_loop(0, 3, step, 0)


def kept(mixed, weight):
    length, width = mixed.shape
    return pl.pallas_call(
        keep_body,
        in_specs=[in_vmem()] * 2,
        out_specs=[in_vmem()] * 2,
        out_shape=[
            jax.ShapeDtypeStruct((length, width), BF16),
            jax.ShapeDtypeStruct((3, length, width), BF16),
        ],
        compiler_params=pltpu.CompilerParams(vmem_limit_bytes=KEEP_LIMIT),
        cost_estimate=product_cost(length, width, 4),
        name="kept",
    )(mixed, weight)


def total_of(*parts):
    return sum(part.astype(F32) for part in parts)


def per_device(
    stream_in, norm_gain, value_proj, gate_proj, out_proj, conv_taps, block_gates, forget_rate
):
    rank = lax.axis_index("tp").reshape(1)
    place = lax.axis_index("sp").reshape(1)
    length, _ = stream_in.shape
    half = length // 2
    stream = to_tiles(stream_in)
    top, end = stream[:half], stream[half:]
    pieces_0 = gathered_pieces([value_proj[0], gate_proj[0]])
    outs_0 = lax.all_gather(out_proj[:1], "sp", axis=1, tiled=True)
    held = jnp.stack([value_proj[1], gate_proj[1], out_proj[1]])
    full_1 = lax.all_gather(held, "sp", axis=1, tiled=True)
    weights = [(pieces_0, outs_0, 0), ((full_1,), full_1, 2)]
    for layer in range(value_proj.shape[0]):
        sources, full, which = weights[layer]
        pieces = gathered_stream(top, end)
        halo = token_halo(top, end)
        mix_in = value_rows(rank, place, pieces, halo, norm_gain, layer, sources)
        local, fwd_cum, bwd_cum, coef, edge = scanned(
            rank, mix_in, conv_taps, forget_rate, block_gates, layer, lax.axis_size("sp")
        )
        edges = lax.all_to_all(edge, "sp", 0, 0, tiled=True)
        gate_z, out_weight = gate_rows(rank, place, pieces, norm_gain, layer, sources, full, which)
        mixed, far_give, rest_give = given(
            place, edges, local, fwd_cum, bwd_cum, coef, gate_z, out_weight
        )
        far_away = across(far_give)
        rest_away = across(rest_give)
        far_keep, rest_keep = kept(mixed, out_weight)
        far = total_of(far_keep, far_away).astype(BF16)
        halves = (slice(0, half), slice(half, length))
        up, down, own = (
            [(rest_keep[n, rows], rest_away[n, rows]) for rows in halves] for n in range(3)
        )
        relay_top = along_x(far[:half], 1)
        relay_end = along_x(far[half:], -1)
        up_end = along_x(total_of(*up[1]).astype(BF16), 1)
        down_top = along_x(total_of(*down[0]).astype(BF16), -1)
        up_top = along_x(total_of(*up[0], relay_top).astype(BF16), 1)
        down_end = along_x(total_of(*down[1], relay_end).astype(BF16), -1)
        up_top, down_top, up_end, down_end = lax.optimization_barrier(
            (up_top, down_top, up_end, down_end)
        )
        top = total_of(top, *own[0], up_top, down_top).astype(BF16)
        end = total_of(end, *own[1], up_end, down_end).astype(BF16)
    return to_tokens(jnp.concatenate([top, end], axis=0))


def solution(mesh):
    placed = (
        P("sp", "tp"),
        P(),
        P(None, "sp", "tp"),
        P(None, "sp", "tp"),
        P(None, "sp", "tp"),
        P(),
        P(None, None, None, "tp", None),
        P(),
    )
    return jax.shard_map(
        per_device, mesh=mesh, in_specs=placed, out_specs=P("sp", "tp"), check_vma=False
    )
```

```python
import jax
import jax.numpy as jnp
from jax import lax
from jax.experimental import pallas as pl
from jax.experimental.pallas import tpu as pltpu
from jax.sharding import PartitionSpec as P


GATE_SCALE = 8.0
NORM_EPS = 1e-06
F32 = jnp.float32
BF16 = jnp.bfloat16


CHUNKS = 8
SCAN_LIMIT = 24 * 2**20
PROJECT_LIMIT = 56 * 2**20
FETCH_LIMIT = 50 * 2**20
GIVE_LIMIT = 12 * 2**20
KEEP_LIMIT = 8 * 2**20
HALO = 16


def to_tiles(array):
    rows, width = array.shape
    return array.reshape(CHUNKS, rows // CHUNKS, width).swapaxes(0, 1).reshape(rows, width)


def to_tokens(array):
    rows, width = array.shape
    return array.reshape(rows // CHUNKS, CHUNKS, width).swapaxes(0, 1).reshape(rows, width)


def shifted(array, axis, move):
    count = lax.axis_size(axis)
    return lax.ppermute(array, axis, [(i, move(i)) for i in range(count)])


def across(array):
    return shifted(array, "tp", lambda i: i ^ 1)


def along_x(array, step):
    return shifted(array, "tp", lambda i: (i + 2 * step) % 8)


def token_halo(top, end):
    rows, width = end.shape
    count = lax.axis_size("sp")
    owners = lax.axis_size("tp")
    ends = jnp.concatenate([end[rows - 9 : rows - 8], end[rows - 1 :], top[:1], top[:1]], axis=0)
    copies = jnp.broadcast_to(ends[None], (owners, *ends.shape))
    every = lax.all_to_all(copies, "tp", 0, 0, tiled=True)
    before = lax.ppermute(every[:, :2], "sp", [(i, i + 1) for i in range(count - 1)])
    after = lax.ppermute(every[:, 2:], "sp", [(i + 1, i) for i in range(count - 1)])
    rest = jnp.zeros((owners, HALO - 4, width), end.dtype)
    return jnp.concatenate([before, after, rest], axis=1)


def gathered_stream(top, end):
    left_top = along_x(top, 1)
    right_end = along_x(end, -1)
    left_end = along_x(end, 1)
    right_top = along_x(top, -1)
    far_top = along_x(left_top, 1)
    far_end = along_x(right_end, -1)
    same = (top, end, left_top, left_end, right_top, right_end, far_top, far_end)
    return same + tuple(across(part) for part in same)


def block_of(rank, dx, flip):
    core = rank % 2
    return 2 * ((rank // 2 + dx + 4) % 4) + (1 - core if flip else core)


SHIFTS = (0, -1, 1, 2)


def along_plane(array, axis, step):
    dz, dy = (step, 0) if axis == "z" else (0, step)
    pairs = [
        (4 * z + y, 4 * ((z + dz) % 4) + (y + dy) % 4) for z in range(4) for y in range(4)
    ]
    return lax.ppermute(array, "sp", pairs)


def around(array, axis):
    half = array.shape[0] // 2
    before = along_plane(array, axis, 1)
    after = along_plane(array, axis, -1)
    return (
        before,
        after,
        along_plane(before[:half], axis, 1),
        along_plane(after[half:], axis, -1),
    )


def gathered_pieces(weights):
    half = weights[0].shape[0] // 2
    pieces = []
    for at, (first, second) in ((0, "yz"), (half, "zy")):
        own = jnp.concatenate([w[at : at + half] for w in weights], axis=0)
        before, after, far_top, far_end = around(own, first)
        top = jnp.concatenate([own, before], axis=0)
        end = jnp.concatenate([after, far_top, far_end], axis=0)
        top_before = along_plane(top, second, 1)
        top_after = along_plane(top, second, -1)
        end_after = along_plane(end, second, -1)
        end_before = along_plane(end, second, 1)
        pieces += [top, end, top_before, end_before, top_after, end_after]
        pieces += [along_plane(top_before, second, 1), along_plane(end_after, second, -1)]
    return tuple(pieces)


def block_copies(weight, which, rank, offsets, target, sems):
    size = target.shape[1]
    copies = []
    for n, (dx, flip) in enumerate(offsets):
        at = pl.multiple_of(block_of(rank, dx, flip) * size, size)
        copies.append(
            pltpu.make_async_copy(
                weight.at[which, pl.ds(at, size), :], target.at[n], sems.at[n]
            )
        )
    return copies


def weight_copies(sources, which, place, target, sems):
    blocks, size, _ = target.shape
    if len(sources) == 1:
        return [
            pltpu.make_async_copy(
                sources[0].at[which, pl.ds(n * size, size), :], target.at[n], sems.at[n]
            )
            for n in range(blocks)
        ]
    copies = []
    rows = size // 4
    group = sources[0].shape[0] // 2
    for half in range(2):
        for outer in range(4):
            for inner in range(4):
                ref = sources[8 * half + 2 * outer + inner // 2]
                start = (inner % 2) * group
                dz, dy = (outer, inner) if half == 0 else (inner, outer)
                z = (place // 4 + 4 + SHIFTS[dz]) % 4
                y = (place % 4 + 4 + SHIFTS[dy]) % 4
                at = pl.multiple_of((y % 2) * (2 * rows) + half * rows, rows)
                copies.append(
                    pltpu.make_async_copy(
                        ref.at[pl.ds(start + which * rows, rows), :],
                        target.at[2 * z + y // 2, pl.ds(at, rows), :],
                        sems.at[len(copies)],
                    )
                )
    return copies


ARRIVE = [(dx, flip) for flip in (0, 1) for dx in (0, -1, 1, 2)]
LEAVE = [(dx, flip) for flip in (1, 0) for dx in (2, 1, -1, 0)]


def contracted(rows, weight, total):
    total[...] = jnp.zeros_like(total)

    def step(k, carry):
        left = jnp.concatenate([rows[2 * k], rows[2 * k + 1]], axis=1)
        right = jnp.concatenate([weight[2 * k], weight[2 * k + 1]], axis=0)
        total[...] += jnp.dot(left, right, preferred_element_type=F32)
        return carry

    lax.fori_loop(0, rows.shape[0] // 2, step, 0)


def row_scale(squares, width):
    return lax.rsqrt(jnp.sum(squares[...], axis=1, keepdims=True) / width + NORM_EPS)


def piece_copies(rank, pieces, rows, sems):
    half = pieces[0].shape[0]
    return [
        pltpu.make_async_copy(
            pieces[2 * k + side],
            rows.at[block_of(rank, dx, flip), pl.ds(side * half, half), :],
            sems.at[2 * k + side],
        )
        for k, (dx, flip) in enumerate(ARRIVE)
        for side in range(2)
    ]


def scaled_rows(layer, rank, gain, copies, halo, rows, squares):
    width = rows.shape[2]
    half = (rows.shape[1] - (0 if halo is None else HALO)) // 2
    step = 64
    for k, (dx, flip) in enumerate(ARRIVE):
        copies[2 * k].wait()
        copies[2 * k + 1].wait()
        block = block_of(rank, dx, flip)
        scale = gain[layer : layer + 1, pl.ds(pl.multiple_of(block * width, width), width)]

        def put(raw, at, k=k, block=block, scale=scale):
            raw = raw.astype(F32)
            rows[block, at, :] = (raw * scale).astype(BF16)
            power = raw * raw
            lanes = sum(power[:, 128 * q : 128 * (q + 1)] for q in range(width // 128))
            if k == 0:
                squares[at, :] = lanes
            else:
                squares[at, :] += lanes

        def chunk(n, carry, block=block, put=put):
            for side in range(2):
                at = pl.ds(pl.multiple_of(n * step + side * half, step), step)
                put(rows[block, at, :], at)
            return carry

        lax.fori_loop(0, half // step, chunk, 0)
        if halo is not None:
            put(halo[block], pl.ds(2 * half, HALO))


def project_body(layer, rank, place, gain, halo, *refs):
    pieces, sources = refs[:16], refs[16:-10]
    mix, gate, rows, squares, value_in, gate_in, total, sems, gate_sems, piece_sems = refs[-10:]
    values = weight_copies(sources, 0, place[0], value_in, sems)
    gates = weight_copies(sources, 1, place[0], gate_in, gate_sems)
    arriving = piece_copies(rank[0], pieces, rows, piece_sems)
    for copy in arriving + values:
        copy.start()
    scaled_rows(layer, rank[0], gain, arriving, halo, rows, squares)
    for copy in gates:
        copy.start()
    for copy in values:
        copy.wait()
    scale = row_scale(squares, mix.shape[1] * len(ARRIVE))
    contracted(rows, value_in, total)
    mix[...] = (total[...] * scale).astype(BF16)
    for copy in gates:
        copy.wait()
    contracted(rows, gate_in, total)
    gate[...] = (total[...] * scale)[: gate.shape[0]].astype(BF16)


def fetch_body(which, rank, after, weight, out, sems):
    copies = block_copies(weight, which, rank[0], LEAVE, out, sems)
    for copy in copies:
        copy.start()
    for copy in copies:
        copy.wait()


def in_smem():
    return pl.BlockSpec(memory_space=pltpu.SMEM)


def in_vmem():
    return pl.BlockSpec(memory_space=pltpu.VMEM)


def in_hbm():
    return pl.BlockSpec(memory_space=pltpu.HBM)


def product_cost(rows, width, count):
    return pl.CostEstimate(
        flops=2 * count * rows * width * width,
        bytes_accessed=2 * count * width * width,
        transcendentals=0,
    )


def projected(rank, place, pieces, halo, norm_gain, layer, sources):
    half, width = pieces[0].shape
    count = norm_gain.shape[1] // width
    deep = 2 * half + HALO
    return pl.pallas_call(
        lambda *refs: project_body(layer, *refs),
        out_shape=[
            jax.ShapeDtypeStruct((deep, width), BF16),
            jax.ShapeDtypeStruct((2 * half, width), BF16),
        ],
        in_specs=[in_smem()] * 2 + [in_vmem()] * 2 + [in_hbm()] * (16 + len(sources)),
        out_specs=[in_vmem()] * 2,
        scratch_shapes=[
            pltpu.VMEM((count, deep, width), BF16),
            pltpu.VMEM((deep, 128), F32),
            pltpu.VMEM((count, width, width), BF16),
            pltpu.VMEM((count, width, width), BF16),
            pltpu.VMEM((deep, width), F32),
            pltpu.SemaphoreType.DMA((32,)),
            pltpu.SemaphoreType.DMA((32,)),
            pltpu.SemaphoreType.DMA((16,)),
        ],
        compiler_params=pltpu.CompilerParams(vmem_limit_bytes=PROJECT_LIMIT),
        cost_estimate=product_cost(deep, width, 2 * count),
        name="projected",
    )(rank, place, norm_gain, halo, *pieces, *sources)


def fetched(rank, after, weights, which):
    width = weights.shape[2]
    count = weights.shape[1] // width
    return pl.pallas_call(
        lambda *refs: fetch_body(which, *refs),
        out_shape=jax.ShapeDtypeStruct((count, width, width), BF16),
        in_specs=[in_smem(), in_vmem(), in_hbm()],
        out_specs=in_vmem(),
        scratch_shapes=[pltpu.SemaphoreType.DMA((count,))],
        compiler_params=pltpu.CompilerParams(vmem_limit_bytes=FETCH_LIMIT),
        cost_estimate=product_cost(width, width, count),
        name="fetched",
    )(rank, after, weights)


def scan_body(
    rank, mix, taps, rate, gates, local, fwd_cum, bwd_cum, coef, edge, padded, conv, pre
):
    steps = conv.shape[0] // CHUNKS
    length = conv.shape[0]
    sub = lax.broadcasted_iota(jnp.int32, (CHUNKS, 128), 0)
    rows = mix[...].astype(F32)
    halo = rows[length : length + 8]
    padded[16 : 16 + length] = rows[:length]
    padded[0:8] = jnp.where(
        sub == 0, halo[0:1], pltpu.roll(rows[length - 16 : length - 8], 1, axis=0)
    )
    padded[8:16] = jnp.where(sub == 0, halo[1:2], pltpu.roll(rows[length - 8 : length], 1, axis=0))
    padded[16 + length : 24 + length] = jnp.where(
        sub == CHUNKS - 1, halo[2:3], pltpu.roll(rows[0:8], CHUNKS - 1, axis=0)
    )
    for part in range(8):
        lo = part * (length // 8)
        hi = lo + length // 8
        conv[lo:hi] = sum(padded[lo + 8 * k : hi + 8 * k] * taps[0, k : k + 1] for k in range(4))
    lhs = conv[...].astype(BF16)
    for g in range(4):
        pre[g] = jnp.dot(lhs, gates[0, g // 2, g % 2], preferred_element_type=F32)

    def cell(i, e):
        at = pl.ds(pl.multiple_of(i * CHUNKS, CHUNKS), CHUNKS)
        recur = jax.nn.sigmoid(pre[2 * e, at, :])
        entry = jax.nn.sigmoid(pre[2 * e + 1, at, :])
        log_a = (-GATE_SCALE) * recur * rate[0, e : e + 1]
        decay = jnp.exp(log_a)
        x = 2.0 * log_a
        near = x * (1.0 + x * (0.5 + x * (1.0 / 6 + x * (1.0 / 24 + x * (1.0 / 120)))))
        room = -jnp.where(x > -0.125, near, decay * decay - 1.0)
        return at, decay, jnp.sqrt(room) * entry * conv[at, :]

    zero = jnp.zeros((CHUNKS, 128), F32)
    one = jnp.ones((CHUNKS, 128), F32)
    inner = 8

    def forward(block, carry):
        state, cum = carry
        for n in range(inner):
            at, decay, drive = cell(block * inner + n, 0)
            state = decay * state + drive
            cum = decay * cum
            local[at, :] = state
            fwd_cum[at, :] = cum
        return state, cum

    def backward(block, carry):
        state, cum = carry
        for n in range(inner):
            at, decay, drive = cell(steps - 1 - (block * inner + n), 1)
            state = decay * state + drive
            cum = decay * cum
            local[at, :] += state
            bwd_cum[at, :] = cum
        return state, cum

    state_f, cum_f = lax.fori_loop(0, steps // inner, forward, (zero, one))
    state_b, cum_b = lax.fori_loop(0, steps // inner, backward, (zero, one))
    alpha = jnp.zeros((1, 128), F32)
    beta = jnp.ones((1, 128), F32)
    for s in range(CHUNKS):
        coef[0, s : s + 1] = alpha
        coef[1, s : s + 1] = beta
        alpha = state_f[s : s + 1] + cum_f[s : s + 1] * alpha
        beta = cum_f[s : s + 1] * beta
    sums_f = (beta, alpha)
    alpha = jnp.zeros((1, 128), F32)
    beta = jnp.ones((1, 128), F32)
    for s in reversed(range(CHUNKS)):
        coef[2, s : s + 1] = alpha
        coef[3, s : s + 1] = beta
        alpha = state_b[s : s + 1] + cum_b[s : s + 1] * alpha
        beta = cum_b[s : s + 1] * beta
    edge[...] = jnp.broadcast_to(
        jnp.concatenate([*sums_f, beta, alpha], axis=0)[None], edge.shape
    )


def scanned(rank, mix, conv_taps, forget_rate, block_gates, layer, copies):
    deep, width = mix.shape
    length = deep - HALO
    blocks = width // 128
    column = lambda b, rank: (0, b)
    owned = lambda b, rank: (layer, 0, rank[0] * blocks + b)
    return pl.pallas_call(
        scan_body,
        grid_spec=pltpu.PrefetchScalarGridSpec(
            num_scalar_prefetch=1,
            grid=(blocks,),
            in_specs=[
                pl.BlockSpec((deep, 128), column),
                pl.BlockSpec((1, 4, 128), owned),
                pl.BlockSpec((1, 2, 128), owned),
                pl.BlockSpec((1, 2, 2, 128, 128), lambda b, rank: (layer, 0, 0, b, 0)),
            ],
            out_specs=[
                pl.BlockSpec((length, 128), column),
                pl.BlockSpec((length, 128), column),
                pl.BlockSpec((length, 128), column),
                pl.BlockSpec((4, CHUNKS, 128), lambda b, rank: (0, 0, b)),
                pl.BlockSpec((copies, 4, 128), lambda b, rank: (0, 0, b)),
            ],
            scratch_shapes=[
                pltpu.VMEM((length + 24, 128), F32),
                pltpu.VMEM((length, 128), F32),
                pltpu.VMEM((4, length, 128), F32),
            ],
        ),
        out_shape=[
            jax.ShapeDtypeStruct((length, width), F32),
            jax.ShapeDtypeStruct((length, width), F32),
            jax.ShapeDtypeStruct((length, width), F32),
            jax.ShapeDtypeStruct((4, CHUNKS, width), F32),
            jax.ShapeDtypeStruct((copies, 4, width), F32),
        ],
        compiler_params=pltpu.CompilerParams(vmem_limit_bytes=SCAN_LIMIT),
        cost_estimate=pl.CostEstimate(
            flops=10_000_000_000, bytes_accessed=4_000_000, transcendentals=4_000_000
        ),
        name="scan",
    )(rank, mix, conv_taps, forget_rate, block_gates)


def features(mixed, weight):
    return lax.dot_general(
        mixed, weight, (((1,), (1,)), ((), ())), preferred_element_type=F32
    ).astype(BF16)


def give_body(
    place, edges, local, fwd_cum, bwd_cum, coef, gate, weight, mixed, far, rest
):
    mine = place[0]
    count, _, width = edges.shape
    enter_f = jnp.zeros((1, width), F32)
    enter_b = jnp.zeros((1, width), F32)
    for r in range(count):
        enter_f = jnp.where(r < mine, edges[r, 1:2] + edges[r, 0:1] * enter_f, enter_f)
        q = count - 1 - r
        enter_b = jnp.where(q > mine, edges[q, 3:4] + edges[q, 2:3] * enter_b, enter_b)
    from_f = coef[0] + coef[1] * enter_f
    from_b = coef[2] + coef[3] * enter_b
    group = 64
    for c in range(width // 128):
        col = slice(128 * c, 128 * (c + 1))
        tiled_f = jnp.concatenate([from_f[:, col]] * (group // CHUNKS), axis=0)
        tiled_b = jnp.concatenate([from_b[:, col]] * (group // CHUNKS), axis=0)

        def part(n, carry, col=col, tiled_f=tiled_f, tiled_b=tiled_b):
            at = pl.ds(pl.multiple_of(n * group, group), group)
            both = local[at, col] + fwd_cum[at, col] * tiled_f + bwd_cum[at, col] * tiled_b
            z = gate[at, col].astype(F32)
            mixed[at, col] = (both * (z * jax.nn.sigmoid(z))).astype(BF16)
            return carry

        lax.fori_loop(0, local.shape[0] // group, part, 0)
    far[...] = features(mixed[...], weight[0])

    def step(n, carry):
        rest[n] = features(mixed[...], weight[n + 1])
        return carry

    lax.fori_loop(0, 3, step, 0)


def given(place, edges, local, fwd_cum, bwd_cum, coef, gate, weight):
    length, width = local.shape
    return pl.pallas_call(
        give_body,
        in_specs=[in_smem()] + [in_vmem()] * 7,
        out_specs=[in_vmem()] * 3,
        out_shape=[
            jax.ShapeDtypeStruct((length, width), BF16),
            jax.ShapeDtypeStruct((length, width), BF16),
            jax.ShapeDtypeStruct((3, length, width), BF16),
        ],
        compiler_params=pltpu.CompilerParams(vmem_limit_bytes=GIVE_LIMIT),
        cost_estimate=product_cost(length, width, 4),
        name="given",
    )(place, edges, local, fwd_cum, bwd_cum, coef, gate, weight)


def keep_body(mixed, weight, far, rest):
    far[...] = features(mixed[...], weight[4])

    def step(n, carry):
        rest[n] = features(mixed[...], weight[n + 5])
        return carry

    lax.fori_loop(0, 3, step, 0)


def kept(mixed, weight):
    length, width = mixed.shape
    return pl.pallas_call(
        keep_body,
        in_specs=[in_vmem()] * 2,
        out_specs=[in_vmem()] * 2,
        out_shape=[
            jax.ShapeDtypeStruct((length, width), BF16),
            jax.ShapeDtypeStruct((3, length, width), BF16),
        ],
        compiler_params=pltpu.CompilerParams(vmem_limit_bytes=KEEP_LIMIT),
        cost_estimate=product_cost(length, width, 4),
        name="kept",
    )(mixed, weight)


def total_of(*parts):
    return sum(part.astype(F32) for part in parts)


def per_device(
    stream_in, norm_gain, value_proj, gate_proj, out_proj, conv_taps, block_gates, forget_rate
):
    rank = lax.axis_index("tp").reshape(1)
    place = lax.axis_index("sp").reshape(1)
    length, _ = stream_in.shape
    half = length // 2
    stream = to_tiles(stream_in)
    top, end = stream[:half], stream[half:]
    pieces_0 = gathered_pieces([value_proj[0], gate_proj[0]])
    outs_0 = lax.all_gather(out_proj[:1], "sp", axis=1, tiled=True)
    held = jnp.stack([value_proj[1], gate_proj[1], out_proj[1]])
    full_1 = lax.all_gather(held, "sp", axis=1, tiled=True)
    weights = [(pieces_0, outs_0, 0), ((full_1,), full_1, 2)]
    for layer in range(value_proj.shape[0]):
        sources, full, which = weights[layer]
        pieces = gathered_stream(top, end)
        halo = token_halo(top, end)
        mix_in, gate_z = projected(rank, place, pieces, halo, norm_gain, layer, sources)
        local, fwd_cum, bwd_cum, coef, edge = scanned(
            rank, mix_in, conv_taps, forget_rate, block_gates, layer, lax.axis_size("sp")
        )
        edges = lax.all_to_all(edge, "sp", 0, 0, tiled=True)
        out_weight = fetched(rank, coef, full, which)
        mixed, far_give, rest_give = given(
            place, edges, local, fwd_cum, bwd_cum, coef, gate_z, out_weight
        )
        far_away = across(far_give)
        rest_away = across(rest_give)
        far_keep, rest_keep = kept(mixed, out_weight)
        far = total_of(far_keep, far_away).astype(BF16)
        halves = (slice(0, half), slice(half, length))
        up, down, own = (
            [(rest_keep[n, rows], rest_away[n, rows]) for rows in halves] for n in range(3)
        )
        relay_top = along_x(far[:half], 1)
        relay_end = along_x(far[half:], -1)
        up_end = along_x(total_of(*up[1]).astype(BF16), 1)
        down_top = along_x(total_of(*down[0]).astype(BF16), -1)
        up_top = along_x(total_of(*up[0], relay_top).astype(BF16), 1)
        down_end = along_x(total_of(*down[1], relay_end).astype(BF16), -1)
        up_top, down_top, up_end, down_end = lax.optimization_barrier(
            (up_top, down_top, up_end, down_end)
        )
        top = total_of(top, *own[0], up_top, down_top).astype(BF16)
        end = total_of(end, *own[1], up_end, down_end).astype(BF16)
    return to_tokens(jnp.concatenate([top, end], axis=0))


def solution(mesh):
    placed = (
        P("sp", "tp"),
        P(),
        P(None, "sp", "tp"),
        P(None, "sp", "tp"),
        P(None, "sp", "tp"),
        P(),
        P(None, None, None, "tp", None),
        P(),
    )
    return jax.shard_map(
        per_device, mesh=mesh, in_specs=placed, out_specs=P("sp", "tp"), check_vma=False
    )
```

```python
import jax
import jax.numpy as jnp
from jax import lax
from jax.experimental import pallas as pl
from jax.experimental.pallas import tpu as pltpu
from jax.sharding import PartitionSpec as P


GATE_SCALE = 8.0
NORM_EPS = 1e-06
F32 = jnp.float32
BF16 = jnp.bfloat16


CHUNKS = 8
SCAN_LIMIT = 24 * 2**20
PROJECT_LIMIT = 56 * 2**20
FETCH_LIMIT = 50 * 2**20
GIVE_LIMIT = 12 * 2**20
KEEP_LIMIT = 8 * 2**20
HALO = 16


def to_tiles(array):
    rows, width = array.shape
    return array.reshape(CHUNKS, rows // CHUNKS, width).swapaxes(0, 1).reshape(rows, width)


def to_tokens(array):
    rows, width = array.shape
    return array.reshape(rows // CHUNKS, CHUNKS, width).swapaxes(0, 1).reshape(rows, width)


def shifted(array, axis, move):
    count = lax.axis_size(axis)
    return lax.ppermute(array, axis, [(i, move(i)) for i in range(count)])


def across(array):
    return shifted(array, "tp", lambda i: i ^ 1)


def along_x(array, step):
    return shifted(array, "tp", lambda i: (i + 2 * step) % 8)


def token_halo(top, end):
    rows, width = end.shape
    count = lax.axis_size("sp")
    owners = lax.axis_size("tp")
    ends = jnp.concatenate([end[rows - 9 : rows - 8], end[rows - 1 :], top[:1], top[:1]], axis=0)
    copies = jnp.broadcast_to(ends[None], (owners, *ends.shape))
    every = lax.all_to_all(copies, "tp", 0, 0, tiled=True)
    before = lax.ppermute(every[:, :2], "sp", [(i, i + 1) for i in range(count - 1)])
    after = lax.ppermute(every[:, 2:], "sp", [(i + 1, i) for i in range(count - 1)])
    rest = jnp.zeros((owners, HALO - 4, width), end.dtype)
    return jnp.concatenate([before, after, rest], axis=1)


def gathered_stream(top, end):
    left_top = along_x(top, 1)
    right_end = along_x(end, -1)
    left_end = along_x(end, 1)
    right_top = along_x(top, -1)
    far_top = along_x(left_top, 1)
    far_end = along_x(right_end, -1)
    same = (top, end, left_top, left_end, right_top, right_end, far_top, far_end)
    return same + tuple(across(part) for part in same)


def block_of(rank, dx, flip):
    core = rank % 2
    return 2 * ((rank // 2 + dx + 4) % 4) + (1 - core if flip else core)


SHIFTS = (0, -1, 1, 2)


def along_plane(array, axis, step):
    dz, dy = (step, 0) if axis == "z" else (0, step)
    pairs = [
        (4 * z + y, 4 * ((z + dz) % 4) + (y + dy) % 4) for z in range(4) for y in range(4)
    ]
    return lax.ppermute(array, "sp", pairs)


def gathered_pieces(weights):
    half = weights[0].shape[0] // 2
    pieces = []
    for turn, (first, second) in enumerate(("yz", "zy")):
        own = jnp.concatenate([w[turn * half : (turn + 1) * half] for w in weights], axis=0)
        part = own.shape[0] // 2
        before = along_plane(own, first, 1)
        after = along_plane(own, first, -1)
        far_top = along_plane(before[:part], first, 1)
        far_end = along_plane(after[part:], first, -1)
        top = jnp.concatenate([own, before], axis=0)
        end = jnp.concatenate([after, far_top, far_end], axis=0)
        top_before = along_plane(top, second, 1)
        top_after = along_plane(top, second, -1)
        end_after = along_plane(end, second, -1)
        end_before = along_plane(end, second, 1)
        pieces += [top, end, top_before, end_before, top_after, end_after]
        pieces += [along_plane(top_before, second, 1), along_plane(end_after, second, -1)]
    return tuple(pieces)


def block_copies(weight, which, rank, offsets, target, sems):
    size = target.shape[1]
    copies = []
    for n, (dx, flip) in enumerate(offsets):
        at = pl.multiple_of(block_of(rank, dx, flip) * size, size)
        copies.append(
            pltpu.make_async_copy(
                weight.at[which, pl.ds(at, size), :], target.at[n], sems.at[n]
            )
        )
    return copies


def weight_copies(sources, which, place, target, sems):
    blocks, size, _ = target.shape
    if len(sources) == 1:
        return [
            pltpu.make_async_copy(
                sources[0].at[which, pl.ds(n * size, size), :], target.at[n], sems.at[n]
            )
            for n in range(blocks)
        ]
    copies = []
    rows = size // 4
    group = sources[0].shape[0] // 2
    for half in range(2):
        for outer in range(4):
            for inner in range(4):
                ref = sources[8 * half + 2 * outer + inner // 2]
                start = (inner % 2) * group
                dz, dy = (outer, inner) if half == 0 else (inner, outer)
                z = (place // 4 + 4 + SHIFTS[dz]) % 4
                y = (place % 4 + 4 + SHIFTS[dy]) % 4
                at = pl.multiple_of((y % 2) * (2 * rows) + half * rows, rows)
                copies.append(
                    pltpu.make_async_copy(
                        ref.at[pl.ds(start + which * rows, rows), :],
                        target.at[2 * z + y // 2, pl.ds(at, rows), :],
                        sems.at[len(copies)],
                    )
                )
    return copies


ARRIVE = [(dx, flip) for flip in (0, 1) for dx in (0, -1, 1, 2)]
LEAVE = [(dx, flip) for flip in (1, 0) for dx in (2, 1, -1, 0)]


def contracted(rows, weight, total):
    total[...] = jnp.zeros_like(total)

    def step(k, carry):
        left = jnp.concatenate([rows[2 * k], rows[2 * k + 1]], axis=1)
        right = jnp.concatenate([weight[2 * k], weight[2 * k + 1]], axis=0)
        total[...] += jnp.dot(left, right, preferred_element_type=F32)
        return carry

    lax.fori_loop(0, rows.shape[0] // 2, step, 0)


def row_scale(squares, width):
    return lax.rsqrt(jnp.sum(squares[...], axis=1, keepdims=True) / width + NORM_EPS)


def piece_copies(rank, pieces, rows, sems):
    half = pieces[0].shape[0]
    return [
        pltpu.make_async_copy(
            pieces[2 * k + side],
            rows.at[block_of(rank, dx, flip), pl.ds(side * half, half), :],
            sems.at[2 * k + side],
        )
        for k, (dx, flip) in enumerate(ARRIVE)
        for side in range(2)
    ]


def scaled_rows(layer, rank, gain, copies, halo, rows, squares):
    width = rows.shape[2]
    half = (rows.shape[1] - (0 if halo is None else HALO)) // 2
    step = 64
    for k, (dx, flip) in enumerate(ARRIVE):
        copies[2 * k].wait()
        copies[2 * k + 1].wait()
        block = block_of(rank, dx, flip)
        scale = gain[layer : layer + 1, pl.ds(pl.multiple_of(block * width, width), width)]

        def put(raw, at, k=k, block=block, scale=scale):
            raw = raw.astype(F32)
            rows[block, at, :] = (raw * scale).astype(BF16)
            power = raw * raw
            lanes = sum(power[:, 128 * q : 128 * (q + 1)] for q in range(width // 128))
            if k == 0:
                squares[at, :] = lanes
            else:
                squares[at, :] += lanes

        def chunk(n, carry, block=block, put=put):
            for side in range(2):
                at = pl.ds(pl.multiple_of(n * step + side * half, step), step)
                put(rows[block, at, :], at)
            return carry

        lax.fori_loop(0, half // step, chunk, 0)
        if halo is not None:
            put(halo[block], pl.ds(2 * half, HALO))


def project_body(layer, rank, place, gain, halo, *refs):
    pieces, sources = refs[:16], refs[16:-10]
    mix, gate, rows, squares, value_in, gate_in, total, sems, gate_sems, piece_sems = refs[-10:]
    values = weight_copies(sources, 0, place[0], value_in, sems)
    gates = weight_copies(sources, 1, place[0], gate_in, gate_sems)
    arriving = piece_copies(rank[0], pieces, rows, piece_sems)
    for copy in arriving + values:
        copy.start()
    scaled_rows(layer, rank[0], gain, arriving, halo, rows, squares)
    for copy in gates:
        copy.start()
    for copy in values:
        copy.wait()
    scale = row_scale(squares, mix.shape[1] * len(ARRIVE))
    contracted(rows, value_in, total)
    mix[...] = (total[...] * scale).astype(BF16)
    for copy in gates:
        copy.wait()
    contracted(rows, gate_in, total)
    gate[...] = (total[...] * scale)[: gate.shape[0]].astype(BF16)


def fetch_body(which, rank, after, weight, out, sems):
    copies = block_copies(weight, which, rank[0], LEAVE, out, sems)
    for copy in copies:
        copy.start()
    for copy in copies:
        copy.wait()


def in_smem():
    return pl.BlockSpec(memory_space=pltpu.SMEM)


def in_vmem():
    return pl.BlockSpec(memory_space=pltpu.VMEM)


def in_hbm():
    return pl.BlockSpec(memory_space=pltpu.HBM)


def product_cost(rows, width, count):
    return pl.CostEstimate(
        flops=2 * count * rows * width * width,
        bytes_accessed=2 * count * width * width,
        transcendentals=0,
    )


def projected(rank, place, pieces, halo, norm_gain, layer, sources):
    half, width = pieces[0].shape
    count = norm_gain.shape[1] // width
    deep = 2 * half + HALO
    return pl.pallas_call(
        lambda *refs: project_body(layer, *refs),
        out_shape=[
            jax.ShapeDtypeStruct((deep, width), BF16),
            jax.ShapeDtypeStruct((2 * half, width), BF16),
        ],
        in_specs=[in_smem()] * 2 + [in_vmem()] * 2 + [in_hbm()] * (16 + len(sources)),
        out_specs=[in_vmem()] * 2,
        scratch_shapes=[
            pltpu.VMEM((count, deep, width), BF16),
            pltpu.VMEM((deep, 128), F32),
            pltpu.VMEM((count, width, width), BF16),
            pltpu.VMEM((count, width, width), BF16),
            pltpu.VMEM((deep, width), F32),
            pltpu.SemaphoreType.DMA((32,)),
            pltpu.SemaphoreType.DMA((32,)),
            pltpu.SemaphoreType.DMA((16,)),
        ],
        compiler_params=pltpu.CompilerParams(vmem_limit_bytes=PROJECT_LIMIT),
        cost_estimate=product_cost(deep, width, 2 * count),
        name="projected",
    )(rank, place, norm_gain, halo, *pieces, *sources)


def fetched(rank, after, weights, which):
    width = weights.shape[2]
    count = weights.shape[1] // width
    return pl.pallas_call(
        lambda *refs: fetch_body(which, *refs),
        out_shape=jax.ShapeDtypeStruct((count, width, width), BF16),
        in_specs=[in_smem(), in_vmem(), in_hbm()],
        out_specs=in_vmem(),
        scratch_shapes=[pltpu.SemaphoreType.DMA((count,))],
        compiler_params=pltpu.CompilerParams(vmem_limit_bytes=FETCH_LIMIT),
        cost_estimate=product_cost(width, width, count),
        name="fetched",
    )(rank, after, weights)


def scan_body(
    rank, mix, taps, rate, gates, local, fwd_cum, bwd_cum, coef, edge, padded, conv, pre
):
    steps = conv.shape[0] // CHUNKS
    length = conv.shape[0]
    sub = lax.broadcasted_iota(jnp.int32, (CHUNKS, 128), 0)
    rows = mix[...].astype(F32)
    halo = rows[length : length + 8]
    padded[16 : 16 + length] = rows[:length]
    padded[0:8] = jnp.where(
        sub == 0, halo[0:1], pltpu.roll(rows[length - 16 : length - 8], 1, axis=0)
    )
    padded[8:16] = jnp.where(sub == 0, halo[1:2], pltpu.roll(rows[length - 8 : length], 1, axis=0))
    padded[16 + length : 24 + length] = jnp.where(
        sub == CHUNKS - 1, halo[2:3], pltpu.roll(rows[0:8], CHUNKS - 1, axis=0)
    )
    for part in range(8):
        lo = part * (length // 8)
        hi = lo + length // 8
        conv[lo:hi] = sum(padded[lo + 8 * k : hi + 8 * k] * taps[0, k : k + 1] for k in range(4))
    lhs = conv[...].astype(BF16)
    for g in range(4):
        pre[g] = jnp.dot(lhs, gates[0, g // 2, g % 2], preferred_element_type=F32)

    def cell(i, e):
        at = pl.ds(pl.multiple_of(i * CHUNKS, CHUNKS), CHUNKS)
        recur = jax.nn.sigmoid(pre[2 * e, at, :])
        entry = jax.nn.sigmoid(pre[2 * e + 1, at, :])
        log_a = (-GATE_SCALE) * recur * rate[0, e : e + 1]
        decay = jnp.exp(log_a)
        x = 2.0 * log_a
        near = x * (1.0 + x * (0.5 + x * (1.0 / 6 + x * (1.0 / 24 + x * (1.0 / 120)))))
        room = -jnp.where(x > -0.125, near, decay * decay - 1.0)
        return at, decay, jnp.sqrt(room) * entry * conv[at, :]

    zero = jnp.zeros((CHUNKS, 128), F32)
    one = jnp.ones((CHUNKS, 128), F32)
    inner = 8

    def forward(block, carry):
        state, cum = carry
        for n in range(inner):
            at, decay, drive = cell(block * inner + n, 0)
            state = decay * state + drive
            cum = decay * cum
            local[at, :] = state
            fwd_cum[at, :] = cum
        return state, cum

    def backward(block, carry):
        state, cum = carry
        for n in range(inner):
            at, decay, drive = cell(steps - 1 - (block * inner + n), 1)
            state = decay * state + drive
            cum = decay * cum
            local[at, :] += state
            bwd_cum[at, :] = cum
        return state, cum

    state_f, cum_f = lax.fori_loop(0, steps // inner, forward, (zero, one))
    state_b, cum_b = lax.fori_loop(0, steps // inner, backward, (zero, one))
    alpha = jnp.zeros((1, 128), F32)
    beta = jnp.ones((1, 128), F32)
    for s in range(CHUNKS):
        coef[0, s : s + 1] = alpha
        coef[1, s : s + 1] = beta
        alpha = state_f[s : s + 1] + cum_f[s : s + 1] * alpha
        beta = cum_f[s : s + 1] * beta
    sums_f = (beta, alpha)
    alpha = jnp.zeros((1, 128), F32)
    beta = jnp.ones((1, 128), F32)
    for s in reversed(range(CHUNKS)):
        coef[2, s : s + 1] = alpha
        coef[3, s : s + 1] = beta
        alpha = state_b[s : s + 1] + cum_b[s : s + 1] * alpha
        beta = cum_b[s : s + 1] * beta
    edge[...] = jnp.broadcast_to(
        jnp.concatenate([*sums_f, beta, alpha], axis=0)[None], edge.shape
    )


def scanned(rank, mix, conv_taps, forget_rate, block_gates, layer, copies):
    deep, width = mix.shape
    length = deep - HALO
    blocks = width // 128
    column = lambda b, rank: (0, b)
    owned = lambda b, rank: (layer, 0, rank[0] * blocks + b)
    return pl.pallas_call(
        scan_body,
        grid_spec=pltpu.PrefetchScalarGridSpec(
            num_scalar_prefetch=1,
            grid=(blocks,),
            in_specs=[
                pl.BlockSpec((deep, 128), column),
                pl.BlockSpec((1, 4, 128), owned),
                pl.BlockSpec((1, 2, 128), owned),
                pl.BlockSpec((1, 2, 2, 128, 128), lambda b, rank: (layer, 0, 0, b, 0)),
            ],
            out_specs=[
                pl.BlockSpec((length, 128), column),
                pl.BlockSpec((length, 128), column),
                pl.BlockSpec((length, 128), column),
                pl.BlockSpec((4, CHUNKS, 128), lambda b, rank: (0, 0, b)),
                pl.BlockSpec((copies, 4, 128), lambda b, rank: (0, 0, b)),
            ],
            scratch_shapes=[
                pltpu.VMEM((length + 24, 128), F32),
                pltpu.VMEM((length, 128), F32),
                pltpu.VMEM((4, length, 128), F32),
            ],
        ),
        out_shape=[
            jax.ShapeDtypeStruct((length, width), F32),
            jax.ShapeDtypeStruct((length, width), F32),
            jax.ShapeDtypeStruct((length, width), F32),
            jax.ShapeDtypeStruct((4, CHUNKS, width), F32),
            jax.ShapeDtypeStruct((copies, 4, width), F32),
        ],
        compiler_params=pltpu.CompilerParams(vmem_limit_bytes=SCAN_LIMIT),
        cost_estimate=pl.CostEstimate(
            flops=10_000_000_000, bytes_accessed=4_000_000, transcendentals=4_000_000
        ),
        name="scan",
    )(rank, mix, conv_taps, forget_rate, block_gates)


def features(mixed, weight):
    return lax.dot_general(
        mixed, weight, (((1,), (1,)), ((), ())), preferred_element_type=F32
    ).astype(BF16)


def give_body(
    place, edges, local, fwd_cum, bwd_cum, coef, gate, weight, mixed, far, rest
):
    mine = place[0]
    count, _, width = edges.shape
    enter_f = jnp.zeros((1, width), F32)
    enter_b = jnp.zeros((1, width), F32)
    for r in range(count):
        enter_f = jnp.where(r < mine, edges[r, 1:2] + edges[r, 0:1] * enter_f, enter_f)
        q = count - 1 - r
        enter_b = jnp.where(q > mine, edges[q, 3:4] + edges[q, 2:3] * enter_b, enter_b)
    from_f = coef[0] + coef[1] * enter_f
    from_b = coef[2] + coef[3] * enter_b
    group = 64
    for c in range(width // 128):
        col = slice(128 * c, 128 * (c + 1))
        tiled_f = jnp.concatenate([from_f[:, col]] * (group // CHUNKS), axis=0)
        tiled_b = jnp.concatenate([from_b[:, col]] * (group // CHUNKS), axis=0)

        def part(n, carry, col=col, tiled_f=tiled_f, tiled_b=tiled_b):
            at = pl.ds(pl.multiple_of(n * group, group), group)
            both = local[at, col] + fwd_cum[at, col] * tiled_f + bwd_cum[at, col] * tiled_b
            z = gate[at, col].astype(F32)
            mixed[at, col] = (both * (z * jax.nn.sigmoid(z))).astype(BF16)
            return carry

        lax.fori_loop(0, local.shape[0] // group, part, 0)
    far[...] = features(mixed[...], weight[0])

    def step(n, carry):
        rest[n] = features(mixed[...], weight[n + 1])
        return carry

    lax.fori_loop(0, 3, step, 0)


def given(place, edges, local, fwd_cum, bwd_cum, coef, gate, weight):
    length, width = local.shape
    return pl.pallas_call(
        give_body,
        in_specs=[in_smem()] + [in_vmem()] * 7,
        out_specs=[in_vmem()] * 3,
        out_shape=[
            jax.ShapeDtypeStruct((length, width), BF16),
            jax.ShapeDtypeStruct((length, width), BF16),
            jax.ShapeDtypeStruct((3, length, width), BF16),
        ],
        compiler_params=pltpu.CompilerParams(vmem_limit_bytes=GIVE_LIMIT),
        cost_estimate=product_cost(length, width, 4),
        name="given",
    )(place, edges, local, fwd_cum, bwd_cum, coef, gate, weight)


def keep_body(mixed, weight, far, rest):
    far[...] = features(mixed[...], weight[4])

    def step(n, carry):
        rest[n] = features(mixed[...], weight[n + 5])
        return carry

    lax.fori_loop(0, 3, step, 0)


def kept(mixed, weight):
    length, width = mixed.shape
    return pl.pallas_call(
        keep_body,
        in_specs=[in_vmem()] * 2,
        out_specs=[in_vmem()] * 2,
        out_shape=[
            jax.ShapeDtypeStruct((length, width), BF16),
            jax.ShapeDtypeStruct((3, length, width), BF16),
        ],
        compiler_params=pltpu.CompilerParams(vmem_limit_bytes=KEEP_LIMIT),
        cost_estimate=product_cost(length, width, 4),
        name="kept",
    )(mixed, weight)


def total_of(*parts):
    return sum(part.astype(F32) for part in parts)


def per_device(
    stream_in, norm_gain, value_proj, gate_proj, out_proj, conv_taps, block_gates, forget_rate
):
    rank = lax.axis_index("tp").reshape(1)
    place = lax.axis_index("sp").reshape(1)
    length, _ = stream_in.shape
    half = length // 2
    stream = to_tiles(stream_in)
    top, end = stream[:half], stream[half:]
    pieces_0 = gathered_pieces([value_proj[0], gate_proj[0]])
    outs_0 = lax.all_gather(out_proj[:1], "sp", axis=1, tiled=True)
    held = jnp.stack([value_proj[1], gate_proj[1], out_proj[1]])
    full_1 = lax.all_gather(held, "sp", axis=1, tiled=True)
    weights = [(pieces_0, outs_0, 0), ((full_1,), full_1, 2)]
    for layer in range(value_proj.shape[0]):
        sources, full, which = weights[layer]
        pieces = gathered_stream(top, end)
        halo = token_halo(top, end)
        mix_in, gate_z = projected(rank, place, pieces, halo, norm_gain, layer, sources)
        local, fwd_cum, bwd_cum, coef, edge = scanned(
            rank, mix_in, conv_taps, forget_rate, block_gates, layer, lax.axis_size("sp")
        )
        edges = lax.all_to_all(edge, "sp", 0, 0, tiled=True)
        out_weight = fetched(rank, coef, full, which)
        mixed, far_give, rest_give = given(
            place, edges, local, fwd_cum, bwd_cum, coef, gate_z, out_weight
        )
        far_away = across(far_give)
        rest_away = across(rest_give)
        far_keep, rest_keep = kept(mixed, out_weight)
        far = total_of(far_keep, far_away).astype(BF16)
        halves = (slice(0, half), slice(half, length))
        up, down, own = (
            [(rest_keep[n, rows], rest_away[n, rows]) for rows in halves] for n in range(3)
        )
        relay_top = along_x(far[:half], 1)
        relay_end = along_x(far[half:], -1)
        up_end = along_x(total_of(*up[1]).astype(BF16), 1)
        down_top = along_x(total_of(*down[0]).astype(BF16), -1)
        up_top = along_x(total_of(*up[0], relay_top).astype(BF16), 1)
        down_end = along_x(total_of(*down[1], relay_end).astype(BF16), -1)
        up_top, down_top, up_end, down_end = lax.optimization_barrier(
            (up_top, down_top, up_end, down_end)
        )
        top = total_of(top, *own[0], up_top, down_top).astype(BF16)
        end = total_of(end, *own[1], up_end, down_end).astype(BF16)
    return to_tokens(jnp.concatenate([top, end], axis=0))


def solution(mesh):
    placed = (
        P("sp", "tp"),
        P(),
        P(None, "sp", "tp"),
        P(None, "sp", "tp"),
        P(None, "sp", "tp"),
        P(),
        P(None, None, None, "tp", None),
        P(),
    )
    return jax.shard_map(
        per_device, mesh=mesh, in_specs=placed, out_specs=P("sp", "tp"), check_vma=False
    )
```

```python
import jax
import jax.numpy as jnp
from jax import lax
from jax.experimental import pallas as pl
from jax.experimental.pallas import tpu as pltpu
from jax.sharding import PartitionSpec as P


GATE_SCALE = 8.0
NORM_EPS = 1e-06
F32 = jnp.float32
BF16 = jnp.bfloat16


CHUNKS = 8
SCAN_LIMIT = 24 * 2**20
PROJECT_LIMIT = 56 * 2**20
GIVE_LIMIT = 48 * 2**20
KEEP_LIMIT = 8 * 2**20
HALO = 16


def to_tiles(array):
    rows, width = array.shape
    return array.reshape(CHUNKS, rows // CHUNKS, width).swapaxes(0, 1).reshape(rows, width)


def to_tokens(array):
    rows, width = array.shape
    return array.reshape(rows // CHUNKS, CHUNKS, width).swapaxes(0, 1).reshape(rows, width)


def shifted(array, axis, move):
    count = lax.axis_size(axis)
    return lax.ppermute(array, axis, [(i, move(i)) for i in range(count)])


def across(array):
    return shifted(array, "tp", lambda i: i ^ 1)


def along_x(array, step):
    return shifted(array, "tp", lambda i: (i + 2 * step) % 8)


def token_halo(top, end):
    rows, width = end.shape
    count = lax.axis_size("sp")
    owners = lax.axis_size("tp")
    ends = jnp.concatenate([end[rows - 9 : rows - 8], end[rows - 1 :], top[:1], top[:1]], axis=0)
    copies = jnp.broadcast_to(ends[None], (owners, *ends.shape))
    every = lax.all_to_all(copies, "tp", 0, 0, tiled=True)
    before = lax.ppermute(every[:, :2], "sp", [(i, i + 1) for i in range(count - 1)])
    after = lax.ppermute(every[:, 2:], "sp", [(i + 1, i) for i in range(count - 1)])
    rest = jnp.zeros((owners, HALO - 4, width), end.dtype)
    return jnp.concatenate([before, after, rest], axis=1)


def gathered_stream(top, end):
    left_top = along_x(top, 1)
    right_end = along_x(end, -1)
    left_end = along_x(end, 1)
    right_top = along_x(top, -1)
    far_top = along_x(left_top, 1)
    far_end = along_x(right_end, -1)
    same = (top, end, left_top, left_end, right_top, right_end, far_top, far_end)
    return same + tuple(across(part) for part in same)


def block_of(rank, dx, flip):
    core = rank % 2
    return 2 * ((rank // 2 + dx + 4) % 4) + (1 - core if flip else core)


SHIFTS = (0, -1, 1, 2)


def along_plane(array, axis, step):
    dz, dy = (step, 0) if axis == "z" else (0, step)
    pairs = [
        (4 * z + y, 4 * ((z + dz) % 4) + (y + dy) % 4) for z in range(4) for y in range(4)
    ]
    return lax.ppermute(array, "sp", pairs)


def gathered_pieces(weights):
    half = weights[0].shape[0] // 2
    pieces = []
    for turn, (first, second) in enumerate(("yz", "zy")):
        own = jnp.concatenate([w[turn * half : (turn + 1) * half] for w in weights], axis=0)
        part = own.shape[0] // 2
        before = along_plane(own, first, 1)
        after = along_plane(own, first, -1)
        far_top = along_plane(before[:part], first, 1)
        far_end = along_plane(after[part:], first, -1)
        top = jnp.concatenate([own, before], axis=0)
        end = jnp.concatenate([after, far_top, far_end], axis=0)
        top_before = along_plane(top, second, 1)
        top_after = along_plane(top, second, -1)
        end_after = along_plane(end, second, -1)
        end_before = along_plane(end, second, 1)
        pieces += [top, end, top_before, end_before, top_after, end_after]
        pieces += [along_plane(top_before, second, 1), along_plane(end_after, second, -1)]
    return tuple(pieces)


def block_copies(weight, which, rank, offsets, target, sems):
    size = target.shape[1]
    copies = []
    for n, (dx, flip) in enumerate(offsets):
        at = pl.multiple_of(block_of(rank, dx, flip) * size, size)
        copies.append(
            pltpu.make_async_copy(
                weight.at[which, pl.ds(at, size), :], target.at[n], sems.at[n]
            )
        )
    return copies


def weight_copies(sources, which, place, target, sems):
    blocks, size, _ = target.shape
    if len(sources) == 1:
        return [
            pltpu.make_async_copy(
                sources[0].at[which, pl.ds(n * size, size), :], target.at[n], sems.at[n]
            )
            for n in range(blocks)
        ]
    copies = []
    rows = size // 4
    group = sources[0].shape[0] // 2
    for half in range(2):
        for outer in range(4):
            for inner in range(4):
                ref = sources[8 * half + 2 * outer + inner // 2]
                start = (inner % 2) * group
                dz, dy = (outer, inner) if half == 0 else (inner, outer)
                z = (place // 4 + 4 + SHIFTS[dz]) % 4
                y = (place % 4 + 4 + SHIFTS[dy]) % 4
                at = pl.multiple_of((y % 2) * (2 * rows) + half * rows, rows)
                copies.append(
                    pltpu.make_async_copy(
                        ref.at[pl.ds(start + which * rows, rows), :],
                        target.at[2 * z + y // 2, pl.ds(at, rows), :],
                        sems.at[len(copies)],
                    )
                )
    return copies


ARRIVE = [(dx, flip) for flip in (0, 1) for dx in (0, -1, 1, 2)]
LEAVE = [(dx, flip) for flip in (1, 0) for dx in (2, 1, -1, 0)]


def contracted(rows, weight, total):
    total[...] = jnp.zeros_like(total)

    def step(k, carry):
        left = jnp.concatenate([rows[2 * k], rows[2 * k + 1]], axis=1)
        right = jnp.concatenate([weight[2 * k], weight[2 * k + 1]], axis=0)
        total[...] += jnp.dot(left, right, preferred_element_type=F32)
        return carry

    lax.fori_loop(0, rows.shape[0] // 2, step, 0)


def row_scale(squares, width):
    return lax.rsqrt(jnp.sum(squares[...], axis=1, keepdims=True) / width + NORM_EPS)


def piece_copies(rank, pieces, rows, sems):
    half = pieces[0].shape[0]
    return [
        pltpu.make_async_copy(
            pieces[2 * k + side],
            rows.at[block_of(rank, dx, flip), pl.ds(side * half, half), :],
            sems.at[2 * k + side],
        )
        for k, (dx, flip) in enumerate(ARRIVE)
        for side in range(2)
    ]


def scaled_rows(layer, rank, gain, copies, halo, rows, squares):
    width = rows.shape[2]
    half = (rows.shape[1] - (0 if halo is None else HALO)) // 2
    step = 64
    for k, (dx, flip) in enumerate(ARRIVE):
        copies[2 * k].wait()
        copies[2 * k + 1].wait()
        block = block_of(rank, dx, flip)
        scale = gain[layer : layer + 1, pl.ds(pl.multiple_of(block * width, width), width)]

        def put(raw, at, k=k, block=block, scale=scale):
            raw = raw.astype(F32)
            rows[block, at, :] = (raw * scale).astype(BF16)
            power = raw * raw
            lanes = sum(power[:, 128 * q : 128 * (q + 1)] for q in range(width // 128))
            if k == 0:
                squares[at, :] = lanes
            else:
                squares[at, :] += lanes

        def chunk(n, carry, block=block, put=put):
            for side in range(2):
                at = pl.ds(pl.multiple_of(n * step + side * half, step), step)
                put(rows[block, at, :], at)
            return carry

        lax.fori_loop(0, half // step, chunk, 0)
        if halo is not None:
            put(halo[block], pl.ds(2 * half, HALO))


def project_body(layer, rank, place, gain, halo, *refs):
    pieces, sources = refs[:16], refs[16:-10]
    mix, gate, rows, squares, value_in, gate_in, total, sems, gate_sems, piece_sems = refs[-10:]
    values = weight_copies(sources, 0, place[0], value_in, sems)
    gates = weight_copies(sources, 1, place[0], gate_in, gate_sems)
    arriving = piece_copies(rank[0], pieces, rows, piece_sems)
    for copy in arriving + values:
        copy.start()
    scaled_rows(layer, rank[0], gain, arriving, halo, rows, squares)
    for copy in gates:
        copy.start()
    for copy in values:
        copy.wait()
    scale = row_scale(squares, mix.shape[1] * len(ARRIVE))
    contracted(rows, value_in, total)
    mix[...] = (total[...] * scale).astype(BF16)
    for copy in gates:
        copy.wait()
    contracted(rows, gate_in, total)
    gate[...] = (total[...] * scale)[: gate.shape[0]].astype(BF16)


def in_smem():
    return pl.BlockSpec(memory_space=pltpu.SMEM)


def in_vmem():
    return pl.BlockSpec(memory_space=pltpu.VMEM)


def in_hbm():
    return pl.BlockSpec(memory_space=pltpu.HBM)


def product_cost(rows, width, count):
    return pl.CostEstimate(
        flops=2 * count * rows * width * width,
        bytes_accessed=2 * count * width * width,
        transcendentals=0,
    )


def projected(rank, place, pieces, halo, norm_gain, layer, sources):
    half, width = pieces[0].shape
    count = norm_gain.shape[1] // width
    deep = 2 * half + HALO
    return pl.pallas_call(
        lambda *refs: project_body(layer, *refs),
        out_shape=[
            jax.ShapeDtypeStruct((deep, width), BF16),
            jax.ShapeDtypeStruct((2 * half, width), BF16),
        ],
        in_specs=[in_smem()] * 2 + [in_vmem()] * 2 + [in_hbm()] * (16 + len(sources)),
        out_specs=[in_vmem()] * 2,
        scratch_shapes=[
            pltpu.VMEM((count, deep, width), BF16),
            pltpu.VMEM((deep, 128), F32),
            pltpu.VMEM((count, width, width), BF16),
            pltpu.VMEM((count, width, width), BF16),
            pltpu.VMEM((deep, width), F32),
            pltpu.SemaphoreType.DMA((32,)),
            pltpu.SemaphoreType.DMA((32,)),
            pltpu.SemaphoreType.DMA((16,)),
        ],
        compiler_params=pltpu.CompilerParams(vmem_limit_bytes=PROJECT_LIMIT),
        cost_estimate=product_cost(deep, width, 2 * count),
        name="projected",
    )(rank, place, norm_gain, halo, *pieces, *sources)


def scan_body(
    rank, mix, taps, rate, gates, local, fwd_cum, bwd_cum, coef, edge, padded, conv, pre
):
    steps = conv.shape[0] // CHUNKS
    length = conv.shape[0]
    sub = lax.broadcasted_iota(jnp.int32, (CHUNKS, 128), 0)
    rows = mix[...].astype(F32)
    halo = rows[length : length + 8]
    padded[16 : 16 + length] = rows[:length]
    padded[0:8] = jnp.where(
        sub == 0, halo[0:1], pltpu.roll(rows[length - 16 : length - 8], 1, axis=0)
    )
    padded[8:16] = jnp.where(sub == 0, halo[1:2], pltpu.roll(rows[length - 8 : length], 1, axis=0))
    padded[16 + length : 24 + length] = jnp.where(
        sub == CHUNKS - 1, halo[2:3], pltpu.roll(rows[0:8], CHUNKS - 1, axis=0)
    )
    for part in range(8):
        lo = part * (length // 8)
        hi = lo + length // 8
        conv[lo:hi] = sum(padded[lo + 8 * k : hi + 8 * k] * taps[0, k : k + 1] for k in range(4))
    lhs = conv[...].astype(BF16)
    for g in range(4):
        pre[g] = jnp.dot(lhs, gates[0, g // 2, g % 2], preferred_element_type=F32)

    def cell(i, e):
        at = pl.ds(pl.multiple_of(i * CHUNKS, CHUNKS), CHUNKS)
        recur = jax.nn.sigmoid(pre[2 * e, at, :])
        entry = jax.nn.sigmoid(pre[2 * e + 1, at, :])
        log_a = (-GATE_SCALE) * recur * rate[0, e : e + 1]
        decay = jnp.exp(log_a)
        x = 2.0 * log_a
        near = x * (1.0 + x * (0.5 + x * (1.0 / 6 + x * (1.0 / 24 + x * (1.0 / 120)))))
        room = -jnp.where(x > -0.125, near, decay * decay - 1.0)
        return at, decay, jnp.sqrt(room) * entry * conv[at, :]

    zero = jnp.zeros((CHUNKS, 128), F32)
    one = jnp.ones((CHUNKS, 128), F32)
    inner = 8

    def forward(block, carry):
        state, cum = carry
        for n in range(inner):
            at, decay, drive = cell(block * inner + n, 0)
            state = decay * state + drive
            cum = decay * cum
            local[at, :] = state
            fwd_cum[at, :] = cum
        return state, cum

    def backward(block, carry):
        state, cum = carry
        for n in range(inner):
            at, decay, drive = cell(steps - 1 - (block * inner + n), 1)
            state = decay * state + drive
            cum = decay * cum
            local[at, :] += state
            bwd_cum[at, :] = cum
        return state, cum

    state_f, cum_f = lax.fori_loop(0, steps // inner, forward, (zero, one))
    state_b, cum_b = lax.fori_loop(0, steps // inner, backward, (zero, one))
    alpha = jnp.zeros((1, 128), F32)
    beta = jnp.ones((1, 128), F32)
    for s in range(CHUNKS):
        coef[0, s : s + 1] = alpha
        coef[1, s : s + 1] = beta
        alpha = state_f[s : s + 1] + cum_f[s : s + 1] * alpha
        beta = cum_f[s : s + 1] * beta
    sums_f = (beta, alpha)
    alpha = jnp.zeros((1, 128), F32)
    beta = jnp.ones((1, 128), F32)
    for s in reversed(range(CHUNKS)):
        coef[2, s : s + 1] = alpha
        coef[3, s : s + 1] = beta
        alpha = state_b[s : s + 1] + cum_b[s : s + 1] * alpha
        beta = cum_b[s : s + 1] * beta
    edge[...] = jnp.broadcast_to(
        jnp.concatenate([*sums_f, beta, alpha], axis=0)[None], edge.shape
    )


def scanned(rank, mix, conv_taps, forget_rate, block_gates, layer, copies):
    deep, width = mix.shape
    length = deep - HALO
    blocks = width // 128
    column = lambda b, rank: (0, b)
    owned = lambda b, rank: (layer, 0, rank[0] * blocks + b)
    return pl.pallas_call(
        scan_body,
        grid_spec=pltpu.PrefetchScalarGridSpec(
            num_scalar_prefetch=1,
            grid=(blocks,),
            in_specs=[
                pl.BlockSpec((deep, 128), column),
                pl.BlockSpec((1, 4, 128), owned),
                pl.BlockSpec((1, 2, 128), owned),
                pl.BlockSpec((1, 2, 2, 128, 128), lambda b, rank: (layer, 0, 0, b, 0)),
            ],
            out_specs=[
                pl.BlockSpec((length, 128), column),
                pl.BlockSpec((length, 128), column),
                pl.BlockSpec((length, 128), column),
                pl.BlockSpec((4, CHUNKS, 128), lambda b, rank: (0, 0, b)),
                pl.BlockSpec((copies, 4, 128), lambda b, rank: (0, 0, b)),
            ],
            scratch_shapes=[
                pltpu.VMEM((length + 24, 128), F32),
                pltpu.VMEM((length, 128), F32),
                pltpu.VMEM((4, length, 128), F32),
            ],
        ),
        out_shape=[
            jax.ShapeDtypeStruct((length, width), F32),
            jax.ShapeDtypeStruct((length, width), F32),
            jax.ShapeDtypeStruct((length, width), F32),
            jax.ShapeDtypeStruct((4, CHUNKS, width), F32),
            jax.ShapeDtypeStruct((copies, 4, width), F32),
        ],
        compiler_params=pltpu.CompilerParams(vmem_limit_bytes=SCAN_LIMIT),
        cost_estimate=pl.CostEstimate(
            flops=10_000_000_000, bytes_accessed=4_000_000, transcendentals=4_000_000
        ),
        name="scan",
    )(rank, mix, conv_taps, forget_rate, block_gates)


def features(mixed, weight):
    return lax.dot_general(
        mixed, weight, (((1,), (1,)), ((), ())), preferred_element_type=F32
    ).astype(BF16)


def give_body(
    which, rank, place, edges, local, fwd_cum, bwd_cum, coef, gate, weight,
    mixed, far, rest, keep_in, give_in, give_sems, keep_sems,
):
    gives = block_copies(weight, which, rank[0], LEAVE[:4], give_in, give_sems)
    keeps = block_copies(weight, which, rank[0], LEAVE[4:], keep_in, keep_sems)
    for copy in gives:
        copy.start()
    mine = place[0]
    count, _, width = edges.shape
    enter_f = jnp.zeros((1, width), F32)
    enter_b = jnp.zeros((1, width), F32)
    for r in range(count):
        enter_f = jnp.where(r < mine, edges[r, 1:2] + edges[r, 0:1] * enter_f, enter_f)
        q = count - 1 - r
        enter_b = jnp.where(q > mine, edges[q, 3:4] + edges[q, 2:3] * enter_b, enter_b)
    from_f = coef[0] + coef[1] * enter_f
    from_b = coef[2] + coef[3] * enter_b
    group = 64
    for c in range(width // 128):
        col = slice(128 * c, 128 * (c + 1))
        tiled_f = jnp.concatenate([from_f[:, col]] * (group // CHUNKS), axis=0)
        tiled_b = jnp.concatenate([from_b[:, col]] * (group // CHUNKS), axis=0)

        def part(n, carry, col=col, tiled_f=tiled_f, tiled_b=tiled_b):
            at = pl.ds(pl.multiple_of(n * group, group), group)
            both = local[at, col] + fwd_cum[at, col] * tiled_f + bwd_cum[at, col] * tiled_b
            z = gate[at, col].astype(F32)
            mixed[at, col] = (both * (z * jax.nn.sigmoid(z))).astype(BF16)
            return carry

        lax.fori_loop(0, local.shape[0] // group, part, 0)
    for copy in keeps:
        copy.start()
    for copy in gives:
        copy.wait()
    far[...] = features(mixed[...], give_in[0])

    def step(n, carry):
        rest[n] = features(mixed[...], give_in[n + 1])
        return carry

    lax.fori_loop(0, 3, step, 0)
    for copy in keeps:
        copy.wait()


def given(rank, place, edges, local, fwd_cum, bwd_cum, coef, gate, weights, which):
    length, width = local.shape
    return pl.pallas_call(
        lambda *refs: give_body(which, *refs),
        in_specs=[in_smem()] * 2 + [in_vmem()] * 6 + [in_hbm()],
        out_specs=[in_vmem()] * 4,
        out_shape=[
            jax.ShapeDtypeStruct((length, width), BF16),
            jax.ShapeDtypeStruct((length, width), BF16),
            jax.ShapeDtypeStruct((3, length, width), BF16),
            jax.ShapeDtypeStruct((4, width, width), BF16),
        ],
        scratch_shapes=[
            pltpu.VMEM((4, width, width), BF16),
            pltpu.SemaphoreType.DMA((4,)),
            pltpu.SemaphoreType.DMA((4,)),
        ],
        compiler_params=pltpu.CompilerParams(vmem_limit_bytes=GIVE_LIMIT),
        cost_estimate=product_cost(length, width, 4),
        name="given",
    )(rank, place, edges, local, fwd_cum, bwd_cum, coef, gate, weights)


def keep_body(mixed, weight, far, rest):
    far[...] = features(mixed[...], weight[0])

    def step(n, carry):
        rest[n] = features(mixed[...], weight[n + 1])
        return carry

    lax.fori_loop(0, 3, step, 0)


def kept(mixed, weight):
    length, width = mixed.shape
    return pl.pallas_call(
        keep_body,
        in_specs=[in_vmem()] * 2,
        out_specs=[in_vmem()] * 2,
        out_shape=[
            jax.ShapeDtypeStruct((length, width), BF16),
            jax.ShapeDtypeStruct((3, length, width), BF16),
        ],
        compiler_params=pltpu.CompilerParams(vmem_limit_bytes=KEEP_LIMIT),
        cost_estimate=product_cost(length, width, 4),
        name="kept",
    )(mixed, weight)


def total_of(*parts):
    return sum(part.astype(F32) for part in parts)


def per_device(
    stream_in, norm_gain, value_proj, gate_proj, out_proj, conv_taps, block_gates, forget_rate
):
    rank = lax.axis_index("tp").reshape(1)
    place = lax.axis_index("sp").reshape(1)
    length, _ = stream_in.shape
    half = length // 2
    stream = to_tiles(stream_in)
    top, end = stream[:half], stream[half:]
    pieces_0 = gathered_pieces([value_proj[0], gate_proj[0]])
    outs_0 = lax.all_gather(out_proj[:1], "sp", axis=1, tiled=True)
    held = jnp.stack([value_proj[1], gate_proj[1], out_proj[1]])
    full_1 = lax.all_gather(held, "sp", axis=1, tiled=True)
    weights = [(pieces_0, outs_0, 0), ((full_1,), full_1, 2)]
    for layer in range(value_proj.shape[0]):
        sources, full, which = weights[layer]
        pieces = gathered_stream(top, end)
        halo = token_halo(top, end)
        mix_in, gate_z = projected(rank, place, pieces, halo, norm_gain, layer, sources)
        local, fwd_cum, bwd_cum, coef, edge = scanned(
            rank, mix_in, conv_taps, forget_rate, block_gates, layer, lax.axis_size("sp")
        )
        edges = lax.all_to_all(edge, "sp", 0, 0, tiled=True)
        mixed, far_give, rest_give, keep_weight = given(
            rank, place, edges, local, fwd_cum, bwd_cum, coef, gate_z, full, which
        )
        far_away = across(far_give)
        rest_away = across(rest_give)
        far_keep, rest_keep = kept(mixed, keep_weight)
        far = total_of(far_keep, far_away).astype(BF16)
        halves = (slice(0, half), slice(half, length))
        up, down, own = (
            [(rest_keep[n, rows], rest_away[n, rows]) for rows in halves] for n in range(3)
        )
        relay_top = along_x(far[:half], 1)
        relay_end = along_x(far[half:], -1)
        up_end = along_x(total_of(*up[1]).astype(BF16), 1)
        down_top = along_x(total_of(*down[0]).astype(BF16), -1)
        up_top = along_x(total_of(*up[0], relay_top).astype(BF16), 1)
        down_end = along_x(total_of(*down[1], relay_end).astype(BF16), -1)
        up_top, down_top, up_end, down_end = lax.optimization_barrier(
            (up_top, down_top, up_end, down_end)
        )
        top = total_of(top, *own[0], up_top, down_top).astype(BF16)
        end = total_of(end, *own[1], up_end, down_end).astype(BF16)
    return to_tokens(jnp.concatenate([top, end], axis=0))


def solution(mesh):
    placed = (
        P("sp", "tp"),
        P(),
        P(None, "sp", "tp"),
        P(None, "sp", "tp"),
        P(None, "sp", "tp"),
        P(),
        P(None, None, None, "tp", None),
        P(),
    )
    return jax.shard_map(
        per_device, mesh=mesh, in_specs=placed, out_specs=P("sp", "tp"), check_vma=False
    )
```
